256 devices in a mesh: dp: 4 (over x), kv: 32 (over z, y), tp: 2 (over core).
Axes of the slice: x: 4, y: 4, z: 8, core: 2. Of those that a mesh axis runs over, the one named last changes fastest.
Arguments:
- tokens: bfloat16 [4, 16384, 1024], P('dp', ('kv', 'tp')), may hold values from -6 to 6
- w_query: bfloat16 [1024, 1024], P(None, 'tp'), may hold values from -0.1875 to 0.1875
- w_key: bfloat16 [1024, 256], P(None, 'tp'), may hold values from -0.1875 to 0.1875
- w_value: bfloat16 [1024, 256], P(None, 'tp'), may hold values from -0.1875 to 0.1875
- w_out: bfloat16 [1024, 1024], P('tp'), may hold values from -0.1875 to 0.1875
- chosen: int32 [4, 256, 15], P('dp', 'kv'), may hold values from -1 to 254, as said below
Outputs:
- normed: bfloat16 [4, 16384, 1024], P('dp', ('kv', 'tp'))
- logsums: float32 [4, 16384, 16], P('dp', 'kv', 'tp')
The draws below stay inside these ranges and needn't reach their ends.
Inputs may be any that keep to these rules, and one draw needn't show every extreme that they name: Each entry of chosen[s, c] is -1 or a block below c; entries of a row that are not -1 differ. Within a sequence, the 15 times 8 entries of the query blocks of one aligned run of 8 blocks name at most 4 different blocks inside any one aligned run, and some run pair reaches exactly 4.
All inputs are finite; a program needn't handle non-finite values.
Results may differ from the reference program's by a relative error of at most 0.0085.
Values may be sent and summed in bfloat16 or wider, within the bound.
A program may use at most 64 MiB of HBM per device.

```python
import jax
import jax.numpy as jnp
from jax import lax

D = 1024
HEADS = 16
KV_HEADS = 4
HEAD_DIM = 64
BLK = 64
PICK = 15
CAP = 4
TOK_DEV = 512
SEQS = 4
SEQ = 16384
NBLK = 256


def draw_chosen(key, part):
    local_blocks = TOK_DEV // BLK
    owner_count = NBLK // local_blocks
    key_pool = jax.random.fold_in(key, 11)
    key_popular = jax.random.fold_in(key, 23)
    key_noise = jax.random.fold_in(key, 37)
    pool_scores = jax.random.randint(key_pool, (SEQS, owner_count, owner_count, local_blocks), 0, 4096) * local_blocks
    pool_scores = pool_scores + jnp.arange(local_blocks, dtype=jnp.int32)
    ranking = jnp.argsort(jnp.argsort(pool_scores, axis=-1, stable=True), axis=-1, stable=True)
    member = (ranking < CAP).reshape(SEQS, owner_count, NBLK)
    blocks = jnp.arange(NBLK, dtype=jnp.int32)
    owners = blocks // local_blocks
    earlier_owner = owners[None, :] <= jnp.arange(owner_count, dtype=jnp.int32)[:, None]
    member = member & earlier_owner[None]
    candidate = member[:, owners, :] & (blocks[None, :] < blocks[:, None])[None]
    last_block = blocks % local_blocks == local_blocks - 1
    forced = last_block[:, None] & (owners[None, :] == owners[:, None] - 1)
    popularity = jax.random.randint(key_popular, (SEQS, owner_count), 0, 8)
    noise = jax.random.randint(key_noise, (SEQS, NBLK, NBLK), 0, 2048)
    score = candidate.astype(jnp.int32) * 2 ** 27
    score = score + (forced[None] & candidate).astype(jnp.int32) * 2 ** 26
    score = score + popularity[:, None, :][:, :, owners] * 2 ** 22
    score = score + noise * NBLK + blocks[None, None, :]
    ordered, picked = lax.top_k(score, PICK)
    taken = jnp.take_along_axis(candidate, picked, axis=-1)
    return jnp.where(taken, picked, -1).astype(jnp.int32)


def level_of(own_key, extent, pieces, low, largest):
    gain = 1.0
    for position, parts in pieces:
        steps = jax.random.uniform(jax.random.fold_in(jax.random.fold_in(own_key, 6), position), (parts,), jnp.float32, low / len(pieces), largest / len(pieces))
        gain = gain * jnp.repeat(jnp.exp(steps), extent[position] // parts).reshape((-1,) + (1,) * (len(extent) - 1 - position))
    return gain


def normal_values(key, shape, width, reach, pieces=(), held_as=jnp.bfloat16):
    drawn = jax.random.normal(key, shape, jnp.float32) * width
    if len(pieces) > 0:
        drawn = level_of(key, shape, pieces, -0.22, 0.18) * drawn
    return jnp.clip(drawn, min=-reach, max=reach).astype(held_as)


def setup_inputs(seed: int = 0) -> dict:
    seeds = jax.random.split(jax.random.key(seed), 7)
    tokens = normal_values(seeds[0], (SEQS, SEQ, D), 1.0, 6.0, ((0, 4), (1, 64)))
    w_query = normal_values(seeds[1], (D, HEADS * HEAD_DIM), D ** -0.5, 0.1875, ((1, 2),))
    w_key = normal_values(seeds[2], (D, KV_HEADS * HEAD_DIM), D ** -0.5, 0.1875, ((1, 2),))
    w_value = normal_values(seeds[3], (D, KV_HEADS * HEAD_DIM), D ** -0.5, 0.1875, ((1, 2),))
    w_out = normal_values(seeds[4], (HEADS * HEAD_DIM, D), (HEADS * HEAD_DIM) ** -0.5, 0.1875, ((0, 2),))
    chosen = draw_chosen(jax.random.fold_in(seeds[6], 71), 0)
    return {"tokens": tokens, "w_query": w_query, "w_key": w_key, "w_value": w_value, "w_out": w_out, "chosen": chosen}


THETA_BASE = 10000.0
NEGATIVE = -1e+30
EPSILON = 1e-06

def rotate(values_in, positions):
    half_width = values_in.shape[-1] // 2
    inverse = THETA_BASE ** (-jnp.arange(half_width, dtype=jnp.float32) / half_width)
    angles = positions.astype(jnp.float32)[:, None] * inverse[None, :]
    cosine_table = jnp.cos(angles)[:, None, :]
    sine_table = jnp.sin(angles)[:, None, :]
    as_float = values_in.astype(jnp.float32)
    first_half = as_float[..., :half_width]
    second_half = as_float[..., half_width:]
    joined = jnp.concatenate([first_half * cosine_table - second_half * sine_table, second_half * cosine_table + first_half * sine_table], axis=-1)
    return joined.astype(jnp.bfloat16)

def attend(queries, key_rows, value_rows, usable):
    scores = jnp.einsum('qkgd,nkd->kgqn', queries.astype(jnp.float32), key_rows.astype(jnp.float32))
    scores = scores * HEAD_DIM ** (-0.5)
    scores = jnp.where(usable[None, None], scores, NEGATIVE)
    maximum = lax.optimization_barrier(jnp.max(scores, axis=-1, keepdims=True))
    exponent = jnp.exp(scores - maximum)
    denominator = lax.optimization_barrier(jnp.sum(exponent, axis=-1, keepdims=True))
    logsum = (maximum + jnp.log(denominator))[..., 0]
    weights = (exponent / denominator).astype(jnp.bfloat16)
    combined = jnp.einsum('kgqn,nkd->qkgd', weights.astype(jnp.float32), value_rows.astype(jnp.float32))
    block_rows = queries.shape[0]
    return (combined.astype(jnp.bfloat16).reshape(block_rows, -1), jnp.transpose(logsum, (2, 0, 1)).reshape(block_rows, -1))

def block_mask(usable_picks):
    picked_keys = jnp.repeat(usable_picks, BLK)
    earlier = jnp.broadcast_to(picked_keys[None, :], (BLK, PICK * BLK))
    query_pos = jnp.arange(BLK, dtype=jnp.int32)
    causal = query_pos[None, :] <= query_pos[:, None]
    return jnp.concatenate([earlier, causal], axis=1)

def reference(tokens, w_query, w_key, w_value, w_out, chosen):
    group_size = HEADS // KV_HEADS
    positions = jnp.arange(SEQ, dtype=jnp.int32)

    def one_sequence(element):
        rows_in, chosen_rows = element
        queries = jnp.dot(rows_in, w_query, preferred_element_type=jnp.float32).astype(jnp.bfloat16)
        key_rows = jnp.dot(rows_in, w_key, preferred_element_type=jnp.float32).astype(jnp.bfloat16)
        value_rows = jnp.dot(rows_in, w_value, preferred_element_type=jnp.float32).astype(jnp.bfloat16)
        queries = rotate(queries.reshape(SEQ, HEADS, HEAD_DIM), positions)
        key_rows = rotate(key_rows.reshape(SEQ, KV_HEADS, HEAD_DIM), positions)
        value_rows = value_rows.reshape(SEQ, KV_HEADS, HEAD_DIM)
        query_blocks = queries.reshape(NBLK, BLK, KV_HEADS, group_size, HEAD_DIM)
        key_blocks = key_rows.reshape(NBLK, BLK, KV_HEADS, HEAD_DIM)
        value_blocks = value_rows.reshape(NBLK, BLK, KV_HEADS, HEAD_DIM)

        def one_block(item):
            block_index, block_picks = item
            usable_picks = block_picks >= 0
            safe_index = jnp.maximum(block_picks, 0).astype(jnp.int32)
            gathered_keys = jnp.concatenate([key_blocks[safe_index].reshape(PICK * BLK, KV_HEADS, HEAD_DIM), key_blocks[block_index]], axis=0)
            gathered_values = jnp.concatenate([value_blocks[safe_index].reshape(PICK * BLK, KV_HEADS, HEAD_DIM), value_blocks[block_index]], axis=0)
            return attend(query_blocks[block_index], gathered_keys, gathered_values, block_mask(usable_picks))
        outputs, block_logs = lax.map(one_block, (jnp.arange(NBLK, dtype=jnp.int32), chosen_rows))
        attended = outputs.reshape(SEQ, HEADS * HEAD_DIM)
        projected = jnp.dot(attended, w_out, preferred_element_type=jnp.float32)
        scale_rows = lax.rsqrt(lax.optimization_barrier(jnp.mean(projected * projected, axis=-1, keepdims=True)) + EPSILON)
        return ((projected * scale_rows).astype(jnp.bfloat16), block_logs.reshape(SEQ, HEADS))
    normed, logsums = lax.map(one_sequence, (tokens, chosen))
    return (normed, logsums)
```

```python
import functools
import math

import jax
import jax.numpy as jnp
import numpy as np
from jax import lax
from jax.experimental import pallas as pl
from jax.experimental.pallas import tpu as pltpu
from jax.sharding import PartitionSpec as P

HEAD_DIM = 64
BLK = 64
PICK = 15
THETA_BASE = 10000.0
NEGATIVE = -1e30
EPSILON = 1e-06
MESH = pl.DeviceIdType.MESH
BF = jnp.bfloat16
F32 = jnp.float32
EXPONENT = math.log2(math.e) / math.sqrt(HEAD_DIM)
NY = 4
NZ = 8


def rotary_tables(rows, bases):
    half = HEAD_DIM // 2
    freq = THETA_BASE ** (-np.arange(half, dtype=np.float64) / half)
    freq = np.tile(freq, 128 // half)[None, :]
    offset = np.arange(rows, dtype=np.float64)[:, None] * freq
    base = np.arange(bases, dtype=np.float64)[:, None] * rows * freq
    return [
        np.asarray(a, np.float32)
        for a in (np.cos(offset), np.sin(offset), np.cos(base), np.sin(base))
    ]


def kernel(
    cr_ref, sr_ref, cb_ref, sb_ref, tok_hbm, wq_hbm, wk_hbm, wv_hbm, wo_hbm, chosen_ref,
    out_ref, ls_ref,
    tok, wq, wk, wv, wo, cosine, sine, kvs, kv_all, qs, q_all, ch_all, ch_smem,
    kg, vt, scores, probs, att_out, att_all, ls_out, acc,
    load_sem, w_send, w_recv, ky_send, ky_recv, up_send, up_recv, dn_send, dn_recv,
    pt_send, pt_recv, q_send, q_recv, c_send, c_recv, a_send, a_recv, l_send, l_recv,
):
    kv = lax.axis_index("kv")
    t = lax.axis_index("tp")
    z, y = kv // NY, kv % NY
    other = 1 - t

    def row_peer(k):
        return z * NY + lax.rem(y + k, NY)

    def chunk(zz, yy):
        return pl.ds(((zz * NY + yy) * 2 + t) * 4, 4)

    def remote(src, dst, send, recv, kv_to, tp_to):
        copy = pltpu.make_async_remote_copy(
            src_ref=src, dst_ref=dst, send_sem=send, recv_sem=recv,
            device_id={"kv": kv_to, "tp": tp_to}, device_id_type=MESH,
        )
        copy.start()
        return copy

    loads = [
        pltpu.make_async_copy(tok_hbm, tok, load_sem.at[0]),
        pltpu.make_async_copy(wk_hbm, wk.at[t], load_sem.at[1]),
        pltpu.make_async_copy(wv_hbm, wv.at[t], load_sem.at[2]),
        pltpu.make_async_copy(wq_hbm, wq.at[t], load_sem.at[3]),
        pltpu.make_async_copy(wo_hbm, wo.at[t], load_sem.at[4]),
    ]
    for load in loads:
        load.start()

    barrier = pltpu.get_barrier_semaphore()
    peers = [(row_peer(k), tt) for k in range(1, NY) for tt in (t, other)]
    peers += [(kv, other)]
    z_up = lax.rem(z + 1, NZ) * NY + y
    z_dn = lax.rem(z + NZ - 1, NZ) * NY + y
    peers += [(z_up, t), (z_dn, t)]
    for kv_to, tp_to in peers:
        pl.semaphore_signal(
            barrier, inc=1, device_id={"kv": kv_to, "tp": tp_to}, device_id_type=MESH
        )
    pl.semaphore_wait(barrier, len(peers))

    sent = []
    halves = [
        remote(wk_hbm, wk.at[t], w_send.at[0], w_recv.at[0], kv, other),
        remote(wv_hbm, wv.at[t], w_send.at[1], w_recv.at[1], kv, other),
        remote(wq_hbm, wq.at[t], w_send.at[2], w_recv.at[2], kv, other),
        remote(wo_hbm, wo.at[t], w_send.at[3], w_recv.at[3], kv, other),
    ]
    sent += halves

    ch_all[0] = chosen_ref[...]
    picks = [
        remote(chosen_ref, ch_all.at[NY - k], c_send.at[k], c_recv.at[NY - k], row_peer(k), t)
        for k in range(1, NY)
    ]
    sent += picks

    lane = lax.broadcasted_iota(jnp.int32, (BLK, 128), 1)
    left = lane < BLK
    wide = lax.broadcasted_iota(jnp.int32, (4 * BLK, 128), 1)
    first = lax.rem(wide, HEAD_DIM) < HEAD_DIM // 2

    base = kv * 2 + t
    cb, sb = cb_ref[pl.ds(base, 1), :], sb_ref[pl.ds(base, 1), :]
    cr, sr = cr_ref[...], sr_ref[...]
    cosine[...] = cb * cr - sb * sr
    turned = sb * cr + cb * sr
    sine[...] = jnp.where(first, -turned, turned)

    def rotate(x):
        swapped = jnp.where(first, pltpu.roll(x, 96, 1), pltpu.roll(x, 32, 1))
        return x * cosine[...] + swapped * sine[...]

    def project_kv(half):
        tokens = tok[...]
        keys = jnp.dot(tokens, wk[half], preferred_element_type=F32).astype(BF).astype(F32)
        keys = rotate(keys)
        values = jnp.dot(tokens, wv[half], preferred_element_type=F32)
        values_t = values.T
        keys_swapped = pltpu.roll(keys, 64, 1)
        for e in range(2):
            k_e = keys if e == 0 else keys_swapped
            for j in range(4):
                v_e = values_t[e * 64 : e * 64 + 64, (j // 2) * 128 : (j // 2) * 128 + 128]
                if j % 2 == 0:
                    v_e = pltpu.roll(v_e, 64, 1)
                kvs[2 * half + e, j] = jnp.where(left, k_e[j * 64 : j * 64 + 64], v_e).astype(BF)

    for load in loads[:3]:
        load.wait()
    project_kv(t)
    for copy in halves[:2]:
        copy.wait_recv()
    project_kv(other)

    mine = pltpu.make_async_copy(kvs.at[y], kv_all.at[chunk(z, y)], load_sem.at[5])
    mine.start()
    gathered = [None] * NY
    for k in (1, 3, 2):
        gathered[NY - k] = remote(
            kvs.at[lax.rem(y + k, NY)], kv_all.at[chunk(z, y)],
            ky_send.at[k], ky_recv.at[NY - k], row_peer(k), t,
        )
    sent += gathered[1:]

    ups, downs, partner = {}, {}, {}

    def pass_on(src, zz, k, up=None, down=None, rel=0):
        place = kv_all.at[chunk(zz, lax.rem(y + k, NY))]
        src = place if src is None else src
        if up is not None:
            ups[up, k] = remote(src, place, up_send.at[up, k], up_recv.at[up, k], z_up, t)
        if down is not None:
            downs[down, k] = remote(src, place, dn_send.at[down, k], dn_recv.at[down, k], z_dn, t)
        partner[rel, k] = remote(src, place, pt_send.at[rel, k], pt_recv.at[rel, k], kv, other)

    pass_on(kvs.at[y], z, 0, up=0, down=0, rel=0)

    def project_q(half):
        tokens = tok[...]
        full = jnp.dot(tokens, wq[half], preferred_element_type=F32)
        for n in range(4):
            x = full[:, n * 128 : n * 128 + 128].astype(BF).astype(F32)
            qs[2 * half + n // 2, :, (n % 2) * 128 : (n % 2) * 128 + 128] = rotate(x).astype(BF)

    loads[3].wait()
    project_q(t)
    for k in (1, 3):
        gathered[k].wait_recv()
        pass_on(None, z, k, up=0, down=0, rel=0)
    halves[2].wait_recv()
    project_q(other)
    gathered[2].wait_recv()
    pass_on(None, z, 2, up=0, down=0, rel=0)

    own_q = pltpu.make_async_copy(qs.at[y], q_all.at[0], load_sem.at[6])
    own_q.start()
    queries = [None] * NY
    for k in (2, 1, 3):
        queries[NY - k] = remote(
            qs.at[lax.rem(y + k, NY)], q_all.at[NY - k],
            q_send.at[k], q_recv.at[NY - k], row_peer(k), t,
        )
    sent += queries[1:]

    order = (0, 1, 3, 2)
    for s in range(1, NZ // 2 + 1):
        last = s == NZ // 2
        for k in order:
            if not last or k in (0, 1):
                ups[s - 1, k].wait_recv()
                more = s + 1 < NZ // 2 or (s + 1 == NZ // 2 and k in (0, 1))
                pass_on(
                    None, lax.rem(z + NZ - s, NZ), k, up=s if more else None, rel=NZ - s
                )
            if not last or k in (2, 3):
                downs[s - 1, k].wait_recv()
                more = s + 1 < NZ // 2 or (s + 1 == NZ // 2 and k in (2, 3))
                pass_on(None, lax.rem(z + s, NZ), k, down=s if more else None, rel=s)

    for copy in picks:
        copy.wait_recv()
    to_smem = pltpu.make_async_copy(ch_all, ch_smem, load_sem.at[7])
    to_smem.start()
    to_smem.wait()
    own_q.wait()
    mine.wait()
    for k in range(1, NY):
        queries[k].wait_recv()
    for copy in partner.values():
        copy.wait_recv()

    key_pos = lax.broadcasted_iota(jnp.int32, (BLK, 4 * BLK), 0)
    query_pos = lax.rem(lax.broadcasted_iota(jnp.int32, (BLK, 4 * BLK), 1), BLK)
    causal = key_pos <= query_pos

    def attend(k, jb):
        rows = pl.ds(pl.multiple_of(jb * BLK, BLK), BLK)
        heads = []
        for n in range(2):
            x = q_all[k, rows, n * 128 : n * 128 + 128].astype(F32)
            heads.append(jnp.where(left, x, 0.0))
            heads.append(jnp.where(left, pltpu.roll(x, 64, 1), 0.0))
        q2 = jnp.concatenate(heads, axis=0).astype(BF)
        own = (z * NY + lax.rem(y + k, NY)) * 8 + t * 4 + jb
        bias = []
        block = None
        for j in range(PICK + 1):
            previous = block
            if j < PICK:
                pick = ch_smem[k, t * 4 + jb, j]
                bias.append(jnp.where(pick < 0, NEGATIVE, 0.0).astype(F32))
                block = kv_all[jnp.maximum(pick, 0)]
            else:
                bias.append(None)
                block = kv_all[own]
            kg[j * BLK : j * BLK + BLK, :] = block
            if j % 2 == 1:
                pair = jnp.where(
                    left, pltpu.roll(previous.astype(F32), 64, 1), block.astype(F32)
                )
                vt[:, (j // 2) * 128 : (j // 2) * 128 + 128] = pair.astype(BF)
        scores[...] = lax.dot_general(
            kg[...], q2, (((1,), (1,)), ((), ())), preferred_element_type=F32
        )
        tail = jnp.where(causal, scores[PICK * BLK :, :], NEGATIVE)
        top = jnp.max(tail, axis=0, keepdims=True)
        for j in range(PICK):
            here = jnp.max(scores[j * BLK : j * BLK + BLK, :], axis=0, keepdims=True)
            top = jnp.maximum(top, here + bias[j])
        total = jnp.zeros((1, 4 * BLK), F32)
        for j in range(PICK + 1):
            s = tail if j == PICK else scores[j * BLK : j * BLK + BLK, :]
            shift = top if j == PICK else top - bias[j]
            p = jnp.exp2((s - shift) * EXPONENT)
            total = total + jnp.sum(p, axis=0, keepdims=True)
            probs[j * BLK : j * BLK + BLK, :] = p.astype(BF)
        mixed = jnp.dot(vt[...], probs[...], preferred_element_type=F32)
        mixed = mixed * (1.0 / total)
        turned_back = mixed.T
        parts = [turned_back[h * BLK : h * BLK + BLK] for h in range(4)]
        att_out[k, rows, :] = jnp.concatenate(parts, axis=1).astype(BF)
        ls_out[k, pl.ds(jb, 1), :] = top * HEAD_DIM**-0.5 + jnp.log(total)

    back, logs = {}, {}
    to_self = y // 2 == t
    for k in (2, 1, 3, 0):
        @pl.loop(0, 4)
        def _(jb):
            attend(k, jb)

        if k > 0:
            back[NY - k] = remote(
                att_out.at[k], att_all.at[NY - k], a_send.at[k], a_recv.at[NY - k],
                row_peer(k), t,
            )
        slot = (lax.rem(y, 2), t)
        logs[k] = pltpu.make_async_remote_copy(
            src_ref=ls_out.at[k], dst_ref=ls_ref.at[slot], send_sem=l_send.at[k],
            recv_sem=l_recv.at[slot], device_id={"kv": row_peer(k), "tp": y // 2},
            device_id_type=MESH,
        )
        if k > 0:
            logs[k].start()
        else:
            @pl.when(jnp.logical_not(to_self))
            def _():
                logs[0].start()

            @pl.when(to_self)
            def _():
                ls_ref[slot] = ls_out[0]
    sent += [back[k] for k in range(1, NY)]

    loads[4].wait()
    halves[3].wait_recv()
    for k in (0, 1, 3, 2):
        if k > 0:
            back[k].wait_recv()
        ys = lax.rem(y + k, NY)
        weights = wo[ys // 2, pl.ds(pl.multiple_of(lax.rem(ys, 2) * 256, 256), 256), :]
        piece = att_out[0] if k == 0 else att_all[k]
        part = jnp.dot(piece, weights, preferred_element_type=F32)
        if k == 0:
            acc[...] = part
        elif k != 2:
            acc[...] += part
        else:
            projected = acc[...] + part
            square = jnp.mean(projected * projected, axis=-1, keepdims=True)
            out_ref[...] = (projected * lax.rsqrt(square + EPSILON)).astype(BF)

    for ys in range(2):
        for tt in range(2):
            @pl.when(jnp.logical_not((t * 2 + ys == y) & (t == tt)))
            def _():
                pltpu.make_async_remote_copy(
                    src_ref=ls_out.at[0], dst_ref=ls_ref.at[ys, tt], send_sem=l_send.at[0],
                    recv_sem=l_recv.at[ys, tt], device_id={"kv": kv, "tp": other},
                    device_id_type=MESH,
                ).wait_recv()
    for k in range(1, NY):
        logs[k].wait_send()

    @pl.when(jnp.logical_not(to_self))
    def _():
        logs[0].wait_send()

    for copy in sent + list(ups.values()) + list(downs.values()) + list(partner.values()):
        copy.wait_send()


def shards(tokens, w_query, w_key, w_value, w_out, chosen):
    rows, width = tokens.shape[1:]
    tables = rotary_tables(rows, 2 * NY * NZ)
    any_space = pl.BlockSpec(memory_space=pl.ANY)
    vmem = pl.BlockSpec(memory_space=pltpu.VMEM)
    dma = pltpu.SemaphoreType.DMA
    out, logs = pl.pallas_call(
        kernel,
        out_shape=(
            jax.ShapeDtypeStruct((rows, width), BF),
            jax.ShapeDtypeStruct((2, 2, 4, 4 * BLK), F32),
        ),
        in_specs=[vmem] * 4 + [any_space] * 5 + [vmem],
        out_specs=(vmem, vmem),
        scratch_shapes=[
            pltpu.VMEM((rows, width), BF),
            pltpu.VMEM((2,) + w_query.shape, BF),
            pltpu.VMEM((2,) + w_key.shape, BF),
            pltpu.VMEM((2,) + w_value.shape, BF),
            pltpu.VMEM((2,) + w_out.shape, BF),
            pltpu.VMEM((rows, 128), F32),
            pltpu.VMEM((rows, 128), F32),
            pltpu.VMEM((4, 4, BLK, 128), BF),
            pltpu.VMEM((NZ * NY * 8, BLK, 128), BF),
            pltpu.VMEM((NY, rows, 256), BF),
            pltpu.VMEM((NY, rows, 256), BF),
            pltpu.VMEM((NY, 8, PICK), jnp.int32),
            pltpu.SMEM((NY, 8, PICK), jnp.int32),
            pltpu.VMEM(((PICK + 1) * BLK, 128), BF),
            pltpu.VMEM((BLK, (PICK + 1) * BLK), BF),
            pltpu.VMEM(((PICK + 1) * BLK, 4 * BLK), F32),
            pltpu.VMEM(((PICK + 1) * BLK, 4 * BLK), BF),
            pltpu.VMEM((NY, rows, 256), BF),
            pltpu.VMEM((NY, rows, 256), BF),
            pltpu.VMEM((NY, 4, 4 * BLK), F32),
            pltpu.VMEM((rows, width), F32),
            dma((8,)), dma((4,)), dma((4,)), dma((4,)), dma((4,)),
            dma((4, 4)), dma((4, 4)), dma((4, 4)), dma((4, 4)),
            dma((NZ, 4)), dma((NZ, 4)), dma((4,)), dma((4,)), dma((4,)), dma((4,)),
            dma((4,)), dma((4,)), dma((4,)), dma((2, 2)),
        ],
        compiler_params=pltpu.CompilerParams(
            collective_id=0, has_side_effects=True, vmem_limit_bytes=48 * 1024 * 1024
        ),
    )(*tables, tokens[0], w_query, w_key, w_value, w_out, chosen[0])
    logs = logs.reshape(2, 2, 4, 4, BLK).transpose(1, 2, 4, 0, 3).reshape(2 * rows, 8)
    return out[None], logs[None]


def solution(mesh):
    placed = (
        P("dp", ("kv", "tp"), None),
        P(None, "tp"),
        P(None, "tp"),
        P(None, "tp"),
        P("tp", None),
        P("dp", "kv", None),
    )
    return jax.shard_map(
        shards,
        mesh=mesh,
        in_specs=placed,
        out_specs=(P("dp", ("kv", "tp"), None), P("dp", "kv", "tp")),
        check_vma=False,
    )
```

```python
import functools
import math

import jax
import jax.numpy as jnp
import numpy as np
from jax import lax
from jax.experimental import pallas as pl
from jax.experimental.pallas import tpu as pltpu
from jax.sharding import PartitionSpec as P

HEAD_DIM = 64
BLK = 64
PICK = 15
THETA_BASE = 10000.0
NEGATIVE = -1e30
EPSILON = 1e-06
MESH = pl.DeviceIdType.MESH
BF = jnp.bfloat16
F32 = jnp.float32
EXPONENT = math.log2(math.e) / math.sqrt(HEAD_DIM)
NY = 4
NZ = 8


def rotary_tables(rows, bases):
    half = HEAD_DIM // 2
    freq = THETA_BASE ** (-np.arange(half, dtype=np.float64) / half)
    freq = np.tile(freq, 128 // half)[None, :]
    offset = np.arange(rows, dtype=np.float64)[:, None] * freq
    base = np.arange(bases, dtype=np.float64)[:, None] * rows * freq
    return [
        np.asarray(a, np.float32)
        for a in (np.cos(offset), np.sin(offset), np.cos(base), np.sin(base))
    ]


def kernel(
    cr_hbm, sr_hbm, cb_hbm, sb_hbm, tok_hbm, wq_hbm, wk_hbm, wv_hbm, wo_hbm, ch_hbm,
    out_ref, ls_ref,
    cr_ref, sr_ref, cb_ref, sb_ref, tok, wq, wk, wv, wo, cosine, sine, kvs, kv_all, qs, q_all, ch_all, ch_smem,
    kg, vt, scores, probs, att_out, att_all, ls_out, acc,
    load_sem, w_send, w_recv, ky_send, ky_recv, up_send, up_recv, dn_send, dn_recv,
    pt_send, pt_recv, q_send, q_recv, c_send, c_recv, a_send, a_recv, l_send, l_recv,
):
    kv = lax.axis_index("kv")
    t = lax.axis_index("tp")
    z, y = kv // NY, kv % NY
    other = 1 - t

    def row_peer(k):
        return z * NY + lax.rem(y + k, NY)

    def chunk(zz, yy):
        return pl.ds(((zz * NY + yy) * 2 + t) * 4, 4)

    def remote(src, dst, send, recv, kv_to, tp_to):
        copy = pltpu.make_async_remote_copy(
            src_ref=src, dst_ref=dst, send_sem=send, recv_sem=recv,
            device_id={"kv": kv_to, "tp": tp_to}, device_id_type=MESH,
        )
        copy.start()
        return copy

    loads = [
        pltpu.make_async_copy(tok_hbm, tok, load_sem.at[0]),
        pltpu.make_async_copy(wk_hbm, wk.at[t], load_sem.at[1]),
        pltpu.make_async_copy(wv_hbm, wv.at[t], load_sem.at[2]),
        pltpu.make_async_copy(wq_hbm, wq.at[t], load_sem.at[3]),
        pltpu.make_async_copy(wo_hbm, wo.at[t], load_sem.at[4]),
    ]
    tables = [
        pltpu.make_async_copy(a, b, load_sem.at[8 + i])
        for i, (a, b) in enumerate(
            ((cr_hbm, cr_ref), (sr_hbm, sr_ref), (cb_hbm, cb_ref), (sb_hbm, sb_ref))
        )
    ]
    own_picks = pltpu.make_async_copy(ch_hbm, ch_all.at[0], load_sem.at[12])
    for load in loads[:3] + tables + loads[3:] + [own_picks]:
        load.start()

    barrier = pltpu.get_barrier_semaphore()
    peers = [(row_peer(k), tt) for k in range(1, NY) for tt in (t, other)]
    peers += [(kv, other)]
    z_up = lax.rem(z + 1, NZ) * NY + y
    z_dn = lax.rem(z + NZ - 1, NZ) * NY + y
    peers += [(z_up, t), (z_dn, t)]
    for kv_to, tp_to in peers:
        pl.semaphore_signal(
            barrier, inc=1, device_id={"kv": kv_to, "tp": tp_to}, device_id_type=MESH
        )
    pl.semaphore_wait(barrier, len(peers))

    sent = []
    halves = [
        remote(wk_hbm, wk.at[t], w_send.at[0], w_recv.at[0], kv, other),
        remote(wv_hbm, wv.at[t], w_send.at[1], w_recv.at[1], kv, other),
        remote(wq_hbm, wq.at[t], w_send.at[2], w_recv.at[2], kv, other),
        remote(wo_hbm, wo.at[t], w_send.at[3], w_recv.at[3], kv, other),
    ]
    sent += halves

    picks = [
        remote(ch_hbm, ch_all.at[NY - k], c_send.at[k], c_recv.at[NY - k], row_peer(k), t)
        for k in range(1, NY)
    ]
    sent += picks

    lane = lax.broadcasted_iota(jnp.int32, (BLK, 128), 1)
    left = lane < BLK
    wide = lax.broadcasted_iota(jnp.int32, (4 * BLK, 128), 1)
    first = lax.rem(wide, HEAD_DIM) < HEAD_DIM // 2

    for load in tables:
        load.wait()
    base = kv * 2 + t
    cb, sb = cb_ref[pl.ds(base, 1), :], sb_ref[pl.ds(base, 1), :]
    cr, sr = cr_ref[...], sr_ref[...]
    cosine[...] = cb * cr - sb * sr
    turned = sb * cr + cb * sr
    sine[...] = jnp.where(first, -turned, turned)

    def rotate(x):
        swapped = jnp.where(first, pltpu.roll(x, 96, 1), pltpu.roll(x, 32, 1))
        return x * cosine[...] + swapped * sine[...]

    def project_kv(half):
        tokens = tok[...]
        keys = jnp.dot(tokens, wk[half], preferred_element_type=F32).astype(BF).astype(F32)
        keys = rotate(keys)
        values = jnp.dot(tokens, wv[half], preferred_element_type=F32)
        values_t = values.T
        keys_swapped = pltpu.roll(keys, 64, 1)
        for e in range(2):
            k_e = keys if e == 0 else keys_swapped
            for j in range(4):
                v_e = values_t[e * 64 : e * 64 + 64, (j // 2) * 128 : (j // 2) * 128 + 128]
                if j % 2 == 0:
                    v_e = pltpu.roll(v_e, 64, 1)
                kvs[2 * half + e, j] = jnp.where(left, k_e[j * 64 : j * 64 + 64], v_e).astype(BF)

    for load in loads[:3]:
        load.wait()
    project_kv(t)
    for copy in halves[:2]:
        copy.wait_recv()
    project_kv(other)

    mine = pltpu.make_async_copy(kvs.at[y], kv_all.at[chunk(z, y)], load_sem.at[5])
    mine.start()
    gathered = [None] * NY
    for k in (1, 3, 2):
        gathered[NY - k] = remote(
            kvs.at[lax.rem(y + k, NY)], kv_all.at[chunk(z, y)],
            ky_send.at[k], ky_recv.at[NY - k], row_peer(k), t,
        )
    sent += gathered[1:]

    ups, downs, partner = {}, {}, {}

    def pass_on(src, zz, k, up=None, down=None, rel=0):
        place = kv_all.at[chunk(zz, lax.rem(y + k, NY))]
        src = place if src is None else src
        if up is not None:
            ups[up, k] = remote(src, place, up_send.at[up, k], up_recv.at[up, k], z_up, t)
        if down is not None:
            downs[down, k] = remote(src, place, dn_send.at[down, k], dn_recv.at[down, k], z_dn, t)
        partner[rel, k] = remote(src, place, pt_send.at[rel, k], pt_recv.at[rel, k], kv, other)

    pass_on(kvs.at[y], z, 0, up=0, down=0, rel=0)

    def project_q(half):
        tokens = tok[...]
        full = jnp.dot(tokens, wq[half], preferred_element_type=F32)
        for n in range(4):
            x = full[:, n * 128 : n * 128 + 128].astype(BF).astype(F32)
            qs[2 * half + n // 2, :, (n % 2) * 128 : (n % 2) * 128 + 128] = rotate(x).astype(BF)

    loads[3].wait()
    project_q(t)
    for k in (1, 3):
        gathered[k].wait_recv()
        pass_on(None, z, k, up=0, down=0, rel=0)
    halves[2].wait_recv()
    project_q(other)
    gathered[2].wait_recv()
    pass_on(None, z, 2, up=0, down=0, rel=0)

    own_q = pltpu.make_async_copy(qs.at[y], q_all.at[0], load_sem.at[6])
    own_q.start()
    queries = [None] * NY
    for k in (2, 1, 3):
        queries[NY - k] = remote(
            qs.at[lax.rem(y + k, NY)], q_all.at[NY - k],
            q_send.at[k], q_recv.at[NY - k], row_peer(k), t,
        )
    sent += queries[1:]

    order = (0, 1, 3, 2)
    for s in range(1, NZ // 2 + 1):
        last = s == NZ // 2
        for k in order:
            if not last or k in (0, 1):
                ups[s - 1, k].wait_recv()
                more = s + 1 < NZ // 2 or (s + 1 == NZ // 2 and k in (0, 1))
                pass_on(
                    None, lax.rem(z + NZ - s, NZ), k, up=s if more else None, rel=NZ - s
                )
            if not last or k in (2, 3):
                downs[s - 1, k].wait_recv()
                more = s + 1 < NZ // 2 or (s + 1 == NZ // 2 and k in (2, 3))
                pass_on(None, lax.rem(z + s, NZ), k, down=s if more else None, rel=s)

    for copy in picks:
        copy.wait_recv()
    own_picks.wait()
    to_smem = pltpu.make_async_copy(ch_all, ch_smem, load_sem.at[7])
    to_smem.start()
    to_smem.wait()
    own_q.wait()
    mine.wait()
    for k in range(1, NY):
        queries[k].wait_recv()
    for copy in partner.values():
        copy.wait_recv()

    key_pos = lax.broadcasted_iota(jnp.int32, (BLK, 4 * BLK), 0)
    query_pos = lax.rem(lax.broadcasted_iota(jnp.int32, (BLK, 4 * BLK), 1), BLK)
    causal = key_pos <= query_pos

    def attend(k, jb):
        rows = pl.ds(pl.multiple_of(jb * BLK, BLK), BLK)
        heads = []
        for n in range(2):
            x = q_all[k, rows, n * 128 : n * 128 + 128].astype(F32)
            heads.append(jnp.where(left, x, 0.0))
            heads.append(jnp.where(left, pltpu.roll(x, 64, 1), 0.0))
        q2 = jnp.concatenate(heads, axis=0).astype(BF)
        own = (z * NY + lax.rem(y + k, NY)) * 8 + t * 4 + jb
        bias = []
        block = None
        for j in range(PICK + 1):
            previous = block
            if j < PICK:
                pick = ch_smem[k, t * 4 + jb, j]
                bias.append(jnp.where(pick < 0, NEGATIVE, 0.0).astype(F32))
                block = kv_all[jnp.maximum(pick, 0)]
            else:
                bias.append(None)
                block = kv_all[own]
            kg[j * BLK : j * BLK + BLK, :] = block
            if j % 2 == 1:
                pair = jnp.where(
                    left, pltpu.roll(previous.astype(F32), 64, 1), block.astype(F32)
                )
                vt[:, (j // 2) * 128 : (j // 2) * 128 + 128] = pair.astype(BF)
        scores[...] = lax.dot_general(
            kg[...], q2, (((1,), (1,)), ((), ())), preferred_element_type=F32
        )
        tail = jnp.where(causal, scores[PICK * BLK :, :], NEGATIVE)
        top = jnp.max(tail, axis=0, keepdims=True)
        for j in range(PICK):
            here = jnp.max(scores[j * BLK : j * BLK + BLK, :], axis=0, keepdims=True)
            top = jnp.maximum(top, here + bias[j])
        total = jnp.zeros((1, 4 * BLK), F32)
        for j in range(PICK + 1):
            s = tail if j == PICK else scores[j * BLK : j * BLK + BLK, :]
            shift = top if j == PICK else top - bias[j]
            p = jnp.exp2((s - shift) * EXPONENT)
            total = total + jnp.sum(p, axis=0, keepdims=True)
            probs[j * BLK : j * BLK + BLK, :] = p.astype(BF)
        mixed = jnp.dot(vt[...], probs[...], preferred_element_type=F32)
        mixed = mixed * (1.0 / total)
        turned_back = mixed.T
        parts = [turned_back[h * BLK : h * BLK + BLK] for h in range(4)]
        att_out[k, rows, :] = jnp.concatenate(parts, axis=1).astype(BF)
        ls_out[k, pl.ds(jb, 1), :] = top * HEAD_DIM**-0.5 + jnp.log(total)

    back, logs = {}, {}
    to_self = y // 2 == t
    for k in (2, 1, 3, 0):
        @pl.loop(0, 4)
        def _(jb):
            attend(k, jb)

        if k > 0:
            back[NY - k] = remote(
                att_out.at[k], att_all.at[NY - k], a_send.at[k], a_recv.at[NY - k],
                row_peer(k), t,
            )
        slot = (lax.rem(y, 2), t)
        logs[k] = pltpu.make_async_remote_copy(
            src_ref=ls_out.at[k], dst_ref=ls_ref.at[slot], send_sem=l_send.at[k],
            recv_sem=l_recv.at[slot], device_id={"kv": row_peer(k), "tp": y // 2},
            device_id_type=MESH,
        )
        if k > 0:
            logs[k].start()
        else:
            @pl.when(jnp.logical_not(to_self))
            def _():
                logs[0].start()

            @pl.when(to_self)
            def _():
                ls_ref[slot] = ls_out[0]
    sent += [back[k] for k in range(1, NY)]

    loads[4].wait()
    halves[3].wait_recv()
    for k in (0, 1, 3, 2):
        if k > 0:
            back[k].wait_recv()
        ys = lax.rem(y + k, NY)
        weights = wo[ys // 2, pl.ds(pl.multiple_of(lax.rem(ys, 2) * 256, 256), 256), :]
        piece = att_out[0] if k == 0 else att_all[k]
        part = jnp.dot(piece, weights, preferred_element_type=F32)
        if k == 0:
            acc[...] = part
        elif k != 2:
            acc[...] += part
        else:
            projected = acc[...] + part
            square = jnp.mean(projected * projected, axis=-1, keepdims=True)
            out_ref[...] = (projected * lax.rsqrt(square + EPSILON)).astype(BF)

    for ys in range(2):
        for tt in range(2):
            @pl.when(jnp.logical_not((t * 2 + ys == y) & (t == tt)))
            def _():
                pltpu.make_async_remote_copy(
                    src_ref=ls_out.at[0], dst_ref=ls_ref.at[ys, tt], send_sem=l_send.at[0],
                    recv_sem=l_recv.at[ys, tt], device_id={"kv": kv, "tp": other},
                    device_id_type=MESH,
                ).wait_recv()
    for k in range(1, NY):
        logs[k].wait_send()

    @pl.when(jnp.logical_not(to_self))
    def _():
        logs[0].wait_send()

    for copy in sent + list(ups.values()) + list(downs.values()) + list(partner.values()):
        copy.wait_send()


def shards(tokens, w_query, w_key, w_value, w_out, chosen):
    rows, width = tokens.shape[1:]
    tables = rotary_tables(rows, 2 * NY * NZ)
    any_space = pl.BlockSpec(memory_space=pl.ANY)
    vmem = pl.BlockSpec(memory_space=pltpu.VMEM)
    dma = pltpu.SemaphoreType.DMA
    out, logs = pl.pallas_call(
        kernel,
        out_shape=(
            jax.ShapeDtypeStruct((rows, width), BF),
            jax.ShapeDtypeStruct((2, 2, 4, 4 * BLK), F32),
        ),
        in_specs=[any_space] * 10,
        out_specs=(vmem, vmem),
        scratch_shapes=[
            pltpu.VMEM((rows, 128), F32),
            pltpu.VMEM((rows, 128), F32),
            pltpu.VMEM((2 * NY * NZ, 128), F32),
            pltpu.VMEM((2 * NY * NZ, 128), F32),
            pltpu.VMEM((rows, width), BF),
            pltpu.VMEM((2,) + w_query.shape, BF),
            pltpu.VMEM((2,) + w_key.shape, BF),
            pltpu.VMEM((2,) + w_value.shape, BF),
            pltpu.VMEM((2,) + w_out.shape, BF),
            pltpu.VMEM((rows, 128), F32),
            pltpu.VMEM((rows, 128), F32),
            pltpu.VMEM((4, 4, BLK, 128), BF),
            pltpu.VMEM((NZ * NY * 8, BLK, 128), BF),
            pltpu.VMEM((NY, rows, 256), BF),
            pltpu.VMEM((NY, rows, 256), BF),
            pltpu.VMEM((NY, 8, PICK), jnp.int32),
            pltpu.SMEM((NY, 8, PICK), jnp.int32),
            pltpu.VMEM(((PICK + 1) * BLK, 128), BF),
            pltpu.VMEM((BLK, (PICK + 1) * BLK), BF),
            pltpu.VMEM(((PICK + 1) * BLK, 4 * BLK), F32),
            pltpu.VMEM(((PICK + 1) * BLK, 4 * BLK), BF),
            pltpu.VMEM((NY, rows, 256), BF),
            pltpu.VMEM((NY, rows, 256), BF),
            pltpu.VMEM((NY, 4, 4 * BLK), F32),
            pltpu.VMEM((rows, width), F32),
            dma((13,)), dma((4,)), dma((4,)), dma((4,)), dma((4,)),
            dma((4, 4)), dma((4, 4)), dma((4, 4)), dma((4, 4)),
            dma((NZ, 4)), dma((NZ, 4)), dma((4,)), dma((4,)), dma((4,)), dma((4,)),
            dma((4,)), dma((4,)), dma((4,)), dma((2, 2)),
        ],
        compiler_params=pltpu.CompilerParams(
            collective_id=0, has_side_effects=True, vmem_limit_bytes=67_000_000
        ),
    )(*tables, tokens[0], w_query, w_key, w_value, w_out, chosen[0])
    logs = logs.reshape(2, 2, 4, 4, BLK).transpose(1, 2, 4, 0, 3).reshape(2 * rows, 8)
    return out[None], logs[None]


def solution(mesh):
    placed = (
        P("dp", ("kv", "tp"), None),
        P(None, "tp"),
        P(None, "tp"),
        P(None, "tp"),
        P("tp", None),
        P("dp", "kv", None),
    )
    return jax.shard_map(
        shards,
        mesh=mesh,
        in_specs=placed,
        out_specs=(P("dp", ("kv", "tp"), None), P("dp", "kv", "tp")),
        check_vma=False,
    )
```

```python
import math

import jax
import jax.numpy as jnp
import numpy as np
from jax import lax
from jax.experimental import pallas as pl
from jax.experimental.pallas import tpu as pltpu
from jax.sharding import PartitionSpec as P

HEAD_DIM = 64
BLK = 64
PICK = 15
THETA_BASE = 10000.0
NEGATIVE = -1e30
EPSILON = 1e-06
MESH = pl.DeviceIdType.MESH
BF = jnp.bfloat16
F32 = jnp.float32
EXPONENT = math.log2(math.e) / math.sqrt(HEAD_DIM)
NY = 4
NZ = 8


def rotary_tables(rows, bases):
    half = HEAD_DIM // 2
    freq = THETA_BASE ** (-np.arange(half, dtype=np.float64) / half)
    freq = np.tile(freq, 128 // half)[None, :]
    offset = np.arange(rows, dtype=np.float64)[:, None] * freq
    base = np.arange(bases, dtype=np.float64)[:, None] * rows * freq
    return [
        np.asarray(a, np.float32)
        for a in (np.cos(offset), np.sin(offset), np.cos(base), np.sin(base))
    ]


def kernel(
    cr_hbm, sr_hbm, cb_hbm, sb_hbm, tok_hbm, wq_hbm, wk_hbm, wv_hbm, wo_hbm, ch_hbm,
    out_ref, ls_ref,
    cr_ref, sr_ref, cb_ref, sb_ref, tok, wq, wk, wv, wo, cosine, sine, k_own, v_own,
    k_all, v_all, qs, q_all, ch_all, ch_smem, kg, vt, scores, probs, inverse,
    att_out, att_all, ls_out, acc,
    load_sem, w_send, w_recv, ky_send, ky_recv, vy_send, vy_recv,
    k_up_send, k_up_recv, k_dn_send, k_dn_recv, k_pt_send, k_pt_recv,
    v_up_send, v_up_recv, v_dn_send, v_dn_recv, v_pt_send, v_pt_recv,
    q_send, q_recv, c_send, c_recv, a_send, a_recv, l_send, l_recv,
):
    kv = lax.axis_index("kv")
    t = lax.axis_index("tp")
    z, y = kv // NY, kv % NY
    other = 1 - t

    def row_chip(k):
        return lax.rem(y + k, NY)

    def row_peer(k):
        return z * NY + row_chip(k)

    def chunk(zz, yy):
        return pl.ds(((zz * NY + yy) * 2 + t) * 4, 4)

    def remote(src, dst, send, recv, kv_to, tp_to):
        return pltpu.make_async_remote_copy(
            src_ref=src, dst_ref=dst, send_sem=send, recv_sem=recv,
            device_id={"kv": kv_to, "tp": tp_to}, device_id_type=MESH,
        )

    loads = [
        pltpu.make_async_copy(tok_hbm, tok, load_sem.at[0]),
        pltpu.make_async_copy(wk_hbm, wk.at[t], load_sem.at[1]),
        pltpu.make_async_copy(wv_hbm, wv.at[t], load_sem.at[2]),
        pltpu.make_async_copy(wq_hbm, wq.at[t], load_sem.at[3]),
        pltpu.make_async_copy(wo_hbm, wo.at[t], load_sem.at[4]),
    ]
    tables = [
        pltpu.make_async_copy(a, b, load_sem.at[8 + i])
        for i, (a, b) in enumerate(
            ((cr_hbm, cr_ref), (sr_hbm, sr_ref), (cb_hbm, cb_ref), (sb_hbm, sb_ref))
        )
    ]
    own_picks = pltpu.make_async_copy(ch_hbm, ch_all.at[0], load_sem.at[12])
    for load in loads[:3] + tables + loads[3:] + [own_picks]:
        load.start()

    barrier = pltpu.get_barrier_semaphore()
    peers = [(row_peer(k), tt) for k in range(1, NY) for tt in (t, other)]
    peers += [(kv, other)]
    z_up = lax.rem(z + 1, NZ) * NY + y
    z_dn = lax.rem(z + NZ - 1, NZ) * NY + y
    peers += [(z_up, t), (z_dn, t)]
    for kv_to, tp_to in peers:
        pl.semaphore_signal(
            barrier, inc=1, device_id={"kv": kv_to, "tp": tp_to}, device_id_type=MESH
        )

    left = lax.broadcasted_iota(jnp.int32, (BLK, 128), 1) < BLK
    left_half = lax.broadcasted_iota(jnp.int32, (BLK // 2, 128), 1) < BLK
    wide = lax.broadcasted_iota(jnp.int32, (4 * BLK, 128), 1)
    first = lax.rem(wide, HEAD_DIM) < HEAD_DIM // 2

    for load in tables:
        load.wait()
    base = kv * 2 + t
    cb, sb = cb_ref[pl.ds(base, 1), :], sb_ref[pl.ds(base, 1), :]
    cr, sr = cr_ref[...], sr_ref[...]
    cosine[...] = cb * cr - sb * sr
    turned = sb * cr + cb * sr
    sine[...] = jnp.where(first, -turned, turned)

    def rotate(x):
        swapped = jnp.where(first, pltpu.roll(x, 96, 1), pltpu.roll(x, 32, 1))
        return x * cosine[...] + swapped * sine[...]

    def project_kv(half):
        tokens = tok[...]
        keys = jnp.dot(tokens, wk[half], preferred_element_type=F32).astype(BF).astype(F32)
        keys = rotate(keys)
        keys = (keys, pltpu.roll(keys, 64, 1))
        values = jnp.dot(tokens, wv[half], preferred_element_type=F32).T
        values = [values[:, i * 128 : i * 128 + 128] for i in range(2)]
        values = [(x, pltpu.roll(x, 64, 1)) for x in values]
        for e in range(2):
            for j in range(4):
                low = keys[e][j * 64 : j * 64 + 32]
                high = keys[1 - e][j * 64 + 32 : j * 64 + 64]
                k_own[2 * half + e, j] = jnp.where(left_half, low, high).astype(BF)
                pair = values[j // 2]
                low = pair[j % 2][e * 64 : e * 64 + 32]
                high = pair[1 - j % 2][e * 64 + 32 : e * 64 + 64]
                v_own[2 * half + e, j] = jnp.where(left_half, low, high).astype(BF)

    def project_q(half):
        tokens = tok[...]
        full = jnp.dot(tokens, wq[half], preferred_element_type=F32)
        for n in range(4):
            x = full[:, n * 128 : n * 128 + 128].astype(BF).astype(F32)
            qs[2 * half + n // 2, :, (n % 2) * 128 : (n % 2) * 128 + 128] = rotate(x).astype(BF)

    for load in loads[:3]:
        load.wait()
    project_kv(t)

    pl.semaphore_wait(barrier, len(peers))

    halves = [
        remote(wk_hbm, wk.at[t], w_send.at[0], w_recv.at[0], kv, other),
        remote(wv_hbm, wv.at[t], w_send.at[1], w_recv.at[1], kv, other),
        remote(wq_hbm, wq.at[t], w_send.at[2], w_recv.at[2], kv, other),
        remote(wo_hbm, wo.at[t], w_send.at[3], w_recv.at[3], kv, other),
    ]

    def to_owner(own, every, send, recv, head):
        return remote(
            own.at[head], every.at[chunk(z, y)], send.at[head], recv.at[y], z * NY + head, t
        )

    def key_to_owner(head):
        return to_owner(k_own, k_all, ky_send, ky_recv, head)

    def value_to_owner(head):
        return to_owner(v_own, v_all, vy_send, vy_recv, head)

    def send_heads(half):
        for make in (key_to_owner, value_to_owner):
            for e in range(2):
                head = 2 * half + e

                @pl.when(head != y)
                def _():
                    make(head).start()

    for copy in halves[:2]:
        copy.start()
    send_heads(t)
    picks = [
        remote(ch_hbm, ch_all.at[NY - k], c_send.at[k], c_recv.at[NY - k], row_peer(k), t)
        for k in range(1, NY)
    ]
    for copy in halves[2:] + picks:
        copy.start()

    loads[3].wait()
    project_q(t)
    for copy in halves[:2]:
        copy.wait_recv()
    project_kv(other)
    send_heads(other)

    def ring(every, up_send, up_recv, dn_send, dn_recv, pt_send, pt_recv):
        def place(zz, k):
            return every.at[chunk(zz, row_chip(k))]

        def up(s, k, src=None):
            spot = place(lax.rem(z + NZ - s, NZ), k)
            src = spot if src is None else src
            return remote(src, spot, up_send.at[s, k], up_recv.at[s, k], z_up, t)

        def down(s, k, src=None):
            spot = place(lax.rem(z + s, NZ), k)
            src = spot if src is None else src
            return remote(src, spot, dn_send.at[s, k], dn_recv.at[s, k], z_dn, t)

        def partner(rel, k, src=None):
            spot = place(lax.rem(z + rel, NZ), k)
            src = spot if src is None else src
            return remote(src, spot, pt_send.at[rel, k], pt_recv.at[rel, k], kv, other)

        return up, down, partner

    k_ring = ring(k_all, k_up_send, k_up_recv, k_dn_send, k_dn_recv, k_pt_send, k_pt_recv)
    v_ring = ring(v_all, v_up_send, v_up_recv, v_dn_send, v_dn_recv, v_pt_send, v_pt_recv)

    def begin(group, k, src=None):
        up, down, partner = group
        up(0, k, src).start()
        down(0, k, src).start()
        partner(0, k, src).start()

    def step(group, s, k):
        up, down, partner = group
        if s < NZ // 2:
            turn = s == NZ // 2 - 1
            up(s - 1, k).wait_recv()
            if not turn:
                up(s, k).start()
            else:
                pl.when(k < 2)(lambda: up(s, k).start())
            partner(NZ - s, k).start()
            down(s - 1, k).wait_recv()
            if not turn:
                down(s, k).start()
            else:
                pl.when(k >= 2)(lambda: down(s, k).start())
            partner(s, k).start()
        else:
            pl.when(k < 2)(lambda: up(s - 1, k).wait_recv())
            pl.when(k >= 2)(lambda: down(s - 1, k).wait_recv())
            partner(s, k).start()

    mine = [
        pltpu.make_async_copy(k_own.at[y], k_all.at[chunk(z, y)], load_sem.at[5]),
        pltpu.make_async_copy(v_own.at[y], v_all.at[chunk(z, y)], load_sem.at[7]),
    ]
    begin(k_ring, 0, k_own.at[y])
    for copy in mine:
        copy.start()

    halves[2].wait_recv()
    project_q(other)
    own_q = pltpu.make_async_copy(qs.at[y], q_all.at[0], load_sem.at[6])
    own_q.start()
    queries = [None] * NY
    for k in (2, 1, 3):
        queries[NY - k] = remote(
            qs.at[row_chip(k)], q_all.at[NY - k], q_send.at[k], q_recv.at[NY - k],
            row_peer(k), t,
        )
        queries[NY - k].start()

    def from_row(every, own, send, recv, k):
        remote(
            own.at[0], every.at[chunk(z, row_chip(k))], send.at[0], recv.at[row_chip(k)],
            row_peer(k), t,
        ).wait_recv()

    for k in (1, 3, 2):
        from_row(k_all, k_own, ky_send, ky_recv, k)
        begin(k_ring, k)
    for s in range(1, NZ // 2):
        for k in range(NY):
            step(k_ring, s, k)
    for copy in mine:
        copy.wait()
    begin(v_ring, 0)
    for k in (1, 2, 3):
        from_row(v_all, v_own, vy_send, vy_recv, k)
        begin(v_ring, k)
    for k in range(NY):
        step(k_ring, NZ // 2, k)

    for copy in picks:
        copy.wait_recv()
    own_picks.wait()
    to_smem = pltpu.make_async_copy(ch_all, ch_smem, load_sem.at[13])
    to_smem.start()
    to_smem.wait()
    own_q.wait()
    for k in range(1, NY):
        queries[k].wait_recv()
    for rel in range(NZ):
        for k in range(NY):
            k_ring[2](rel, k).wait_recv()

    key_pos = lax.broadcasted_iota(jnp.int32, (BLK, 4 * BLK), 0)
    query_pos = lax.rem(lax.broadcasted_iota(jnp.int32, (BLK, 4 * BLK), 1), BLK)
    causal = key_pos <= query_pos
    half_blk = BLK // 2

    def own_block(k, jb):
        return (z * NY + row_chip(k)) * 8 + t * 4 + jb

    def weigh(k, jb):
        rows = pl.ds(pl.multiple_of(jb * BLK, BLK), BLK)
        heads = []
        for n in range(2):
            x = q_all[k, rows, n * 128 : n * 128 + 128].astype(F32)
            swapped = pltpu.roll(x, 64, 1)
            heads += [jnp.where(left, x, swapped), jnp.where(left, swapped, x)]
        q2 = jnp.concatenate(heads, axis=0).astype(BF)
        bias = []
        for j in range(PICK + 1):
            if j < PICK:
                pick = ch_smem[k, t * 4 + jb, j]
                bias.append(jnp.where(pick < 0, NEGATIVE, 0.0).astype(F32))
                block = k_all[jnp.maximum(pick, 0)]
            else:
                block = k_all[own_block(k, jb)]
            nothing = jnp.zeros_like(block)
            kg[j * BLK : j * BLK + half_blk, :] = jnp.where(left_half, block, nothing)
            kg[j * BLK + half_blk : j * BLK + BLK, :] = jnp.where(left_half, nothing, block)
        scores[...] = lax.dot_general(
            kg[...], q2, (((1,), (1,)), ((), ())), preferred_element_type=F32
        )
        tail = jnp.where(causal, scores[PICK * BLK :, :], NEGATIVE)
        top = jnp.max(tail, axis=0, keepdims=True)
        for j in range(PICK):
            here = jnp.max(scores[j * BLK : j * BLK + BLK, :], axis=0, keepdims=True)
            top = jnp.maximum(top, here + bias[j])
        total = jnp.zeros((1, 4 * BLK), F32)
        for j in range(PICK + 1):
            s = tail if j == PICK else scores[j * BLK : j * BLK + BLK, :]
            shift = top if j == PICK else top - bias[j]
            p = jnp.exp2((s - shift) * EXPONENT)
            total = total + jnp.sum(p, axis=0, keepdims=True)
            probs[k * 4 + jb, j * BLK : j * BLK + BLK, :] = p.astype(BF)
        inverse[k, pl.ds(jb, 1), :] = 1.0 / total
        ls_out[k, pl.ds(jb, 1), :] = top * HEAD_DIM**-0.5 + jnp.log(total)

    def combine(k, jb):
        rows = pl.ds(pl.multiple_of(jb * BLK, BLK), BLK)
        previous = None
        for j in range(PICK + 1):
            if j < PICK:
                block = v_all[jnp.maximum(ch_smem[k, t * 4 + jb, j], 0)]
            else:
                block = v_all[own_block(k, jb)]
            block = block.astype(F32)
            if j % 2 == 1:
                low = jnp.where(left_half, previous, pltpu.roll(block, 64, 1))
                high = jnp.where(left_half, pltpu.roll(previous, 64, 1), block)
                columns = slice((j // 2) * 128, (j // 2) * 128 + 128)
                vt[:half_blk, columns] = low.astype(BF)
                vt[half_blk:, columns] = high.astype(BF)
            previous = block
        mixed = jnp.dot(vt[...], probs[k * 4 + jb], preferred_element_type=F32)
        turned_back = (mixed * inverse[k, pl.ds(jb, 1), :]).T
        parts = [turned_back[h * BLK : h * BLK + BLK] for h in range(4)]
        att_out[k, rows, :] = jnp.concatenate(parts, axis=1).astype(BF)

    to_self = y // 2 == t
    slot = (lax.rem(y, 2), t)

    def log_piece(k):
        return remote(
            ls_out.at[k], ls_ref.at[slot], l_send.at[k], l_recv.at[slot], row_peer(k), y // 2
        )

    for s, k in enumerate((2, 1, 3, 0)):
        @pl.loop(0, 4)
        def _(jb):
            weigh(k, jb)
            step(v_ring, s + 1, jb)

        if k > 0:
            log_piece(k).start()
        else:
            pl.when(jnp.logical_not(to_self))(lambda: log_piece(0).start())

            @pl.when(to_self)
            def _():
                ls_ref[slot] = ls_out[0]

    for rel in range(NZ):
        for k in range(NY):
            v_ring[2](rel, k).wait_recv()

    back = {}
    for k in (2, 1, 3, 0):
        @pl.loop(0, 4)
        def _(jb):
            combine(k, jb)

        if k > 0:
            back[NY - k] = remote(
                att_out.at[k], att_all.at[NY - k], a_send.at[k], a_recv.at[NY - k],
                row_peer(k), t,
            )
            back[NY - k].start()

    loads[4].wait()
    halves[3].wait_recv()
    for k in (0, 1, 3, 2):
        if k > 0:
            back[k].wait_recv()
        ys = row_chip(k)
        weights = wo[ys // 2, pl.ds(pl.multiple_of(lax.rem(ys, 2) * 256, 256), 256), :]
        piece = att_out[0] if k == 0 else att_all[k]
        part = jnp.dot(piece, weights, preferred_element_type=F32)
        if k == 0:
            acc[...] = part
        elif k != 2:
            acc[...] += part
        else:
            projected = acc[...] + part
            square = jnp.mean(projected * projected, axis=-1, keepdims=True)
            out_ref[...] = (projected * lax.rsqrt(square + EPSILON)).astype(BF)

    for ys in range(2):
        for tt in range(2):
            @pl.when(jnp.logical_not((t * 2 + ys == y) & (t == tt)))
            def _():
                remote(
                    ls_out.at[0], ls_ref.at[ys, tt], l_send.at[0], l_recv.at[ys, tt], kv, other
                ).wait_recv()
    for k in range(1, NY):
        log_piece(k).wait_send()
    pl.when(jnp.logical_not(to_self))(lambda: log_piece(0).wait_send())
    for k in range(1, NY):
        key_to_owner(row_chip(k)).wait_send()
        value_to_owner(row_chip(k)).wait_send()
        queries[k].wait_send()
        back[k].wait_send()
    for copy in halves + picks:
        copy.wait_send()
    for up, down, partner in (k_ring, v_ring):
        for k in range(NY):
            for s in range(NZ // 2):
                if s < NZ // 2 - 1 or k < 2:
                    up(s, k).wait_send()
                if s < NZ // 2 - 1 or k >= 2:
                    down(s, k).wait_send()
            for rel in range(NZ):
                partner(rel, k).wait_send()


def shards(tokens, w_query, w_key, w_value, w_out, chosen):
    rows, width = tokens.shape[1:]
    tables = rotary_tables(rows, 2 * NY * NZ)
    any_space = pl.BlockSpec(memory_space=pl.ANY)
    vmem = pl.BlockSpec(memory_space=pltpu.VMEM)
    dma = pltpu.SemaphoreType.DMA
    out, logs = pl.pallas_call(
        kernel,
        out_shape=(
            jax.ShapeDtypeStruct((rows, width), BF),
            jax.ShapeDtypeStruct((2, 2, 4, 4 * BLK), F32),
        ),
        in_specs=[any_space] * 10,
        out_specs=(vmem, vmem),
        scratch_shapes=[
            pltpu.VMEM((rows, 128), F32),
            pltpu.VMEM((rows, 128), F32),
            pltpu.VMEM((2 * NY * NZ, 128), F32),
            pltpu.VMEM((2 * NY * NZ, 128), F32),
            pltpu.VMEM((rows, width), BF),
            pltpu.VMEM((2,) + w_query.shape, BF),
            pltpu.VMEM((2,) + w_key.shape, BF),
            pltpu.VMEM((2,) + w_value.shape, BF),
            pltpu.VMEM((2,) + w_out.shape, BF),
            pltpu.VMEM((rows, 128), F32),
            pltpu.VMEM((rows, 128), F32),
            pltpu.VMEM((4, 4, BLK // 2, 128), BF),
            pltpu.VMEM((4, 4, BLK // 2, 128), BF),
            pltpu.VMEM((NZ * NY * 8, BLK // 2, 128), BF),
            pltpu.VMEM((NZ * NY * 8, BLK // 2, 128), BF),
            pltpu.VMEM((NY, rows, 256), BF),
            pltpu.VMEM((NY, rows, 256), BF),
            pltpu.VMEM((NY, 8, PICK), jnp.int32),
            pltpu.SMEM((NY, 8, PICK), jnp.int32),
            pltpu.VMEM(((PICK + 1) * BLK, 128), BF),
            pltpu.VMEM((BLK, (PICK + 1) * BLK), BF),
            pltpu.VMEM(((PICK + 1) * BLK, 4 * BLK), F32),
            pltpu.VMEM((NY * 4, (PICK + 1) * BLK, 4 * BLK), BF),
            pltpu.VMEM((NY, 4, 4 * BLK), F32),
            pltpu.VMEM((NY, rows, 256), BF),
            pltpu.VMEM((NY, rows, 256), BF),
            pltpu.VMEM((NY, 4, 4 * BLK), F32),
            pltpu.VMEM((rows, width), F32),
            dma((14,)), dma((4,)), dma((4,)), dma((4,)), dma((4,)), dma((4,)), dma((4,)),
            dma((4, 4)), dma((4, 4)), dma((4, 4)), dma((4, 4)), dma((NZ, 4)), dma((NZ, 4)),
            dma((4, 4)), dma((4, 4)), dma((4, 4)), dma((4, 4)), dma((NZ, 4)), dma((NZ, 4)),
            dma((4,)), dma((4,)), dma((4,)), dma((4,)),
            dma((4,)), dma((4,)), dma((4,)), dma((2, 2)),
        ],
        compiler_params=pltpu.CompilerParams(
            collective_id=0, has_side_effects=True, vmem_limit_bytes=67_000_000
        ),
    )(*tables, tokens[0], w_query, w_key, w_value, w_out, chosen[0])
    logs = logs.reshape(2, 2, 4, 4, BLK).transpose(1, 2, 4, 0, 3).reshape(2 * rows, 8)
    return out[None], logs[None]


def solution(mesh):
    placed = (
        P("dp", ("kv", "tp"), None),
        P(None, "tp"),
        P(None, "tp"),
        P(None, "tp"),
        P("tp", None),
        P("dp", "kv", None),
    )
    return jax.shard_map(
        shards,
        mesh=mesh,
        in_specs=placed,
        out_specs=(P("dp", ("kv", "tp"), None), P("dp", "kv", "tp")),
        check_vma=False,
    )
```

```python
import math

import jax
import jax.numpy as jnp
import numpy as np
from jax import lax
from jax.experimental import pallas as pl
from jax.experimental.pallas import tpu as pltpu
from jax.sharding import PartitionSpec as P

HEAD_DIM = 64
BLK = 64
PICK = 15
THETA_BASE = 10000.0
NEGATIVE = -1e30
EPSILON = 1e-06
MESH = pl.DeviceIdType.MESH
BF = jnp.bfloat16
F32 = jnp.float32
EXPONENT = math.log2(math.e) / math.sqrt(HEAD_DIM)
NY = 4
NZ = 8


def rotary_tables(rows, bases):
    half = HEAD_DIM // 2
    freq = THETA_BASE ** (-np.arange(half, dtype=np.float64) / half)
    freq = np.tile(freq, 128 // half)[None, :]
    offset = np.arange(rows, dtype=np.float64)[:, None] * freq
    base = np.arange(bases, dtype=np.float64)[:, None] * rows * freq
    return [
        np.asarray(a, np.float32)
        for a in (np.cos(offset), np.sin(offset), np.cos(base), np.sin(base))
    ]


def kernel(
    cr_hbm, sr_hbm, cb_hbm, sb_hbm, tok_hbm, wq_hbm, wk_hbm, wv_hbm, wo_hbm, ch_hbm,
    out_ref, ls_ref,
    cr_ref, sr_ref, cb_ref, sb_ref, tok, wq, wk, wv, wo, cosine, sine, k_own, v_own,
    k_all, v_all, qs, q_all, ch_all, ch_smem, kg, vt, scores, probs, inverse,
    att_out, att_all, ls_out, acc,
    load_sem, w_send, w_recv, ky_send, ky_recv, vy_send, vy_recv,
    k_own_send, k_own_recv, k_up_send, k_up_recv, k_dn_send, k_dn_recv, k_pt_send, k_pt_recv,
    v_own_send, v_own_recv, v_up_send, v_up_recv, v_dn_send, v_dn_recv, v_pt_send, v_pt_recv,
    q_send, q_recv, c_send, c_recv, a_send, a_recv, l_send, l_recv,
):
    kv = lax.axis_index("kv")
    t = lax.axis_index("tp")
    z, y = kv // NY, kv % NY
    other = 1 - t

    def row_chip(k):
        return lax.rem(y + k, NY)

    def row_peer(k):
        return z * NY + row_chip(k)

    def chunk(zz, yy):
        return pl.ds(zz * 32 + t * 16 + yy * 4, 4)

    def near(r):
        c, i = r // 2, r % 2
        return 2 * lax.rem(y // 2 + c, 2) + lax.rem(y * (1 - c) + i, 2)

    def pair_chunk(zz, c):
        return pl.ds(zz * 32 + t * 16 + lax.rem(y // 2 + c, 2) * 8, 8)

    def place_of(block):
        return block // 32 * 32 + block // 4 % 2 * 16 + block // 8 % 4 * 4 + block % 4

    def remote(src, dst, send, recv, kv_to, tp_to):
        return pltpu.make_async_remote_copy(
            src_ref=src, dst_ref=dst, send_sem=send, recv_sem=recv,
            device_id={"kv": kv_to, "tp": tp_to}, device_id_type=MESH,
        )

    loads = [
        pltpu.make_async_copy(tok_hbm, tok, load_sem.at[0]),
        pltpu.make_async_copy(wk_hbm, wk.at[t], load_sem.at[1]),
        pltpu.make_async_copy(wv_hbm, wv.at[t], load_sem.at[2]),
        pltpu.make_async_copy(wq_hbm, wq.at[t], load_sem.at[3]),
        pltpu.make_async_copy(wo_hbm, wo.at[t], load_sem.at[4]),
    ]
    tables = [
        pltpu.make_async_copy(a, b, load_sem.at[8 + i])
        for i, (a, b) in enumerate(
            ((cr_hbm, cr_ref), (sr_hbm, sr_ref), (cb_hbm, cb_ref), (sb_hbm, sb_ref))
        )
    ]
    own_picks = pltpu.make_async_copy(ch_hbm, ch_all.at[0], load_sem.at[12])
    for load in loads[:3] + tables + loads[3:] + [own_picks]:
        load.start()

    barrier = pltpu.get_barrier_semaphore()
    peers = [(row_peer(k), tt) for k in range(1, NY) for tt in (t, other)]
    peers += [(kv, other)]
    z_up = lax.rem(z + 1, NZ) * NY + y
    z_dn = lax.rem(z + NZ - 1, NZ) * NY + y
    peers += [(z_up, t), (z_dn, t)]
    for kv_to, tp_to in peers:
        pl.semaphore_signal(
            barrier, inc=1, device_id={"kv": kv_to, "tp": tp_to}, device_id_type=MESH
        )

    left = lax.broadcasted_iota(jnp.int32, (BLK, 128), 1) < BLK
    left_half = lax.broadcasted_iota(jnp.int32, (BLK // 2, 128), 1) < BLK
    wide = lax.broadcasted_iota(jnp.int32, (4 * BLK, 128), 1)
    first = lax.rem(wide, HEAD_DIM) < HEAD_DIM // 2

    for load in tables:
        load.wait()
    base = kv * 2 + t
    cb, sb = cb_ref[pl.ds(base, 1), :], sb_ref[pl.ds(base, 1), :]
    cr, sr = cr_ref[...], sr_ref[...]
    cosine[...] = cb * cr - sb * sr
    turned = sb * cr + cb * sr
    sine[...] = jnp.where(first, -turned, turned)

    def rotate(x):
        swapped = jnp.where(first, pltpu.roll(x, 96, 1), pltpu.roll(x, 32, 1))
        return x * cosine[...] + swapped * sine[...]

    def project_kv(half):
        tokens = tok[...]
        keys = jnp.dot(tokens, wk[half], preferred_element_type=F32).astype(BF).astype(F32)
        keys = rotate(keys)
        keys = (keys, pltpu.roll(keys, 64, 1))
        values = jnp.dot(tokens, wv[half], preferred_element_type=F32).T
        values = [values[:, i * 128 : i * 128 + 128] for i in range(2)]
        values = [(x, pltpu.roll(x, 64, 1)) for x in values]
        for e in range(2):
            for j in range(4):
                low = keys[e][j * 64 : j * 64 + 32]
                high = keys[1 - e][j * 64 + 32 : j * 64 + 64]
                k_own[2 * half + e, j] = jnp.where(left_half, low, high).astype(BF)
                pair = values[j // 2]
                low = pair[j % 2][e * 64 : e * 64 + 32]
                high = pair[1 - j % 2][e * 64 + 32 : e * 64 + 64]
                v_own[2 * half + e, j] = jnp.where(left_half, low, high).astype(BF)

    def project_q(half):
        tokens = tok[...]
        full = jnp.dot(tokens, wq[half], preferred_element_type=F32)
        for n in range(4):
            x = full[:, n * 128 : n * 128 + 128].astype(BF).astype(F32)
            qs[2 * half + n // 2, :, (n % 2) * 128 : (n % 2) * 128 + 128] = rotate(x).astype(BF)

    for load in loads[:3]:
        load.wait()
    project_kv(t)

    pl.semaphore_wait(barrier, len(peers))

    halves = [
        remote(wk_hbm, wk.at[t], w_send.at[0], w_recv.at[0], kv, other),
        remote(wv_hbm, wv.at[t], w_send.at[1], w_recv.at[1], kv, other),
        remote(wq_hbm, wq.at[t], w_send.at[2], w_recv.at[2], kv, other),
        remote(wo_hbm, wo.at[t], w_send.at[3], w_recv.at[3], kv, other),
    ]

    def to_owner(own, every, send, recv, head):
        return remote(
            own.at[head], every.at[chunk(z, y)], send.at[head], recv.at[y], z * NY + head, t
        )

    def key_to_owner(head):
        return to_owner(k_own, k_all, ky_send, ky_recv, head)

    def value_to_owner(head):
        return to_owner(v_own, v_all, vy_send, vy_recv, head)

    def send_heads(half):
        for make in (key_to_owner, value_to_owner):
            for e in range(2):
                head = 2 * half + e

                @pl.when(head != y)
                def _():
                    make(head).start()

    for copy in halves[:2]:
        copy.start()
    send_heads(t)
    picks = [
        remote(ch_hbm, ch_all.at[NY - k], c_send.at[k], c_recv.at[NY - k], row_peer(k), t)
        for k in range(1, NY)
    ]
    for copy in halves[2:] + picks:
        copy.start()

    loads[3].wait()
    project_q(t)
    for copy in halves[:2]:
        copy.wait_recv()
    project_kv(other)
    send_heads(other)

    def ring(every, own_send, own_recv, up_send, up_recv, dn_send, dn_recv, pt_send, pt_recv):
        def up(s, c, src=None):
            if s == 0:
                spot = every.at[chunk(z, near(c))]
                return remote(
                    spot if src is None else src, spot, own_send.at[0, c], own_recv.at[0, c],
                    z_up, t,
                )
            spot = every.at[pair_chunk(lax.rem(z + NZ - s, NZ), c)]
            return remote(spot, spot, up_send.at[s, c], up_recv.at[s, c], z_up, t)

        def down(s, c, src=None):
            if s == 0:
                spot = every.at[chunk(z, near(c))]
                return remote(
                    spot if src is None else src, spot, own_send.at[1, c], own_recv.at[1, c],
                    z_dn, t,
                )
            spot = every.at[pair_chunk(lax.rem(z + s, NZ), c)]
            return remote(spot, spot, dn_send.at[s, c], dn_recv.at[s, c], z_dn, t)

        def partner(rel, c):
            spot = every.at[pair_chunk(lax.rem(z + rel, NZ), c)]
            return remote(spot, spot, pt_send.at[rel, c], pt_recv.at[rel, c], kv, other)

        return up, down, partner

    k_ring = ring(
        k_all, k_own_send, k_own_recv, k_up_send, k_up_recv, k_dn_send, k_dn_recv,
        k_pt_send, k_pt_recv,
    )
    v_ring = ring(
        v_all, v_own_send, v_own_recv, v_up_send, v_up_recv, v_dn_send, v_dn_recv,
        v_pt_send, v_pt_recv,
    )

    def begin(group, r, src=None):
        group[0](0, r, src).start()
        group[1](0, r, src).start()

    def step(group, s, c):
        up, down, partner = group
        if s == 1:
            for both in (up, down):
                for i in range(2):
                    both(0, 2 * c + i).wait_recv()
                both(1, c).start()
            partner(NZ - 1, c).start()
            partner(1, c).start()
        elif s < NZ // 2:
            turn = s == NZ // 2 - 1
            up(s - 1, c).wait_recv()
            pl.when(not turn or c == 0)(lambda: up(s, c).start())
            partner(NZ - s, c).start()
            down(s - 1, c).wait_recv()
            pl.when(not turn or c == 1)(lambda: down(s, c).start())
            partner(s, c).start()
        else:
            pl.when(c == 0)(lambda: up(s - 1, c).wait_recv())
            pl.when(c == 1)(lambda: down(s - 1, c).wait_recv())
            partner(s, c).start()

    mine = [
        pltpu.make_async_copy(k_own.at[y], k_all.at[chunk(z, y)], load_sem.at[5]),
        pltpu.make_async_copy(v_own.at[y], v_all.at[chunk(z, y)], load_sem.at[7]),
    ]
    begin(k_ring, 0, k_own.at[y])
    for copy in mine:
        copy.start()

    halves[2].wait_recv()
    project_q(other)
    own_q = pltpu.make_async_copy(qs.at[y], q_all.at[0], load_sem.at[6])
    own_q.start()
    queries = [None] * NY
    for k in (2, 1, 3):
        queries[NY - k] = remote(
            qs.at[row_chip(k)], q_all.at[NY - k], q_send.at[k], q_recv.at[NY - k],
            row_peer(k), t,
        )
        queries[NY - k].start()

    for copy in picks:
        copy.wait_recv()
    own_picks.wait()
    to_smem = pltpu.make_async_copy(ch_all, ch_smem, load_sem.at[13])
    to_smem.start()

    def from_row(every, own, send, recv, r):
        from_y = near(r)
        remote(
            own.at[0], every.at[chunk(z, from_y)], send.at[0], recv.at[from_y],
            z * NY + from_y, t,
        ).wait_recv()

    for r in (1, 2, 3):
        from_row(k_all, k_own, ky_send, ky_recv, r)
        begin(k_ring, r)
    for copy in mine:
        copy.wait()
    for c in range(2):
        k_ring[2](0, c).start()
    for s in range(1, NZ // 2):
        for c in range(2):
            step(k_ring, s, c)
    begin(v_ring, 0)
    for r in (1, 2, 3):
        from_row(v_all, v_own, vy_send, vy_recv, r)
        begin(v_ring, r)
    for c in range(2):
        v_ring[2](0, c).start()
    for c in range(2):
        step(k_ring, NZ // 2, c)

    to_smem.wait()
    own_q.wait()
    for k in range(1, NY):
        queries[k].wait_recv()
    for rel in range(NZ):
        for c in range(2):
            k_ring[2](rel, c).wait_recv()

    key_pos = lax.broadcasted_iota(jnp.int32, (BLK, 4 * BLK), 0)
    query_pos = lax.rem(lax.broadcasted_iota(jnp.int32, (BLK, 4 * BLK), 1), BLK)
    causal = key_pos <= query_pos
    half_blk = BLK // 2

    def own_place(k, jb):
        return z * 32 + t * 16 + row_chip(k) * 4 + jb

    def gather_keys(k, jb, u):
        bias = []
        for j in range(PICK + 1):
            if j < PICK:
                pick = ch_smem[k, t * 4 + jb, j]
                bias.append(jnp.where(pick < 0, NEGATIVE, 0.0).astype(F32))
                block = k_all[place_of(jnp.maximum(pick, 0))]
            else:
                block = k_all[own_place(k, jb)]
            nothing = jnp.zeros_like(block)
            kg[u, j * BLK : j * BLK + half_blk, :] = jnp.where(left_half, block, nothing)
            kg[u, j * BLK + half_blk : j * BLK + BLK, :] = jnp.where(left_half, nothing, block)
        return bias

    def score(k, jb, u):
        rows = pl.ds(pl.multiple_of(jb * BLK, BLK), BLK)
        heads = []
        for n in range(2):
            x = q_all[k, rows, n * 128 : n * 128 + 128].astype(F32)
            swapped = pltpu.roll(x, 64, 1)
            heads += [jnp.where(left, x, swapped), jnp.where(left, swapped, x)]
        q2 = jnp.concatenate(heads, axis=0).astype(BF)
        scores[u] = lax.dot_general(
            kg[u], q2, (((1,), (1,)), ((), ())), preferred_element_type=F32
        )

    def softmax(k, jb, u, bias):
        def rows_of(j):
            return scores[u, j * BLK : j * BLK + BLK, :]

        def eight(x, op):
            return op(x.reshape(BLK // 8, 8, 4 * BLK), axis=0)

        tail = jnp.where(causal, rows_of(PICK), NEGATIVE)
        top = eight(tail, jnp.max)
        for j in range(PICK):
            top = jnp.maximum(top, eight(rows_of(j), jnp.max) + bias[j])
        top = jnp.max(top, axis=0, keepdims=True)
        total = jnp.zeros((8, 4 * BLK), F32)
        for j in range(PICK + 1):
            s = tail if j == PICK else rows_of(j)
            shift = top if j == PICK else top - bias[j]
            p = jnp.exp2((s - shift) * EXPONENT)
            total = total + eight(p, jnp.sum)
            probs[k * 4 + jb, j * BLK : j * BLK + BLK, :] = p.astype(BF)
        total = jnp.sum(total, axis=0, keepdims=True)
        inverse[k, pl.ds(jb, 1), :] = 1.0 / total
        ls_out[k, pl.ds(jb, 1), :] = top * HEAD_DIM**-0.5 + jnp.log(total)

    def weigh(k, pair):
        blocks = [(k, 2 * pair + u, u) for u in range(2)]
        bias = [gather_keys(*block) for block in blocks]
        for block in blocks:
            score(*block)
        for block in blocks:
            softmax(*block, bias[block[2]])

    def gather_values(k, jb):
        previous = None
        for j in range(PICK + 1):
            if j < PICK:
                block = v_all[place_of(jnp.maximum(ch_smem[k, t * 4 + jb, j], 0))]
            else:
                block = v_all[own_place(k, jb)]
            block = block.astype(F32)
            if j % 2 == 1:
                low = jnp.where(left_half, previous, pltpu.roll(block, 64, 1))
                high = jnp.where(left_half, pltpu.roll(previous, 64, 1), block)
                columns = slice((j // 2) * 128, (j // 2) * 128 + 128)
                vt[jb, :half_blk, columns] = low.astype(BF)
                vt[jb, half_blk:, columns] = high.astype(BF)
            previous = block

    def combine(k):
        for jb in range(4):
            gather_values(k, jb)
        mixed = [
            jnp.dot(vt[jb], probs[k * 4 + jb], preferred_element_type=F32) for jb in range(4)
        ]
        for jb in range(4):
            turned_back = (mixed[jb] * inverse[k, jb : jb + 1, :]).T
            parts = [turned_back[h * BLK : h * BLK + BLK] for h in range(4)]
            att_out[k, jb * BLK : jb * BLK + BLK, :] = jnp.concatenate(parts, axis=1).astype(BF)

    to_self = y // 2 == t
    slot = (lax.rem(y, 2), t)

    def log_piece(k):
        return remote(
            ls_out.at[k], ls_ref.at[slot], l_send.at[k], l_recv.at[slot], row_peer(k), y // 2
        )

    for s, k in enumerate((2, 1, 3, 0)):
        @pl.loop(0, 2)
        def _(pair):
            weigh(k, pair)
            step(v_ring, s + 1, pair)

        if k > 0:
            log_piece(k).start()
        else:
            pl.when(jnp.logical_not(to_self))(lambda: log_piece(0).start())

            @pl.when(to_self)
            def _():
                ls_ref[slot] = ls_out[0]

    for rel in range(NZ):
        for c in range(2):
            v_ring[2](rel, c).wait_recv()

    back = {}
    for k in (2, 1, 3, 0):
        combine(k)
        if k > 0:
            back[NY - k] = remote(
                att_out.at[k], att_all.at[NY - k], a_send.at[k], a_recv.at[NY - k],
                row_peer(k), t,
            )
            back[NY - k].start()

    loads[4].wait()
    halves[3].wait_recv()
    for k in (0, 1, 3, 2):
        if k > 0:
            back[k].wait_recv()
        ys = row_chip(k)
        weights = wo[ys // 2, pl.ds(pl.multiple_of(lax.rem(ys, 2) * 256, 256), 256), :]
        piece = att_out[0] if k == 0 else att_all[k]
        part = jnp.dot(piece, weights, preferred_element_type=F32)
        if k == 0:
            acc[...] = part
        elif k != 2:
            acc[...] += part
        else:
            projected = acc[...] + part
            square = jnp.mean(projected * projected, axis=-1, keepdims=True)
            out_ref[...] = (projected * lax.rsqrt(square + EPSILON)).astype(BF)

    for ys in range(2):
        for tt in range(2):
            @pl.when(jnp.logical_not((t * 2 + ys == y) & (t == tt)))
            def _():
                remote(
                    ls_out.at[0], ls_ref.at[ys, tt], l_send.at[0], l_recv.at[ys, tt], kv, other
                ).wait_recv()
    for k in range(1, NY):
        log_piece(k).wait_send()
    pl.when(jnp.logical_not(to_self))(lambda: log_piece(0).wait_send())
    for k in range(1, NY):
        key_to_owner(row_chip(k)).wait_send()
        value_to_owner(row_chip(k)).wait_send()
        queries[k].wait_send()
        back[k].wait_send()
    for copy in halves + picks:
        copy.wait_send()
    for up, down, partner in (k_ring, v_ring):
        for r in range(NY):
            up(0, r).wait_send()
            down(0, r).wait_send()
        for c in range(2):
            for s in range(1, NZ // 2):
                if s < NZ // 2 - 1 or c == 0:
                    up(s, c).wait_send()
                if s < NZ // 2 - 1 or c == 1:
                    down(s, c).wait_send()
            for rel in range(NZ):
                partner(rel, c).wait_send()


def shards(tokens, w_query, w_key, w_value, w_out, chosen):
    rows, width = tokens.shape[1:]
    tables = rotary_tables(rows, 2 * NY * NZ)
    any_space = pl.BlockSpec(memory_space=pl.ANY)
    vmem = pl.BlockSpec(memory_space=pltpu.VMEM)
    dma = pltpu.SemaphoreType.DMA
    out, logs = pl.pallas_call(
        kernel,
        out_shape=(
            jax.ShapeDtypeStruct((rows, width), BF),
            jax.ShapeDtypeStruct((2, 2, 4, 4 * BLK), F32),
        ),
        in_specs=[any_space] * 10,
        out_specs=(vmem, vmem),
        scratch_shapes=[
            pltpu.VMEM((rows, 128), F32),
            pltpu.VMEM((rows, 128), F32),
            pltpu.VMEM((2 * NY * NZ, 128), F32),
            pltpu.VMEM((2 * NY * NZ, 128), F32),
            pltpu.VMEM((rows, width), BF),
            pltpu.VMEM((2,) + w_query.shape, BF),
            pltpu.VMEM((2,) + w_key.shape, BF),
            pltpu.VMEM((2,) + w_value.shape, BF),
            pltpu.VMEM((2,) + w_out.shape, BF),
            pltpu.VMEM((rows, 128), F32),
            pltpu.VMEM((rows, 128), F32),
            pltpu.VMEM((4, 4, BLK // 2, 128), BF),
            pltpu.VMEM((4, 4, BLK // 2, 128), BF),
            pltpu.VMEM((NZ * NY * 8, BLK // 2, 128), BF),
            pltpu.VMEM((NZ * NY * 8, BLK // 2, 128), BF),
            pltpu.VMEM((NY, rows, 256), BF),
            pltpu.VMEM((NY, rows, 256), BF),
            pltpu.VMEM((NY, 8, PICK), jnp.int32),
            pltpu.SMEM((NY, 8, PICK), jnp.int32),
            pltpu.VMEM((2, (PICK + 1) * BLK, 128), BF),
            pltpu.VMEM((4, BLK, (PICK + 1) * BLK), BF),
            pltpu.VMEM((2, (PICK + 1) * BLK, 4 * BLK), F32),
            pltpu.VMEM((NY * 4, (PICK + 1) * BLK, 4 * BLK), BF),
            pltpu.VMEM((NY, 4, 4 * BLK), F32),
            pltpu.VMEM((NY, rows, 256), BF),
            pltpu.VMEM((NY, rows, 256), BF),
            pltpu.VMEM((NY, 4, 4 * BLK), F32),
            pltpu.VMEM((rows, width), F32),
            dma((14,)), dma((4,)), dma((4,)), dma((4,)), dma((4,)), dma((4,)), dma((4,)),
            dma((2, 4)), dma((2, 4)), dma((4, 2)), dma((4, 2)), dma((4, 2)), dma((4, 2)),
            dma((NZ, 2)), dma((NZ, 2)),
            dma((2, 4)), dma((2, 4)), dma((4, 2)), dma((4, 2)), dma((4, 2)), dma((4, 2)),
            dma((NZ, 2)), dma((NZ, 2)),
            dma((4,)), dma((4,)), dma((4,)), dma((4,)),
            dma((4,)), dma((4,)), dma((4,)), dma((2, 2)),
        ],
        compiler_params=pltpu.CompilerParams(
            collective_id=0, has_side_effects=True, vmem_limit_bytes=67_000_000
        ),
    )(*tables, tokens[0], w_query, w_key, w_value, w_out, chosen[0])
    logs = logs.reshape(2, 2, 4, 4, BLK).transpose(1, 2, 4, 0, 3).reshape(2 * rows, 8)
    return out[None], logs[None]


def solution(mesh):
    placed = (
        P("dp", ("kv", "tp"), None),
        P(None, "tp"),
        P(None, "tp"),
        P(None, "tp"),
        P("tp", None),
        P("dp", "kv", None),
    )
    return jax.shard_map(
        shards,
        mesh=mesh,
        in_specs=placed,
        out_specs=(P("dp", ("kv", "tp"), None), P("dp", "kv", "tp")),
        check_vma=False,
    )
```

```python
import math

import jax
import jax.numpy as jnp
import numpy as np
from jax import lax
from jax.experimental import pallas as pl
from jax.experimental.pallas import tpu as pltpu
from jax.sharding import PartitionSpec as P

HEAD_DIM = 64
BLK = 64
PICK = 15
THETA_BASE = 10000.0
NEGATIVE = -1e30
EPSILON = 1e-06
MESH = pl.DeviceIdType.MESH
BF = jnp.bfloat16
F32 = jnp.float32
EXPONENT = math.log2(math.e) / math.sqrt(HEAD_DIM)
NY = 4
NZ = 8


def rotary_tables(rows, bases):
    half = HEAD_DIM // 2
    freq = THETA_BASE ** (-np.arange(half, dtype=np.float64) / half)
    freq = np.tile(freq, 128 // half)[None, :]
    offset = np.arange(rows, dtype=np.float64)[:, None] * freq
    base = np.arange(bases, dtype=np.float64)[:, None] * rows * freq
    return [
        np.asarray(a, np.float32)
        for a in (np.cos(offset), np.sin(offset), np.cos(base), np.sin(base))
    ]


def kernel(
    cr_hbm, sr_hbm, cb_hbm, sb_hbm, tok_hbm, wq_hbm, wk_hbm, wv_hbm, wo_hbm, ch_hbm,
    out_ref, ls_ref,
    cr_ref, sr_ref, cb_ref, sb_ref, tok, wq, wk, wv, wo, cosine, sine, k_own, v_own,
    k_all, v_all, qs, q_all, ch_all, ch_smem, kg, vt, scores, probs, inverse,
    att_out, att_all, ls_out, acc,
    load_sem, w_send, w_recv, ky_send, ky_recv, vy_send, vy_recv,
    k_up_send, k_up_recv, k_dn_send, k_dn_recv, k_pt_send, k_pt_recv,
    v_up_send, v_up_recv, v_dn_send, v_dn_recv, v_pt_send, v_pt_recv,
    q_send, q_recv, c_send, c_recv, a_send, a_recv, l_send, l_recv,
):
    kv = lax.axis_index("kv")
    t = lax.axis_index("tp")
    z, y = kv // NY, kv % NY
    other = 1 - t

    def row_chip(k):
        return lax.rem(y + k, NY)

    def row_peer(k):
        return z * NY + row_chip(k)

    def chunk(zz, yy):
        return pl.ds(((zz * NY + yy) * 2 + t) * 4, 4)

    def remote(src, dst, send, recv, kv_to, tp_to):
        return pltpu.make_async_remote_copy(
            src_ref=src, dst_ref=dst, send_sem=send, recv_sem=recv,
            device_id={"kv": kv_to, "tp": tp_to}, device_id_type=MESH,
        )

    loads = [
        pltpu.make_async_copy(tok_hbm, tok, load_sem.at[0]),
        pltpu.make_async_copy(wk_hbm, wk.at[t], load_sem.at[1]),
        pltpu.make_async_copy(wv_hbm, wv.at[t], load_sem.at[2]),
        pltpu.make_async_copy(wq_hbm, wq.at[t], load_sem.at[3]),
        pltpu.make_async_copy(wo_hbm, wo.at[t], load_sem.at[4]),
    ]
    tables = [
        pltpu.make_async_copy(a, b, load_sem.at[8 + i])
        for i, (a, b) in enumerate(
            ((cr_hbm, cr_ref), (sr_hbm, sr_ref), (cb_hbm, cb_ref), (sb_hbm, sb_ref))
        )
    ]
    own_picks = pltpu.make_async_copy(ch_hbm, ch_all.at[0], load_sem.at[12])
    for load in loads[:3] + tables + loads[3:] + [own_picks]:
        load.start()

    barrier = pltpu.get_barrier_semaphore()
    peers = [(row_peer(k), tt) for k in range(1, NY) for tt in (t, other)]
    peers += [(kv, other)]
    z_up = lax.rem(z + 1, NZ) * NY + y
    z_dn = lax.rem(z + NZ - 1, NZ) * NY + y
    peers += [(z_up, t), (z_dn, t)]
    for kv_to, tp_to in peers:
        pl.semaphore_signal(
            barrier, inc=1, device_id={"kv": kv_to, "tp": tp_to}, device_id_type=MESH
        )

    left = lax.broadcasted_iota(jnp.int32, (BLK, 128), 1) < BLK
    left_half = lax.broadcasted_iota(jnp.int32, (BLK // 2, 128), 1) < BLK
    wide = lax.broadcasted_iota(jnp.int32, (4 * BLK, 128), 1)
    first = lax.rem(wide, HEAD_DIM) < HEAD_DIM // 2

    for load in tables:
        load.wait()
    base = kv * 2 + t
    cb, sb = cb_ref[pl.ds(base, 1), :], sb_ref[pl.ds(base, 1), :]
    cr, sr = cr_ref[...], sr_ref[...]
    cosine[...] = cb * cr - sb * sr
    turned = sb * cr + cb * sr
    sine[...] = jnp.where(first, -turned, turned)

    def rotate(x):
        swapped = jnp.where(first, pltpu.roll(x, 96, 1), pltpu.roll(x, 32, 1))
        return x * cosine[...] + swapped * sine[...]

    def project_kv(half):
        tokens = tok[...]
        keys = jnp.dot(tokens, wk[half], preferred_element_type=F32).astype(BF).astype(F32)
        keys = rotate(keys)
        keys = (keys, pltpu.roll(keys, 64, 1))
        values = jnp.dot(tokens, wv[half], preferred_element_type=F32).T
        values = [values[:, i * 128 : i * 128 + 128] for i in range(2)]
        values = [(x, pltpu.roll(x, 64, 1)) for x in values]
        for e in range(2):
            for j in range(4):
                low = keys[e][j * 64 : j * 64 + 32]
                high = keys[1 - e][j * 64 + 32 : j * 64 + 64]
                k_own[2 * half + e, j] = jnp.where(left_half, low, high).astype(BF)
                pair = values[j // 2]
                low = pair[j % 2][e * 64 : e * 64 + 32]
                high = pair[1 - j % 2][e * 64 + 32 : e * 64 + 64]
                v_own[2 * half + e, j] = jnp.where(left_half, low, high).astype(BF)

    def project_q(half):
        tokens = tok[...]
        full = jnp.dot(tokens, wq[half], preferred_element_type=F32)
        for n in range(4):
            x = full[:, n * 128 : n * 128 + 128].astype(BF).astype(F32)
            qs[2 * half + n // 2, :, (n % 2) * 128 : (n % 2) * 128 + 128] = rotate(x).astype(BF)

    for load in loads[:3]:
        load.wait()
    project_kv(t)

    pl.semaphore_wait(barrier, len(peers))

    halves = [
        remote(wk.at[t], wk.at[t], w_send.at[0], w_recv.at[0], kv, other),
        remote(wv.at[t], wv.at[t], w_send.at[1], w_recv.at[1], kv, other),
        remote(wq_hbm, wq.at[t], w_send.at[2], w_recv.at[2], kv, other),
        remote(wo_hbm, wo.at[t], w_send.at[3], w_recv.at[3], kv, other),
    ]

    def to_owner(own, every, send, recv, head):
        return remote(
            own.at[head], every.at[chunk(z, y)], send.at[head], recv.at[y], z * NY + head, t
        )

    def key_to_owner(head):
        return to_owner(k_own, k_all, ky_send, ky_recv, head)

    def value_to_owner(head):
        return to_owner(v_own, v_all, vy_send, vy_recv, head)

    def send_heads(half):
        for make in (key_to_owner, value_to_owner):
            for e in range(2):
                head = 2 * half + e

                @pl.when(head != y)
                def _():
                    make(head).start()

    for copy in halves[:2]:
        copy.start()
    send_heads(t)
    picks = [
        remote(ch_hbm, ch_all.at[NY - k], c_send.at[k], c_recv.at[NY - k], row_peer(k), t)
        for k in range(1, NY)
    ]
    for copy in halves[2:] + picks:
        copy.start()

    loads[3].wait()
    project_q(t)
    for copy in halves[:2]:
        copy.wait_recv()
    project_kv(other)
    send_heads(other)

    def ring(every, up_send, up_recv, dn_send, dn_recv, pt_send, pt_recv):
        def place(zz, k):
            return every.at[chunk(zz, row_chip(k))]

        def up(s, k, src=None):
            spot = place(lax.rem(z + NZ - s, NZ), k)
            src = spot if src is None else src
            return remote(src, spot, up_send.at[s, k], up_recv.at[s, k], z_up, t)

        def down(s, k, src=None):
            spot = place(lax.rem(z + s, NZ), k)
            src = spot if src is None else src
            return remote(src, spot, dn_send.at[s, k], dn_recv.at[s, k], z_dn, t)

        def partner(rel, k, src=None):
            spot = place(lax.rem(z + rel, NZ), k)
            src = spot if src is None else src
            return remote(src, spot, pt_send.at[rel, k], pt_recv.at[rel, k], kv, other)

        return up, down, partner

    k_ring = ring(k_all, k_up_send, k_up_recv, k_dn_send, k_dn_recv, k_pt_send, k_pt_recv)
    v_ring = ring(v_all, v_up_send, v_up_recv, v_dn_send, v_dn_recv, v_pt_send, v_pt_recv)

    def begin(group, k, src=None):
        up, down, partner = group
        up(0, k, src).start()
        down(0, k, src).start()
        partner(0, k, src).start()

    def step(group, s, k):
        up, down, partner = group
        if s < NZ // 2:
            turn = s == NZ // 2 - 1
            up(s - 1, k).wait_recv()
            if not turn:
                up(s, k).start()
            else:
                pl.when(k < 2)(lambda: up(s, k).start())
            partner(NZ - s, k).start()
            down(s - 1, k).wait_recv()
            if not turn:
                down(s, k).start()
            else:
                pl.when(k >= 2)(lambda: down(s, k).start())
            partner(s, k).start()
        else:
            pl.when(k < 2)(lambda: up(s - 1, k).wait_recv())
            pl.when(k >= 2)(lambda: down(s - 1, k).wait_recv())
            partner(s, k).start()

    mine = [
        pltpu.make_async_copy(k_own.at[y], k_all.at[chunk(z, y)], load_sem.at[5]),
        pltpu.make_async_copy(v_own.at[y], v_all.at[chunk(z, y)], load_sem.at[7]),
    ]
    begin(k_ring, 0, k_own.at[y])
    for copy in mine:
        copy.start()

    halves[2].wait_recv()
    project_q(other)
    own_q = pltpu.make_async_copy(qs.at[y], q_all.at[0], load_sem.at[6])
    own_q.start()
    queries = [None] * NY
    for k in (2, 1, 3):
        queries[NY - k] = remote(
            qs.at[row_chip(k)], q_all.at[NY - k], q_send.at[k], q_recv.at[NY - k],
            row_peer(k), t,
        )
        queries[NY - k].start()

    def from_row(every, own, send, recv, k):
        remote(
            own.at[0], every.at[chunk(z, row_chip(k))], send.at[0], recv.at[row_chip(k)],
            row_peer(k), t,
        ).wait_recv()

    for copy in picks:
        copy.wait_recv()
    own_picks.wait()
    to_smem = pltpu.make_async_copy(ch_all, ch_smem, load_sem.at[13])
    to_smem.start()
    for k in (1, 3, 2):
        from_row(k_all, k_own, ky_send, ky_recv, k)
        begin(k_ring, k)
    for copy in mine:
        copy.wait()
    begin(v_ring, 0)
    for k in (1, 3, 2):
        from_row(v_all, v_own, vy_send, vy_recv, k)
        begin(v_ring, k)
    order = (0, 1, 3, 2)
    for s in range(1, NZ // 2 + 1):
        for k in order:
            step(k_ring, s, k)
        if s > 1 and s <= NZ // 2 - 1:
            for k in order:
                step(v_ring, s - 1, k)

    to_smem.wait()
    own_q.wait()
    for k in range(1, NY):
        queries[k].wait_recv()
    for rel in range(NZ):
        for k in range(NY):
            k_ring[2](rel, k).wait_recv()

    key_pos = lax.broadcasted_iota(jnp.int32, (BLK, 4 * BLK), 0)
    query_pos = lax.rem(lax.broadcasted_iota(jnp.int32, (BLK, 4 * BLK), 1), BLK)
    causal = key_pos <= query_pos
    half_blk = BLK // 2

    def own_block(k, jb):
        return (z * NY + row_chip(k)) * 8 + t * 4 + jb

    def gather_keys(k, jb):
        bias = []
        for j in range(PICK + 1):
            if j < PICK:
                pick = ch_smem[k, t * 4 + jb, j]
                bias.append(jnp.where(pick < 0, NEGATIVE, 0.0).astype(F32))
                block = k_all[jnp.maximum(pick, 0)]
            else:
                block = k_all[own_block(k, jb)]
            nothing = jnp.zeros_like(block)
            u, row = jb % 2, j * BLK
            kg[u, row : row + half_blk, :] = jnp.where(left_half, block, nothing)
            kg[u, row + half_blk : row + BLK, :] = jnp.where(left_half, nothing, block)
        return bias

    def load_queries(k, jb):
        heads = []
        for n in range(2):
            x = q_all[k, jb * BLK : jb * BLK + BLK, n * 128 : n * 128 + 128].astype(F32)
            swapped = pltpu.roll(x, 64, 1)
            heads += [jnp.where(left, x, swapped), jnp.where(left, swapped, x)]
        return jnp.concatenate(heads, axis=0).astype(BF)

    def eight(x, op):
        return op(x.reshape(BLK // 8, 8, 4 * BLK), axis=0)

    def score(u, half, q2, bias):
        span = 8 * BLK
        part = lax.dot_general(
            kg[u, half * span : half * span + span, :], q2, (((1,), (1,)), ((), ())),
            preferred_element_type=F32,
        )
        top = None
        for i in range(8):
            j = half * 8 + i
            block = part[i * BLK : i * BLK + BLK, :]
            if j == PICK:
                block = jnp.where(causal, block, NEGATIVE)
            scores[u, j * BLK : j * BLK + BLK, :] = block
            here = eight(block, jnp.max)
            here = here if j == PICK else here + bias[j]
            top = here if top is None else jnp.maximum(top, here)
        return top

    def softmax(state, half):
        k, jb, top, bias, total = state
        for j in range(half * 8, half * 8 + 8):
            shift = top if j == PICK else top - bias[j]
            p = jnp.exp2((scores[jb % 2, j * BLK : j * BLK + BLK, :] - shift) * EXPONENT)
            part = eight(p, jnp.sum)
            total = part if total is None else total + part
            probs[jb, j * BLK : j * BLK + BLK, :] = p.astype(BF)
        if half == 1:
            total = jnp.sum(total, axis=0, keepdims=True)
            inverse[k, pl.ds(jb, 1), :] = 1.0 / total
            ls_out[k, pl.ds(jb, 1), :] = top * HEAD_DIM**-0.5 + jnp.log(total)
        return k, jb, top, bias, total

    def weigh(k):
        state = None
        for jb in range(4):
            bias = gather_keys(k, jb)
            q2 = load_queries(k, jb)
            tops = []
            for half in range(2):
                tops.append(score(jb % 2, half, q2, bias))
                if state is not None:
                    state = softmax(state, half)
            top = jnp.max(jnp.maximum(*tops), axis=0, keepdims=True)
            state = (k, jb, top, bias, None)
        for half in range(2):
            state = softmax(state, half)

    def gather_values(k, jb):
        previous = None
        for j in range(PICK + 1):
            if j < PICK:
                block = v_all[jnp.maximum(ch_smem[k, t * 4 + jb, j], 0)]
            else:
                block = v_all[own_block(k, jb)]
            block = block.astype(F32)
            if j % 2 == 1:
                low = jnp.where(left_half, previous, pltpu.roll(block, 64, 1))
                high = jnp.where(left_half, pltpu.roll(previous, 64, 1), block)
                columns = slice((j // 2) * 128, (j // 2) * 128 + 128)
                vt[jb, :half_blk, columns] = low.astype(BF)
                vt[jb, half_blk:, columns] = high.astype(BF)
            previous = block

    def combine(k):
        for jb in range(4):
            gather_values(k, jb)
        mixed = [
            jnp.dot(vt[jb], probs[jb], preferred_element_type=F32) for jb in range(4)
        ]
        for jb in range(4):
            turned_back = (mixed[jb] * inverse[k, pl.ds(jb, 1), :]).T
            parts = [turned_back[h * BLK : h * BLK + BLK] for h in range(4)]
            att_out[k, jb * BLK : jb * BLK + BLK, :] = jnp.concatenate(parts, axis=1).astype(BF)

    to_self = y // 2 == t
    slot = (lax.rem(y, 2), t)

    def log_piece(k):
        return remote(
            ls_out.at[k], ls_ref.at[slot], l_send.at[k], l_recv.at[slot], row_peer(k), y // 2
        )

    def give_back(k):
        return remote(
            att_out.at[k], att_all.at[NY - k], a_send.at[k], a_recv.at[NY - k], row_peer(k), t
        )

    @pl.loop(0, NY)
    def _(i):
        k = lax.rem(i + 1, NY)
        weigh(k)

        @pl.when(i == 0)
        def _():
            for s in (NZ // 2 - 1, NZ // 2):
                for r in order:
                    step(v_ring, s, r)
            for rel in range(NZ):
                for r in range(NY):
                    v_ring[2](rel, r).wait_recv()

        combine(k)

        @pl.when(k > 0)
        def _():
            give_back(k).start()
            log_piece(k).start()

    pl.when(jnp.logical_not(to_self))(lambda: log_piece(0).start())

    @pl.when(to_self)
    def _():
        ls_ref[slot] = ls_out[0]

    loads[4].wait()
    halves[3].wait_recv()
    for k in (0, 1, 3, 2):
        if k > 0:
            give_back(NY - k).wait_recv()
        ys = row_chip(k)
        weights = wo[ys // 2, pl.ds(pl.multiple_of(lax.rem(ys, 2) * 256, 256), 256), :]
        piece = att_out[0] if k == 0 else att_all[k]
        part = jnp.dot(piece, weights, preferred_element_type=F32)
        if k == 0:
            acc[...] = part
        elif k != 2:
            acc[...] += part
        else:
            projected = acc[...] + part
            square = jnp.mean(projected * projected, axis=-1, keepdims=True)
            out_ref[...] = (projected * lax.rsqrt(square + EPSILON)).astype(BF)

    for ys in range(2):
        for tt in range(2):
            @pl.when(jnp.logical_not((t * 2 + ys == y) & (t == tt)))
            def _():
                remote(
                    ls_out.at[0], ls_ref.at[ys, tt], l_send.at[0], l_recv.at[ys, tt], kv, other
                ).wait_recv()
    for k in range(1, NY):
        log_piece(k).wait_send()
    pl.when(jnp.logical_not(to_self))(lambda: log_piece(0).wait_send())
    for k in range(1, NY):
        key_to_owner(row_chip(k)).wait_send()
        value_to_owner(row_chip(k)).wait_send()
        queries[k].wait_send()
        give_back(k).wait_send()
    for copy in halves + picks:
        copy.wait_send()
    for up, down, partner in (k_ring, v_ring):
        for k in range(NY):
            for s in range(NZ // 2):
                if s < NZ // 2 - 1 or k < 2:
                    up(s, k).wait_send()
                if s < NZ // 2 - 1 or k >= 2:
                    down(s, k).wait_send()
            for rel in range(NZ):
                partner(rel, k).wait_send()


def shards(tokens, w_query, w_key, w_value, w_out, chosen):
    rows, width = tokens.shape[1:]
    tables = rotary_tables(rows, 2 * NY * NZ)
    any_space = pl.BlockSpec(memory_space=pl.ANY)
    vmem = pl.BlockSpec(memory_space=pltpu.VMEM)
    dma = pltpu.SemaphoreType.DMA
    out, logs = pl.pallas_call(
        kernel,
        out_shape=(
            jax.ShapeDtypeStruct((rows, width), BF),
            jax.ShapeDtypeStruct((2, 2, 4, 4 * BLK), F32),
        ),
        in_specs=[any_space] * 10,
        out_specs=(vmem, vmem),
        scratch_shapes=[
            pltpu.VMEM((rows, 128), F32),
            pltpu.VMEM((rows, 128), F32),
            pltpu.VMEM((2 * NY * NZ, 128), F32),
            pltpu.VMEM((2 * NY * NZ, 128), F32),
            pltpu.VMEM((rows, width), BF),
            pltpu.VMEM((2,) + w_query.shape, BF),
            pltpu.VMEM((2,) + w_key.shape, BF),
            pltpu.VMEM((2,) + w_value.shape, BF),
            pltpu.VMEM((2,) + w_out.shape, BF),
            pltpu.VMEM((rows, 128), F32),
            pltpu.VMEM((rows, 128), F32),
            pltpu.VMEM((4, 4, BLK // 2, 128), BF),
            pltpu.VMEM((4, 4, BLK // 2, 128), BF),
            pltpu.VMEM((NZ * NY * 8, BLK // 2, 128), BF),
            pltpu.VMEM((NZ * NY * 8, BLK // 2, 128), BF),
            pltpu.VMEM((NY, rows, 256), BF),
            pltpu.VMEM((NY, rows, 256), BF),
            pltpu.VMEM((NY, 8, PICK), jnp.int32),
            pltpu.SMEM((NY, 8, PICK), jnp.int32),
            pltpu.VMEM((2, (PICK + 1) * BLK, 128), BF),
            pltpu.VMEM((4, BLK, (PICK + 1) * BLK), BF),
            pltpu.VMEM((2, (PICK + 1) * BLK, 4 * BLK), F32),
            pltpu.VMEM((4, (PICK + 1) * BLK, 4 * BLK), BF),
            pltpu.VMEM((NY, 4, 4 * BLK), F32),
            pltpu.VMEM((NY, rows, 256), BF),
            pltpu.VMEM((NY, rows, 256), BF),
            pltpu.VMEM((NY, 4, 4 * BLK), F32),
            pltpu.VMEM((rows, width), F32),
            dma((14,)), dma((4,)), dma((4,)), dma((4,)), dma((4,)), dma((4,)), dma((4,)),
            dma((4, 4)), dma((4, 4)), dma((4, 4)), dma((4, 4)), dma((NZ, 4)), dma((NZ, 4)),
            dma((4, 4)), dma((4, 4)), dma((4, 4)), dma((4, 4)), dma((NZ, 4)), dma((NZ, 4)),
            dma((4,)), dma((4,)), dma((4,)), dma((4,)),
            dma((4,)), dma((4,)), dma((4,)), dma((2, 2)),
        ],
        compiler_params=pltpu.CompilerParams(
            collective_id=0, has_side_effects=True, vmem_limit_bytes=67_000_000
        ),
    )(*tables, tokens[0], w_query, w_key, w_value, w_out, chosen[0])
    logs = logs.reshape(2, 2, 4, 4, BLK).transpose(1, 2, 4, 0, 3).reshape(2 * rows, 8)
    return out[None], logs[None]


def solution(mesh):
    placed = (
        P("dp", ("kv", "tp"), None),
        P(None, "tp"),
        P(None, "tp"),
        P(None, "tp"),
        P("tp", None),
        P("dp", "kv", None),
    )
    return jax.shard_map(
        shards,
        mesh=mesh,
        in_specs=placed,
        out_specs=(P("dp", ("kv", "tp"), None), P("dp", "kv", "tp")),
        check_vma=False,
    )
```

```python
import math

import jax
import jax.numpy as jnp
import numpy as np
from jax import lax
from jax.experimental import pallas as pl
from jax.experimental.pallas import tpu as pltpu
from jax.sharding import PartitionSpec as P

HEAD_DIM = 64
BLK = 64
PICK = 15
THETA_BASE = 10000.0
NEGATIVE = -1e30
EPSILON = 1e-06
MESH = pl.DeviceIdType.MESH
BF = jnp.bfloat16
F32 = jnp.float32
EXPONENT = math.log2(math.e) / math.sqrt(HEAD_DIM)
NY = 4
NZ = 8


def rotary_tables(rows, bases):
    half = HEAD_DIM // 2
    freq = THETA_BASE ** (-np.arange(half, dtype=np.float64) / half)
    freq = np.tile(freq, 128 // half)[None, :]
    offset = np.arange(rows, dtype=np.float64)[:, None] * freq
    base = np.arange(bases, dtype=np.float64)[:, None] * rows * freq
    return [
        np.asarray(a, np.float32)
        for a in (np.cos(offset), np.sin(offset), np.cos(base), np.sin(base))
    ]


def kernel(
    cr_hbm, sr_hbm, cb_hbm, sb_hbm, tok_hbm, wq_hbm, wk_hbm, wv_hbm, wo_hbm, ch_hbm,
    out_ref, ls_ref,
    cr_ref, sr_ref, cb_ref, sb_ref, tok, wq, wk, wv, wo, cosine, sine, k_own, v_own,
    k_all, v_all, qs, q_all, ch_all, ch_smem, kg, vt, scores, probs, inverse,
    att_out, att_all, ls_out, ls_all, acc,
    load_sem, w_send, w_recv, ky_send, ky_recv, vy_send, vy_recv,
    k_up_send, k_up_recv, k_dn_send, k_dn_recv, k_pt_send, k_pt_recv,
    v_up_send, v_up_recv, v_dn_send, v_dn_recv, v_pt_send, v_pt_recv,
    q_send, q_recv, c_send, c_recv, a_send, a_recv, l_send, l_recv,
):
    kv = lax.axis_index("kv")
    t = lax.axis_index("tp")
    z, y = kv // NY, kv % NY
    other = 1 - t

    def row_chip(k):
        return lax.rem(y + k, NY)

    def row_peer(k):
        return z * NY + row_chip(k)

    def chunk(zz, yy):
        return pl.ds(((zz * NY + yy) * 2 + t) * 4, 4)

    def remote(src, dst, send, recv, kv_to, tp_to):
        return pltpu.make_async_remote_copy(
            src_ref=src, dst_ref=dst, send_sem=send, recv_sem=recv,
            device_id={"kv": kv_to, "tp": tp_to}, device_id_type=MESH,
        )

    loads = [
        pltpu.make_async_copy(tok_hbm, tok, load_sem.at[0]),
        pltpu.make_async_copy(wk_hbm, wk.at[t], load_sem.at[1]),
        pltpu.make_async_copy(wv_hbm, wv.at[t], load_sem.at[2]),
        pltpu.make_async_copy(wq_hbm, wq.at[t], load_sem.at[3]),
        pltpu.make_async_copy(wo_hbm, wo.at[t], load_sem.at[4]),
    ]
    tables = [
        pltpu.make_async_copy(a, b, load_sem.at[8 + i])
        for i, (a, b) in enumerate(
            ((cr_hbm, cr_ref), (sr_hbm, sr_ref), (cb_hbm, cb_ref), (sb_hbm, sb_ref))
        )
    ]
    own_picks = pltpu.make_async_copy(ch_hbm, ch_all.at[0], load_sem.at[12])
    for load in loads[:3] + tables + loads[3:] + [own_picks]:
        load.start()

    barrier = pltpu.get_barrier_semaphore()
    peers = [(row_peer(k), tt) for k in range(1, NY) for tt in (t, other)]
    peers += [(kv, other)]
    z_up = lax.rem(z + 1, NZ) * NY + y
    z_dn = lax.rem(z + NZ - 1, NZ) * NY + y
    peers += [(z_up, t), (z_dn, t)]
    for kv_to, tp_to in peers:
        pl.semaphore_signal(
            barrier, inc=1, device_id={"kv": kv_to, "tp": tp_to}, device_id_type=MESH
        )

    left = lax.broadcasted_iota(jnp.int32, (BLK, 128), 1) < BLK
    left_half = lax.broadcasted_iota(jnp.int32, (BLK // 2, 128), 1) < BLK
    wide = lax.broadcasted_iota(jnp.int32, (4 * BLK, 128), 1)
    first = lax.rem(wide, HEAD_DIM) < HEAD_DIM // 2

    for load in tables:
        load.wait()
    base = kv * 2 + t
    cb, sb = cb_ref[pl.ds(base, 1), :], sb_ref[pl.ds(base, 1), :]
    cr, sr = cr_ref[...], sr_ref[...]
    cosine[...] = cb * cr - sb * sr
    turned = sb * cr + cb * sr
    sine[...] = jnp.where(first, -turned, turned)

    def rotate(x):
        swapped = jnp.where(first, pltpu.roll(x, 96, 1), pltpu.roll(x, 32, 1))
        return x * cosine[...] + swapped * sine[...]

    def project_k(half):
        keys = jnp.dot(tok[...], wk[half], preferred_element_type=F32).astype(BF).astype(F32)
        keys = rotate(keys)
        keys = (keys, pltpu.roll(keys, 64, 1))
        for e in range(2):
            for j in range(4):
                low = keys[e][j * 64 : j * 64 + 32]
                high = keys[1 - e][j * 64 + 32 : j * 64 + 64]
                k_own[2 * half + e, j] = jnp.where(left_half, low, high).astype(BF)

    def project_v(half):
        values = jnp.dot(tok[...], wv[half], preferred_element_type=F32).T
        values = [values[:, i * 128 : i * 128 + 128] for i in range(2)]
        values = [(x, pltpu.roll(x, 64, 1)) for x in values]
        for e in range(2):
            for j in range(4):
                pair = values[j // 2]
                low = pair[j % 2][e * 64 : e * 64 + 32]
                high = pair[1 - j % 2][e * 64 + 32 : e * 64 + 64]
                v_own[2 * half + e, j] = jnp.where(left_half, low, high).astype(BF)

    def project_q(half):
        tokens = tok[...]
        full = jnp.dot(tokens, wq[half], preferred_element_type=F32)
        for n in range(4):
            x = full[:, n * 128 : n * 128 + 128].astype(BF).astype(F32)
            qs[2 * half + n // 2, :, (n % 2) * 128 : (n % 2) * 128 + 128] = rotate(x).astype(BF)

    for load in loads[:3]:
        load.wait()
    project_k(t)
    project_v(t)

    pl.semaphore_wait(barrier, len(peers))

    halves = [
        remote(wk.at[t], wk.at[t], w_send.at[0], w_recv.at[0], kv, other),
        remote(wv.at[t], wv.at[t], w_send.at[1], w_recv.at[1], kv, other),
        remote(wq.at[t], wq.at[t], w_send.at[2], w_recv.at[2], kv, other),
        remote(wo_hbm, wo.at[t], w_send.at[3], w_recv.at[3], kv, other),
    ]

    def to_owner(own, every, send, recv, head):
        return remote(
            own.at[head], every.at[chunk(z, y)], send.at[head], recv.at[y], z * NY + head, t
        )

    def key_to_owner(head):
        return to_owner(k_own, k_all, ky_send, ky_recv, head)

    def value_to_owner(head):
        return to_owner(v_own, v_all, vy_send, vy_recv, head)

    def send_heads(make, half):
        for e in range(2):
            head = 2 * half + e

            @pl.when(head != y)
            def _():
                make(head).start()

    for copy in halves[:2]:
        copy.start()
    send_heads(key_to_owner, t)
    picks = [
        remote(ch_hbm, ch_all.at[NY - k], c_send.at[k], c_recv.at[NY - k], row_peer(k), t)
        for k in range(1, NY)
    ]
    loads[3].wait()
    for copy in halves[2:] + picks:
        copy.start()
    halves[0].wait_recv()
    project_k(other)
    send_heads(key_to_owner, other)

    def ring(every, up_send, up_recv, dn_send, dn_recv, pt_send, pt_recv):
        def place(zz, k):
            return every.at[chunk(zz, row_chip(k))]

        def up(s, k, src=None):
            spot = place(lax.rem(z + NZ - s, NZ), k)
            src = spot if src is None else src
            return remote(src, spot, up_send.at[s, k], up_recv.at[s, k], z_up, t)

        def down(s, k, src=None):
            spot = place(lax.rem(z + s, NZ), k)
            src = spot if src is None else src
            return remote(src, spot, dn_send.at[s, k], dn_recv.at[s, k], z_dn, t)

        def partner(rel, k, src=None):
            spot = place(lax.rem(z + rel, NZ), k)
            src = spot if src is None else src
            return remote(src, spot, pt_send.at[rel, k], pt_recv.at[rel, k], kv, other)

        return up, down, partner

    k_ring = ring(k_all, k_up_send, k_up_recv, k_dn_send, k_dn_recv, k_pt_send, k_pt_recv)
    v_ring = ring(v_all, v_up_send, v_up_recv, v_dn_send, v_dn_recv, v_pt_send, v_pt_recv)

    def begin(group, k, src=None):
        up, down, partner = group
        up(0, k, src).start()
        down(0, k, src).start()
        partner(0, k, src).start()

    def step(group, s, k):
        up, down, partner = group
        if s < NZ // 2:
            turn = s == NZ // 2 - 1
            up(s - 1, k).wait_recv()
            if not turn:
                up(s, k).start()
            else:
                pl.when(k < 2)(lambda: up(s, k).start())
            partner(NZ - s, k).start()
            down(s - 1, k).wait_recv()
            if not turn:
                down(s, k).start()
            else:
                pl.when(k >= 2)(lambda: down(s, k).start())
            partner(s, k).start()
        else:
            pl.when(k < 2)(lambda: up(s - 1, k).wait_recv())
            pl.when(k >= 2)(lambda: down(s - 1, k).wait_recv())
            partner(s, k).start()

    mine = [
        pltpu.make_async_copy(k_own.at[y], k_all.at[chunk(z, y)], load_sem.at[5]),
        pltpu.make_async_copy(v_own.at[y], v_all.at[chunk(z, y)], load_sem.at[7]),
    ]
    begin(k_ring, 0, k_own.at[y])
    send_heads(value_to_owner, t)
    halves[1].wait_recv()
    project_v(other)
    send_heads(value_to_owner, other)
    for copy in mine:
        copy.start()

    def from_row(every, own, send, recv, k):
        remote(
            own.at[0], every.at[chunk(z, row_chip(k))], send.at[0], recv.at[row_chip(k)],
            row_peer(k), t,
        ).wait_recv()

    for k in (1, 3, 2):
        from_row(k_all, k_own, ky_send, ky_recv, k)
        begin(k_ring, k)
    for copy in mine:
        copy.wait()
    begin(v_ring, 0)
    for k in (1, 3, 2):
        from_row(v_all, v_own, vy_send, vy_recv, k)
        begin(v_ring, k)
    project_q(t)
    halves[2].wait_recv()
    project_q(other)
    own_q = pltpu.make_async_copy(qs.at[y], q_all.at[0], load_sem.at[6])
    own_q.start()
    queries = [None] * NY
    for k in (2, 1, 3):
        queries[NY - k] = remote(
            qs.at[row_chip(k)], q_all.at[NY - k], q_send.at[k], q_recv.at[NY - k],
            row_peer(k), t,
        )
        queries[NY - k].start()

    for copy in picks:
        copy.wait_recv()
    own_picks.wait()
    to_smem = pltpu.make_async_copy(ch_all, ch_smem, load_sem.at[13])
    to_smem.start()

    order = (0, 1, 3, 2)
    for s in range(1, NZ // 2 + 1):
        for k in order:
            step(k_ring, s, k)
        if s < NZ // 2:
            for k in order:
                step(v_ring, s, k)

    to_smem.wait()
    own_q.wait()
    for k in range(1, NY):
        queries[k].wait_recv()
    for rel in range(NZ):
        for k in range(NY):
            k_ring[2](rel, k).wait_recv()

    key_pos = lax.broadcasted_iota(jnp.int32, (BLK, 4 * BLK), 0)
    query_pos = lax.rem(lax.broadcasted_iota(jnp.int32, (BLK, 4 * BLK), 1), BLK)
    causal = key_pos <= query_pos
    half_blk = BLK // 2

    def own_block(k, jb):
        return (z * NY + row_chip(k)) * 8 + t * 4 + jb

    def gather_keys(k, jb):
        bias = []
        for j in range(PICK + 1):
            if j < PICK:
                pick = ch_smem[k, t * 4 + jb, j]
                bias.append(jnp.where(pick < 0, NEGATIVE, 0.0).astype(F32))
                block = k_all[jnp.maximum(pick, 0)]
            else:
                block = k_all[own_block(k, jb)]
            nothing = jnp.zeros_like(block)
            u, row = jb % 2, j * BLK
            kg[u, row : row + half_blk, :] = jnp.where(left_half, block, nothing)
            kg[u, row + half_blk : row + BLK, :] = jnp.where(left_half, nothing, block)
        return bias

    def load_queries(k, jb):
        heads = []
        for n in range(2):
            x = q_all[k, jb * BLK : jb * BLK + BLK, n * 128 : n * 128 + 128].astype(F32)
            swapped = pltpu.roll(x, 64, 1)
            heads += [jnp.where(left, x, swapped), jnp.where(left, swapped, x)]
        return jnp.concatenate(heads, axis=0).astype(BF)

    def eight(x, op):
        return op(x.reshape(BLK // 8, 8, 4 * BLK), axis=0)

    def score(u, half, q2, bias):
        span = 8 * BLK
        part = lax.dot_general(
            kg[u, half * span : half * span + span, :], q2, (((1,), (1,)), ((), ())),
            preferred_element_type=F32,
        )
        top = None
        for i in range(8):
            j = half * 8 + i
            block = part[i * BLK : i * BLK + BLK, :]
            if j == PICK:
                block = jnp.where(causal, block, NEGATIVE)
            scores[u, j * BLK : j * BLK + BLK, :] = block
            here = eight(block, jnp.max)
            here = here if j == PICK else here + bias[j]
            top = here if top is None else jnp.maximum(top, here)
        return top

    def softmax(state, half):
        k, jb, top, bias, total = state
        for j in range(half * 8, half * 8 + 8):
            shift = top if j == PICK else top - bias[j]
            p = jnp.exp2((scores[jb % 2, j * BLK : j * BLK + BLK, :] - shift) * EXPONENT)
            part = eight(p, jnp.sum)
            total = part if total is None else total + part
            probs[jb, j * BLK : j * BLK + BLK, :] = p.astype(BF)
        if half == 1:
            total = jnp.sum(total, axis=0, keepdims=True)
            inverse[k, pl.ds(jb, 1), :] = 1.0 / total
            logsum = top * HEAD_DIM**-0.5 + jnp.log(total)
            for h in range(4):
                ls_out[k, pl.ds(h, 1), jb * BLK : jb * BLK + BLK] = logsum[:, h * BLK : h * BLK + BLK]
        return k, jb, top, bias, total

    def weigh(k):
        state = None
        for jb in range(4):
            bias = gather_keys(k, jb)
            q2 = load_queries(k, jb)
            tops = []
            for half in range(2):
                tops.append(score(jb % 2, half, q2, bias))
                if state is not None:
                    state = softmax(state, half)
            top = jnp.max(jnp.maximum(*tops), axis=0, keepdims=True)
            state = (k, jb, top, bias, None)
        for half in range(2):
            state = softmax(state, half)

    def gather_values(k, jb):
        previous = None
        for j in range(PICK + 1):
            if j < PICK:
                block = v_all[jnp.maximum(ch_smem[k, t * 4 + jb, j], 0)]
            else:
                block = v_all[own_block(k, jb)]
            block = block.astype(F32)
            if j % 2 == 1:
                low = jnp.where(left_half, previous, pltpu.roll(block, 64, 1))
                high = jnp.where(left_half, pltpu.roll(previous, 64, 1), block)
                columns = slice((j // 2) * 128, (j // 2) * 128 + 128)
                vt[jb, :half_blk, columns] = low.astype(BF)
                vt[jb, half_blk:, columns] = high.astype(BF)
            previous = block

    def combine(k):
        for jb in range(4):
            gather_values(k, jb)
        mixed = [
            jnp.dot(vt[jb], probs[jb], preferred_element_type=F32) for jb in range(4)
        ]
        for jb in range(4):
            turned_back = (mixed[jb] * inverse[k, pl.ds(jb, 1), :]).T
            parts = [turned_back[h * BLK : h * BLK + BLK] for h in range(4)]
            att_out[k, jb * BLK : jb * BLK + BLK, :] = jnp.concatenate(parts, axis=1).astype(BF)

    to_self = y // 2 == t
    slot = (lax.rem(y, 2), t)

    def log_piece(k):
        return remote(
            ls_out.at[k], ls_all.at[slot], l_send.at[k], l_recv.at[slot], row_peer(k), y // 2
        )

    def give_back(k):
        return remote(
            att_out.at[k], att_all.at[NY - k], a_send.at[k], a_recv.at[NY - k], row_peer(k), t
        )

    @pl.loop(0, NY)
    def _(i):
        k = lax.rem(i + 1, NY)
        weigh(k)

        @pl.when(i == 0)
        def _():
            for r in order:
                step(v_ring, NZ // 2, r)
            for rel in range(NZ):
                for r in range(NY):
                    v_ring[2](rel, r).wait_recv()

        combine(k)

        @pl.when(k > 0)
        def _():
            give_back(k).start()
            log_piece(k).start()

    pl.when(jnp.logical_not(to_self))(lambda: log_piece(0).start())

    @pl.when(to_self)
    def _():
        ls_all[slot] = ls_out[0]

    loads[4].wait()
    halves[3].wait_recv()
    for k in (0, 3, 2, 1):
        if k > 0:
            give_back(NY - k).wait_recv()
        ys = row_chip(k)
        weights = wo[ys // 2, pl.ds(pl.multiple_of(lax.rem(ys, 2) * 256, 256), 256), :]
        piece = att_out[0] if k == 0 else att_all[k]
        part = jnp.dot(piece, weights, preferred_element_type=F32)
        if k == 0:
            acc[...] = part
        elif k != 1:
            acc[...] += part
        else:
            projected = acc[...] + part
            square = jnp.mean(projected * projected, axis=-1, keepdims=True)
            out_ref[...] = (projected * lax.rsqrt(square + EPSILON)).astype(BF)

    for ys in range(2):
        for tt in range(2):
            @pl.when(jnp.logical_not((t * 2 + ys == y) & (t == tt)))
            def _():
                remote(
                    ls_out.at[0], ls_all.at[ys, tt], l_send.at[0], l_recv.at[ys, tt], kv, other
                ).wait_recv()

            ls_ref[ys * 4 : ys * 4 + 4, tt * 4 * BLK : tt * 4 * BLK + 4 * BLK] = ls_all[ys, tt]
    for k in range(1, NY):
        log_piece(k).wait_send()
    pl.when(jnp.logical_not(to_self))(lambda: log_piece(0).wait_send())
    for k in range(1, NY):
        key_to_owner(row_chip(k)).wait_send()
        value_to_owner(row_chip(k)).wait_send()
        queries[k].wait_send()
        give_back(k).wait_send()
    for copy in halves + picks:
        copy.wait_send()
    for up, down, partner in (k_ring, v_ring):
        for k in range(NY):
            for s in range(NZ // 2):
                if s < NZ // 2 - 1 or k < 2:
                    up(s, k).wait_send()
                if s < NZ // 2 - 1 or k >= 2:
                    down(s, k).wait_send()
            for rel in range(NZ):
                partner(rel, k).wait_send()


def shards(tokens, w_query, w_key, w_value, w_out, chosen):
    rows, width = tokens.shape[1:]
    tables = rotary_tables(rows, 2 * NY * NZ)
    any_space = pl.BlockSpec(memory_space=pl.ANY)
    vmem = pl.BlockSpec(memory_space=pltpu.VMEM)
    dma = pltpu.SemaphoreType.DMA
    out, logs = pl.pallas_call(
        kernel,
        out_shape=(
            jax.ShapeDtypeStruct((rows, width), BF),
            jax.ShapeDtypeStruct((8, 2 * rows), F32),
        ),
        in_specs=[any_space] * 10,
        out_specs=(vmem, vmem),
        scratch_shapes=[
            pltpu.VMEM((rows, 128), F32),
            pltpu.VMEM((rows, 128), F32),
            pltpu.VMEM((2 * NY * NZ, 128), F32),
            pltpu.VMEM((2 * NY * NZ, 128), F32),
            pltpu.VMEM((rows, width), BF),
            pltpu.VMEM((2,) + w_query.shape, BF),
            pltpu.VMEM((2,) + w_key.shape, BF),
            pltpu.VMEM((2,) + w_value.shape, BF),
            pltpu.VMEM((2,) + w_out.shape, BF),
            pltpu.VMEM((rows, 128), F32),
            pltpu.VMEM((rows, 128), F32),
            pltpu.VMEM((4, 4, BLK // 2, 128), BF),
            pltpu.VMEM((4, 4, BLK // 2, 128), BF),
            pltpu.VMEM((NZ * NY * 8, BLK // 2, 128), BF),
            pltpu.VMEM((NZ * NY * 8, BLK // 2, 128), BF),
            pltpu.VMEM((NY, rows, 256), BF),
            pltpu.VMEM((NY, rows, 256), BF),
            pltpu.VMEM((NY, 8, PICK), jnp.int32),
            pltpu.SMEM((NY, 8, PICK), jnp.int32),
            pltpu.VMEM((2, (PICK + 1) * BLK, 128), BF),
            pltpu.VMEM((4, BLK, (PICK + 1) * BLK), BF),
            pltpu.VMEM((2, (PICK + 1) * BLK, 4 * BLK), F32),
            pltpu.VMEM((4, (PICK + 1) * BLK, 4 * BLK), BF),
            pltpu.VMEM((NY, 4, 4 * BLK), F32),
            pltpu.VMEM((NY, rows, 256), BF),
            pltpu.VMEM((NY, rows, 256), BF),
            pltpu.VMEM((NY, 4, 4 * BLK), F32),
            pltpu.VMEM((2, 2, 4, 4 * BLK), F32),
            pltpu.VMEM((rows, width), F32),
            dma((14,)), dma((4,)), dma((4,)), dma((4,)), dma((4,)), dma((4,)), dma((4,)),
            dma((4, 4)), dma((4, 4)), dma((4, 4)), dma((4, 4)), dma((NZ, 4)), dma((NZ, 4)),
            dma((4, 4)), dma((4, 4)), dma((4, 4)), dma((4, 4)), dma((NZ, 4)), dma((NZ, 4)),
            dma((4,)), dma((4,)), dma((4,)), dma((4,)),
            dma((4,)), dma((4,)), dma((4,)), dma((2, 2)),
        ],
        compiler_params=pltpu.CompilerParams(
            collective_id=0, has_side_effects=True, vmem_limit_bytes=67_000_000
        ),
    )(*tables, tokens[0], w_query, w_key, w_value, w_out, chosen[0])
    return out[None], logs.T[None]


def solution(mesh):
    placed = (
        P("dp", ("kv", "tp"), None),
        P(None, "tp"),
        P(None, "tp"),
        P(None, "tp"),
        P("tp", None),
        P("dp", "kv", None),
    )
    return jax.shard_map(
        shards,
        mesh=mesh,
        in_specs=placed,
        out_specs=(P("dp", ("kv", "tp"), None), P("dp", "kv", "tp")),
        check_vma=False,
    )
```

```python
import math

import jax
import jax.numpy as jnp
import numpy as np
from jax import lax
from jax.experimental import pallas as pl
from jax.experimental.pallas import tpu as pltpu
from jax.sharding import PartitionSpec as P

HEAD_DIM = 64
BLK = 64
PICK = 15
THETA_BASE = 10000.0
NEGATIVE = -1e30
EPSILON = 1e-06
MESH = pl.DeviceIdType.MESH
BF = jnp.bfloat16
F32 = jnp.float32
EXPONENT = math.log2(math.e) / math.sqrt(HEAD_DIM)
NY = 4
NZ = 8


def rotary_tables(rows, bases):
    half = HEAD_DIM // 2
    freq = THETA_BASE ** (-np.arange(half, dtype=np.float64) / half)
    freq = np.tile(freq, 128 // half)[None, :]
    offset = np.arange(rows, dtype=np.float64)[:, None] * freq
    base = np.arange(bases, dtype=np.float64)[:, None] * rows * freq
    return [
        np.asarray(a, np.float32)
        for a in (np.cos(offset), np.sin(offset), np.cos(base), np.sin(base))
    ]


def kernel(
    cr_hbm, sr_hbm, cb_hbm, sb_hbm, tok_hbm, wq_hbm, wk_hbm, wv_hbm, wo_hbm, ch_hbm,
    out_ref, ls_ref,
    cr_ref, sr_ref, cb_ref, sb_ref, tok, wq, wk, wv, wo, cosine, sine, k_own, v_own,
    k_all, v_all, qs, q_all, ch_all, ch_smem, kg, vt, scores, probs, inverse,
    att_out, att_all, ls_out, ls_all, acc,
    load_sem, w_send, w_recv, ky_send, ky_recv, vy_send, vy_recv,
    k_up_send, k_up_recv, k_dn_send, k_dn_recv, k_pt_send, k_pt_recv,
    v_up_send, v_up_recv, v_dn_send, v_dn_recv, v_pt_send, v_pt_recv,
    q_send, q_recv, c_send, c_recv, a_send, a_recv, l_send, l_recv,
):
    kv = lax.axis_index("kv")
    t = lax.axis_index("tp")
    z, y = kv // NY, kv % NY
    other = 1 - t

    def row_chip(k):
        return lax.rem(y + k, NY)

    def row_peer(k):
        return z * NY + row_chip(k)

    def chunk(zz, yy):
        return pl.ds(((zz * NY + yy) * 2 + t) * 4, 4)

    def remote(src, dst, send, recv, kv_to, tp_to):
        return pltpu.make_async_remote_copy(
            src_ref=src, dst_ref=dst, send_sem=send, recv_sem=recv,
            device_id={"kv": kv_to, "tp": tp_to}, device_id_type=MESH,
        )

    loads = [
        pltpu.make_async_copy(tok_hbm, tok, load_sem.at[0]),
        pltpu.make_async_copy(wk_hbm, wk.at[t], load_sem.at[1]),
        pltpu.make_async_copy(wv_hbm, wv.at[t], load_sem.at[2]),
        pltpu.make_async_copy(wq_hbm, wq.at[t], load_sem.at[3]),
        pltpu.make_async_copy(wo_hbm, wo.at[t], load_sem.at[4]),
    ]
    tables = [
        pltpu.make_async_copy(a, b, load_sem.at[8 + i])
        for i, (a, b) in enumerate(
            ((cr_hbm, cr_ref), (sr_hbm, sr_ref), (cb_hbm, cb_ref), (sb_hbm, sb_ref))
        )
    ]
    own_picks = pltpu.make_async_copy(ch_hbm, ch_all.at[0], load_sem.at[12])
    for load in loads[:3] + tables + loads[3:] + [own_picks]:
        load.start()

    barrier = pltpu.get_barrier_semaphore()
    peers = [(row_peer(k), tt) for k in range(1, NY) for tt in (t, other)]
    peers += [(kv, other)]
    z_up = lax.rem(z + 1, NZ) * NY + y
    z_dn = lax.rem(z + NZ - 1, NZ) * NY + y
    peers += [(z_up, t), (z_dn, t)]
    for kv_to, tp_to in peers:
        pl.semaphore_signal(
            barrier, inc=1, device_id={"kv": kv_to, "tp": tp_to}, device_id_type=MESH
        )

    left = lax.broadcasted_iota(jnp.int32, (BLK, 128), 1) < BLK
    left_half = lax.broadcasted_iota(jnp.int32, (BLK // 2, 128), 1) < BLK
    wide = lax.broadcasted_iota(jnp.int32, (4 * BLK, 128), 1)
    first = lax.rem(wide, HEAD_DIM) < HEAD_DIM // 2

    for load in tables:
        load.wait()
    base = kv * 2 + t
    cb, sb = cb_ref[pl.ds(base, 1), :], sb_ref[pl.ds(base, 1), :]
    cr, sr = cr_ref[...], sr_ref[...]
    cosine[...] = cb * cr - sb * sr
    turned = sb * cr + cb * sr
    sine[...] = jnp.where(first, -turned, turned)

    def rotate(x):
        swapped = jnp.where(first, pltpu.roll(x, 96, 1), pltpu.roll(x, 32, 1))
        return x * cosine[...] + swapped * sine[...]

    def project_k(half):
        keys = jnp.dot(tok[...], wk[half], preferred_element_type=F32).astype(BF).astype(F32)
        keys = rotate(keys)
        keys = (keys, pltpu.roll(keys, 64, 1))
        for e in range(2):
            for j in range(4):
                low = keys[e][j * 64 : j * 64 + 32]
                high = keys[1 - e][j * 64 + 32 : j * 64 + 64]
                k_own[2 * half + e, j] = jnp.where(left_half, low, high).astype(BF)

    def project_v(half):
        values = jnp.dot(tok[...], wv[half], preferred_element_type=F32).T
        values = [values[:, i * 128 : i * 128 + 128] for i in range(2)]
        values = [(x, pltpu.roll(x, 64, 1)) for x in values]
        for e in range(2):
            for j in range(4):
                pair = values[j // 2]
                low = pair[j % 2][e * 64 : e * 64 + 32]
                high = pair[1 - j % 2][e * 64 + 32 : e * 64 + 64]
                v_own[2 * half + e, j] = jnp.where(left_half, low, high).astype(BF)

    def project_q(half):
        tokens = tok[...]
        full = jnp.dot(tokens, wq[half], preferred_element_type=F32)
        for n in range(4):
            x = full[:, n * 128 : n * 128 + 128].astype(BF).astype(F32)
            qs[2 * half + n // 2, :, (n % 2) * 128 : (n % 2) * 128 + 128] = rotate(x).astype(BF)

    for load in loads[:3]:
        load.wait()
    project_k(t)
    project_v(t)

    pl.semaphore_wait(barrier, len(peers))

    halves = [
        remote(wk.at[t], wk.at[t], w_send.at[0], w_recv.at[0], kv, other),
        remote(wv.at[t], wv.at[t], w_send.at[1], w_recv.at[1], kv, other),
        remote(wq.at[t], wq.at[t], w_send.at[2], w_recv.at[2], kv, other),
        remote(wo_hbm, wo.at[t], w_send.at[3], w_recv.at[3], kv, other),
    ]

    def to_owner(own, every, send, recv, head):
        return remote(
            own.at[head], every.at[chunk(z, y)], send.at[head], recv.at[y], z * NY + head, t
        )

    def key_to_owner(head):
        return to_owner(k_own, k_all, ky_send, ky_recv, head)

    def value_to_owner(head):
        return to_owner(v_own, v_all, vy_send, vy_recv, head)

    def send_heads(make, half):
        for e in range(2):
            head = 2 * half + e

            @pl.when(head != y)
            def _():
                make(head).start()

    def ring(every, up_send, up_recv, dn_send, dn_recv, pt_send, pt_recv):
        def place(zz, k):
            return every.at[chunk(zz, row_chip(k))]

        def up(s, k, src=None):
            spot = place(lax.rem(z + NZ - s, NZ), k)
            src = spot if src is None else src
            return remote(src, spot, up_send.at[s, k], up_recv.at[s, k], z_up, t)

        def down(s, k, src=None):
            spot = place(lax.rem(z + s, NZ), k)
            src = spot if src is None else src
            return remote(src, spot, dn_send.at[s, k], dn_recv.at[s, k], z_dn, t)

        def partner(rel, k, src=None):
            spot = place(lax.rem(z + rel, NZ), k)
            src = spot if src is None else src
            return remote(src, spot, pt_send.at[rel, k], pt_recv.at[rel, k], kv, other)

        return up, down, partner

    k_ring = ring(k_all, k_up_send, k_up_recv, k_dn_send, k_dn_recv, k_pt_send, k_pt_recv)
    v_ring = ring(v_all, v_up_send, v_up_recv, v_dn_send, v_dn_recv, v_pt_send, v_pt_recv)

    def begin(group, k, src=None):
        up, down, partner = group
        up(0, k, src).start()
        down(0, k, src).start()
        partner(0, k, src).start()

    def step(group, s, k):
        up, down, partner = group
        if s < NZ // 2:
            turn = s == NZ // 2 - 1
            up(s - 1, k).wait_recv()
            if not turn:
                up(s, k).start()
            else:
                pl.when(k < 2)(lambda: up(s, k).start())
            partner(NZ - s, k).start()
            down(s - 1, k).wait_recv()
            if not turn:
                down(s, k).start()
            else:
                pl.when(k >= 2)(lambda: down(s, k).start())
            partner(s, k).start()
        else:
            pl.when(k < 2)(lambda: up(s - 1, k).wait_recv())
            pl.when(k >= 2)(lambda: down(s - 1, k).wait_recv())
            partner(s, k).start()

    for copy in halves[:2]:
        copy.start()
    ready = y // 2 == t
    pl.when(ready)(lambda: begin(k_ring, 0, k_own.at[y]))
    send_heads(key_to_owner, t)
    picks = [
        remote(ch_hbm, ch_all.at[NY - k], c_send.at[k], c_recv.at[NY - k], row_peer(k), t)
        for k in range(1, NY)
    ]
    loads[3].wait()
    for copy in halves[2:] + picks:
        copy.start()
    halves[0].wait_recv()
    project_k(other)
    send_heads(key_to_owner, other)

    mine = [
        pltpu.make_async_copy(k_own.at[y], k_all.at[chunk(z, y)], load_sem.at[5]),
        pltpu.make_async_copy(v_own.at[y], v_all.at[chunk(z, y)], load_sem.at[7]),
    ]
    pl.when(jnp.logical_not(ready))(lambda: begin(k_ring, 0, k_own.at[y]))
    send_heads(value_to_owner, t)
    halves[1].wait_recv()
    project_v(other)
    send_heads(value_to_owner, other)
    begin(v_ring, 0, v_own.at[y])
    for copy in mine:
        copy.start()

    def from_row(every, own, send, recv, k):
        remote(
            own.at[0], every.at[chunk(z, row_chip(k))], send.at[0], recv.at[row_chip(k)],
            row_peer(k), t,
        ).wait_recv()

    for k in (1, 3, 2):
        from_row(k_all, k_own, ky_send, ky_recv, k)
        begin(k_ring, k)
    for copy in mine:
        copy.wait()
    for k in (1, 3, 2):
        from_row(v_all, v_own, vy_send, vy_recv, k)
        begin(v_ring, k)
    project_q(t)
    halves[2].wait_recv()
    project_q(other)
    own_q = pltpu.make_async_copy(qs.at[y], q_all.at[0], load_sem.at[6])
    own_q.start()
    queries = [None] * NY
    for k in (2, 1, 3):
        queries[NY - k] = remote(
            qs.at[row_chip(k)], q_all.at[NY - k], q_send.at[k], q_recv.at[NY - k],
            row_peer(k), t,
        )
        queries[NY - k].start()

    for copy in picks:
        copy.wait_recv()
    own_picks.wait()
    to_smem = pltpu.make_async_copy(ch_all, ch_smem, load_sem.at[13])
    to_smem.start()

    order = (0, 1, 3, 2)
    for s in range(1, NZ // 2 + 1):
        for k in order:
            step(k_ring, s, k)
        if s < NZ // 2:
            for k in order:
                step(v_ring, s, k)

    to_smem.wait()
    own_q.wait()
    for k in range(1, NY):
        queries[k].wait_recv()
    for rel in range(NZ):
        for k in range(NY):
            k_ring[2](rel, k).wait_recv()

    key_pos = lax.broadcasted_iota(jnp.int32, (BLK, 4 * BLK), 0)
    query_pos = lax.rem(lax.broadcasted_iota(jnp.int32, (BLK, 4 * BLK), 1), BLK)
    causal = key_pos <= query_pos
    half_blk = BLK // 2

    def own_block(k, jb):
        return (z * NY + row_chip(k)) * 8 + t * 4 + jb

    def gather_keys(k, jb):
        bias = []
        for j in range(PICK + 1):
            if j < PICK:
                pick = ch_smem[k, t * 4 + jb, j]
                bias.append(jnp.where(pick < 0, NEGATIVE, 0.0).astype(F32))
                block = k_all[jnp.maximum(pick, 0)]
            else:
                block = k_all[own_block(k, jb)]
            nothing = jnp.zeros_like(block)
            u, row = jb % 2, j * BLK
            kg[u, row : row + half_blk, :] = jnp.where(left_half, block, nothing)
            kg[u, row + half_blk : row + BLK, :] = jnp.where(left_half, nothing, block)
        return bias

    def load_queries(k, jb):
        heads = []
        for n in range(2):
            x = q_all[k, jb * BLK : jb * BLK + BLK, n * 128 : n * 128 + 128].astype(F32)
            swapped = pltpu.roll(x, 64, 1)
            heads += [jnp.where(left, x, swapped), jnp.where(left, swapped, x)]
        return jnp.concatenate(heads, axis=0).astype(BF)

    def eight(x, op):
        return op(x.reshape(BLK // 8, 8, 4 * BLK), axis=0)

    def score(u, half, q2, bias):
        span = 8 * BLK
        part = lax.dot_general(
            kg[u, half * span : half * span + span, :], q2, (((1,), (1,)), ((), ())),
            preferred_element_type=F32,
        )
        top = None
        for i in range(8):
            j = half * 8 + i
            block = part[i * BLK : i * BLK + BLK, :]
            if j == PICK:
                block = jnp.where(causal, block, NEGATIVE)
            scores[u, j * BLK : j * BLK + BLK, :] = block
            here = eight(block, jnp.max)
            here = here if j == PICK else here + bias[j]
            top = here if top is None else jnp.maximum(top, here)
        return top

    def softmax(state, half):
        k, jb, top, bias, total = state
        for j in range(half * 8, half * 8 + 8):
            shift = top if j == PICK else top - bias[j]
            p = jnp.exp2((scores[jb % 2, j * BLK : j * BLK + BLK, :] - shift) * EXPONENT)
            part = eight(p, jnp.sum)
            total = part if total is None else total + part
            probs[jb, j * BLK : j * BLK + BLK, :] = p.astype(BF)
        if half == 1:
            total = jnp.sum(total, axis=0, keepdims=True)
            inverse[k, pl.ds(jb, 1), :] = 1.0 / total
            logsum = top * HEAD_DIM**-0.5 + jnp.log(total)
            for h in range(4):
                ls_out[k, pl.ds(h, 1), jb * BLK : jb * BLK + BLK] = logsum[:, h * BLK : h * BLK + BLK]
        return k, jb, top, bias, total

    def weigh(k):
        state = None
        for jb in range(4):
            bias = gather_keys(k, jb)
            q2 = load_queries(k, jb)
            tops = []
            for half in range(2):
                tops.append(score(jb % 2, half, q2, bias))
                if state is not None:
                    state = softmax(state, half)
            top = jnp.max(jnp.maximum(*tops), axis=0, keepdims=True)
            state = (k, jb, top, bias, None)
        for half in range(2):
            state = softmax(state, half)

    def gather_values(k, jb):
        previous = None
        for j in range(PICK + 1):
            if j < PICK:
                block = v_all[jnp.maximum(ch_smem[k, t * 4 + jb, j], 0)]
            else:
                block = v_all[own_block(k, jb)]
            block = block.astype(F32)
            if j % 2 == 1:
                low = jnp.where(left_half, previous, pltpu.roll(block, 64, 1))
                high = jnp.where(left_half, pltpu.roll(previous, 64, 1), block)
                columns = slice((j // 2) * 128, (j // 2) * 128 + 128)
                vt[jb, :half_blk, columns] = low.astype(BF)
                vt[jb, half_blk:, columns] = high.astype(BF)
            previous = block

    def combine(k):
        for jb in range(4):
            gather_values(k, jb)
        mixed = [
            jnp.dot(vt[jb], probs[jb], preferred_element_type=F32) for jb in range(4)
        ]
        for jb in range(4):
            turned_back = (mixed[jb] * inverse[k, pl.ds(jb, 1), :]).T
            parts = [turned_back[h * BLK : h * BLK + BLK] for h in range(4)]
            att_out[k, jb * BLK : jb * BLK + BLK, :] = jnp.concatenate(parts, axis=1).astype(BF)

    to_self = y // 2 == t
    slot = (lax.rem(y, 2), t)

    def log_piece(k):
        return remote(
            ls_out.at[k], ls_all.at[slot], l_send.at[k], l_recv.at[slot], row_peer(k), y // 2
        )

    def give_back(k):
        return remote(
            att_out.at[k], att_all.at[NY - k], a_send.at[k], a_recv.at[NY - k], row_peer(k), t
        )

    @pl.loop(0, NY)
    def _(i):
        k = lax.rem(i + 1, NY)
        weigh(k)

        @pl.when(i == 0)
        def _():
            for r in order:
                step(v_ring, NZ // 2, r)
            for rel in range(NZ):
                for r in range(NY):
                    v_ring[2](rel, r).wait_recv()

        combine(k)

        @pl.when(k > 0)
        def _():
            give_back(k).start()
            log_piece(k).start()

    pl.when(jnp.logical_not(to_self))(lambda: log_piece(0).start())

    @pl.when(to_self)
    def _():
        ls_all[slot] = ls_out[0]

    loads[4].wait()
    halves[3].wait_recv()
    def part(k):
        ys = row_chip(k)
        weights = wo[ys // 2, pl.ds(pl.multiple_of(lax.rem(ys, 2) * 256, 256), 256), :]
        piece = att_out[0] if k == 0 else att_all[k]
        return jnp.dot(piece, weights, preferred_element_type=F32)

    for k in (1, 2):
        give_back(k).wait_recv()
    acc[...] = part(0) + part(3) + part(2)
    give_back(3).wait_recv()
    projected = acc[...] + part(1)
    square = jnp.mean(projected * projected, axis=-1, keepdims=True)
    out_ref[...] = (projected * lax.rsqrt(square + EPSILON)).astype(BF)

    for ys in range(2):
        for tt in range(2):
            @pl.when(jnp.logical_not((t * 2 + ys == y) & (t == tt)))
            def _():
                remote(
                    ls_out.at[0], ls_all.at[ys, tt], l_send.at[0], l_recv.at[ys, tt], kv, other
                ).wait_recv()

            ls_ref[ys * 4 : ys * 4 + 4, tt * 4 * BLK : tt * 4 * BLK + 4 * BLK] = ls_all[ys, tt]
    for k in range(1, NY):
        log_piece(k).wait_send()
    pl.when(jnp.logical_not(to_self))(lambda: log_piece(0).wait_send())
    for k in range(1, NY):
        key_to_owner(row_chip(k)).wait_send()
        value_to_owner(row_chip(k)).wait_send()
        queries[k].wait_send()
        give_back(k).wait_send()
    for copy in halves + picks:
        copy.wait_send()
    for up, down, partner in (k_ring, v_ring):
        for k in range(NY):
            for s in range(NZ // 2):
                if s < NZ // 2 - 1 or k < 2:
                    up(s, k).wait_send()
                if s < NZ // 2 - 1 or k >= 2:
                    down(s, k).wait_send()
            for rel in range(NZ):
                partner(rel, k).wait_send()


def shards(tokens, w_query, w_key, w_value, w_out, chosen):
    rows, width = tokens.shape[1:]
    tables = rotary_tables(rows, 2 * NY * NZ)
    any_space = pl.BlockSpec(memory_space=pl.ANY)
    vmem = pl.BlockSpec(memory_space=pltpu.VMEM)
    dma = pltpu.SemaphoreType.DMA
    out, logs = pl.pallas_call(
        kernel,
        out_shape=(
            jax.ShapeDtypeStruct((rows, width), BF),
            jax.ShapeDtypeStruct((8, 2 * rows), F32),
        ),
        in_specs=[any_space] * 10,
        out_specs=(vmem, vmem),
        scratch_shapes=[
            pltpu.VMEM((rows, 128), F32),
            pltpu.VMEM((rows, 128), F32),
            pltpu.VMEM((2 * NY * NZ, 128), F32),
            pltpu.VMEM((2 * NY * NZ, 128), F32),
            pltpu.VMEM((rows, width), BF),
            pltpu.VMEM((2,) + w_query.shape, BF),
            pltpu.VMEM((2,) + w_key.shape, BF),
            pltpu.VMEM((2,) + w_value.shape, BF),
            pltpu.VMEM((2,) + w_out.shape, BF),
            pltpu.VMEM((rows, 128), F32),
            pltpu.VMEM((rows, 128), F32),
            pltpu.VMEM((4, 4, BLK // 2, 128), BF),
            pltpu.VMEM((4, 4, BLK // 2, 128), BF),
            pltpu.VMEM((NZ * NY * 8, BLK // 2, 128), BF),
            pltpu.VMEM((NZ * NY * 8, BLK // 2, 128), BF),
            pltpu.VMEM((NY, rows, 256), BF),
            pltpu.VMEM((NY, rows, 256), BF),
            pltpu.VMEM((NY, 8, PICK), jnp.int32),
            pltpu.SMEM((NY, 8, PICK), jnp.int32),
            pltpu.VMEM((2, (PICK + 1) * BLK, 128), BF),
            pltpu.VMEM((4, BLK, (PICK + 1) * BLK), BF),
            pltpu.VMEM((2, (PICK + 1) * BLK, 4 * BLK), F32),
            pltpu.VMEM((4, (PICK + 1) * BLK, 4 * BLK), BF),
            pltpu.VMEM((NY, 4, 4 * BLK), F32),
            pltpu.VMEM((NY, rows, 256), BF),
            pltpu.VMEM((NY, rows, 256), BF),
            pltpu.VMEM((NY, 4, 4 * BLK), F32),
            pltpu.VMEM((2, 2, 4, 4 * BLK), F32),
            pltpu.VMEM((rows, width), F32),
            dma((14,)), dma((4,)), dma((4,)), dma((4,)), dma((4,)), dma((4,)), dma((4,)),
            dma((4, 4)), dma((4, 4)), dma((4, 4)), dma((4, 4)), dma((NZ, 4)), dma((NZ, 4)),
            dma((4, 4)), dma((4, 4)), dma((4, 4)), dma((4, 4)), dma((NZ, 4)), dma((NZ, 4)),
            dma((4,)), dma((4,)), dma((4,)), dma((4,)),
            dma((4,)), dma((4,)), dma((4,)), dma((2, 2)),
        ],
        compiler_params=pltpu.CompilerParams(
            collective_id=0, has_side_effects=True, vmem_limit_bytes=67_000_000
        ),
    )(*tables, tokens[0], w_query, w_key, w_value, w_out, chosen[0])
    return out[None], logs.T[None]


def solution(mesh):
    placed = (
        P("dp", ("kv", "tp"), None),
        P(None, "tp"),
        P(None, "tp"),
        P(None, "tp"),
        P("tp", None),
        P("dp", "kv", None),
    )
    return jax.shard_map(
        shards,
        mesh=mesh,
        in_specs=placed,
        out_specs=(P("dp", ("kv", "tp"), None), P("dp", "kv", "tp")),
        check_vma=False,
    )
```

```python
import math

import jax
import jax.numpy as jnp
import numpy as np
from jax import lax
from jax.experimental import pallas as pl
from jax.experimental.pallas import tpu as pltpu
from jax.sharding import PartitionSpec as P

HEAD_DIM = 64
BLK = 64
PICK = 15
THETA_BASE = 10000.0
NEGATIVE = -1e30
EPSILON = 1e-06
MESH = pl.DeviceIdType.MESH
BF = jnp.bfloat16
F32 = jnp.float32
EXPONENT = math.log2(math.e) / math.sqrt(HEAD_DIM)
NY = 4
NZ = 8


def rotary_tables(rows, bases):
    half = HEAD_DIM // 2
    freq = THETA_BASE ** (-np.arange(half, dtype=np.float64) / half)
    freq = np.tile(freq, 128 // half)[None, :]
    offset = np.arange(rows, dtype=np.float64)[:, None] * freq
    base = np.arange(bases, dtype=np.float64)[:, None] * rows * freq
    return [
        np.asarray(a, np.float32)
        for a in (np.cos(offset), np.sin(offset), np.cos(base), np.sin(base))
    ]


def kernel(
    cr_hbm, sr_hbm, cb_hbm, sb_hbm, tok_hbm, wq_hbm, wk_hbm, wv_hbm, wo_hbm, ch_hbm,
    out_ref, ls_ref,
    cr_ref, sr_ref, cb_ref, sb_ref, tok, wq, wk, wv, wo, cosine, sine, k_own, v_own,
    k_all, v_all, qs, q_all, ch_all, ch_smem, kg, vt, scores, probs, inverse,
    att_out, att_all, ls_out, ls_all, acc,
    load_sem, w_send, w_recv, ky_send, ky_recv, vy_send, vy_recv,
    k_up_send, k_up_recv, k_dn_send, k_dn_recv, k_pt_send, k_pt_recv,
    v_up_send, v_up_recv, v_dn_send, v_dn_recv, v_pt_send, v_pt_recv,
    q_send, q_recv, c_send, c_recv, a_send, a_recv, l_send, l_recv,
):
    kv = lax.axis_index("kv")
    t = lax.axis_index("tp")
    z, y = kv // NY, kv % NY
    other = 1 - t

    def row_chip(k):
        return lax.rem(y + k, NY)

    def row_peer(k):
        return z * NY + row_chip(k)

    def chunk(zz, yy):
        return pl.ds(((zz * NY + yy) * 2 + t) * 4, 4)

    def remote(src, dst, send, recv, kv_to, tp_to):
        return pltpu.make_async_remote_copy(
            src_ref=src, dst_ref=dst, send_sem=send, recv_sem=recv,
            device_id={"kv": kv_to, "tp": tp_to}, device_id_type=MESH,
        )

    loads = [
        pltpu.make_async_copy(tok_hbm, tok, load_sem.at[0]),
        pltpu.make_async_copy(wk_hbm, wk.at[t], load_sem.at[1]),
        pltpu.make_async_copy(wv_hbm, wv.at[t], load_sem.at[2]),
        pltpu.make_async_copy(wq_hbm, wq.at[t], load_sem.at[3]),
        pltpu.make_async_copy(wo_hbm, wo.at[t], load_sem.at[4]),
    ]
    tables = [
        pltpu.make_async_copy(a, b, load_sem.at[8 + i])
        for i, (a, b) in enumerate(
            ((cr_hbm, cr_ref), (sr_hbm, sr_ref), (cb_hbm, cb_ref), (sb_hbm, sb_ref))
        )
    ]
    own_picks = pltpu.make_async_copy(ch_hbm, ch_all.at[0], load_sem.at[12])
    for load in loads[:3] + tables + loads[3:] + [own_picks]:
        load.start()

    barrier = pltpu.get_barrier_semaphore()
    peers = [(row_peer(k), tt) for k in range(1, NY) for tt in (t, other)]
    peers += [(kv, other)]
    z_up = lax.rem(z + 1, NZ) * NY + y
    z_dn = lax.rem(z + NZ - 1, NZ) * NY + y
    peers += [(z_up, t), (z_dn, t)]
    for kv_to, tp_to in peers:
        pl.semaphore_signal(
            barrier, inc=1, device_id={"kv": kv_to, "tp": tp_to}, device_id_type=MESH
        )

    left = lax.broadcasted_iota(jnp.int32, (BLK, 128), 1) < BLK
    left_half = lax.broadcasted_iota(jnp.int32, (BLK // 2, 128), 1) < BLK
    wide = lax.broadcasted_iota(jnp.int32, (4 * BLK, 128), 1)
    first = lax.rem(wide, HEAD_DIM) < HEAD_DIM // 2

    for load in tables:
        load.wait()
    base = kv * 2 + t
    cb, sb = cb_ref[pl.ds(base, 1), :], sb_ref[pl.ds(base, 1), :]
    cr, sr = cr_ref[...], sr_ref[...]
    cosine[...] = cb * cr - sb * sr
    turned = sb * cr + cb * sr
    sine[...] = jnp.where(first, -turned, turned)

    def rotate(x):
        swapped = jnp.where(first, pltpu.roll(x, 96, 1), pltpu.roll(x, 32, 1))
        return x * cosine[...] + swapped * sine[...]

    def project_k(half):
        keys = jnp.dot(tok[...], wk[half], preferred_element_type=F32).astype(BF).astype(F32)
        keys = rotate(keys)
        keys = (keys, pltpu.roll(keys, 64, 1))
        for e in range(2):
            for j in range(4):
                low = keys[e][j * 64 : j * 64 + 32]
                high = keys[1 - e][j * 64 + 32 : j * 64 + 64]
                k_own[2 * half + e, j] = jnp.where(left_half, low, high).astype(BF)

    def project_v(half):
        values = jnp.dot(tok[...], wv[half], preferred_element_type=F32).T
        values = [values[:, i * 128 : i * 128 + 128] for i in range(2)]
        values = [(x, pltpu.roll(x, 64, 1)) for x in values]
        for e in range(2):
            for j in range(4):
                pair = values[j // 2]
                low = pair[j % 2][e * 64 : e * 64 + 32]
                high = pair[1 - j % 2][e * 64 + 32 : e * 64 + 64]
                v_own[2 * half + e, j] = jnp.where(left_half, low, high).astype(BF)

    def project_q(half):
        tokens = tok[...]
        full = jnp.dot(tokens, wq[half], preferred_element_type=F32)
        for n in range(4):
            x = full[:, n * 128 : n * 128 + 128].astype(BF).astype(F32)
            qs[2 * half + n // 2, :, (n % 2) * 128 : (n % 2) * 128 + 128] = rotate(x).astype(BF)

    for load in loads[:3]:
        load.wait()
    project_k(t)
    project_v(t)

    pl.semaphore_wait(barrier, len(peers))

    halves = [
        remote(wk.at[t], wk.at[t], w_send.at[0], w_recv.at[0], kv, other),
        remote(wv.at[t], wv.at[t], w_send.at[1], w_recv.at[1], kv, other),
        remote(wq.at[t], wq.at[t], w_send.at[2], w_recv.at[2], kv, other),
        remote(wo_hbm, wo.at[t], w_send.at[3], w_recv.at[3], kv, other),
    ]

    def to_owner(own, every, send, recv, head):
        return remote(
            own.at[head], every.at[chunk(z, y)], send.at[head], recv.at[y], z * NY + head, t
        )

    def key_to_owner(head):
        return to_owner(k_own, k_all, ky_send, ky_recv, head)

    def value_to_owner(head):
        return to_owner(v_own, v_all, vy_send, vy_recv, head)

    def send_heads(make, half):
        for e in range(2):
            head = 2 * half + e

            @pl.when(head != y)
            def _():
                make(head).start()

    def ring(every, up_send, up_recv, dn_send, dn_recv, pt_send, pt_recv):
        def place(zz, k):
            return every.at[chunk(zz, row_chip(k))]

        def up(s, k, src=None):
            spot = place(lax.rem(z + NZ - s, NZ), k)
            src = spot if src is None else src
            return remote(src, spot, up_send.at[s, k], up_recv.at[s, k], z_up, t)

        def down(s, k, src=None):
            spot = place(lax.rem(z + s, NZ), k)
            src = spot if src is None else src
            return remote(src, spot, dn_send.at[s, k], dn_recv.at[s, k], z_dn, t)

        def partner(rel, k, src=None):
            spot = place(lax.rem(z + rel, NZ), k)
            src = spot if src is None else src
            return remote(src, spot, pt_send.at[rel, k], pt_recv.at[rel, k], kv, other)

        return up, down, partner

    k_ring = ring(k_all, k_up_send, k_up_recv, k_dn_send, k_dn_recv, k_pt_send, k_pt_recv)
    v_ring = ring(v_all, v_up_send, v_up_recv, v_dn_send, v_dn_recv, v_pt_send, v_pt_recv)

    def begin(group, k, src=None):
        up, down, partner = group
        up(0, k, src).start()
        down(0, k, src).start()
        partner(0, k, src).start()

    def step(group, s, k):
        up, down, partner = group
        if s < NZ // 2:
            turn = s == NZ // 2 - 1
            up(s - 1, k).wait_recv()
            if not turn:
                up(s, k).start()
            else:
                pl.when(k < 2)(lambda: up(s, k).start())
            partner(NZ - s, k).start()
            down(s - 1, k).wait_recv()
            if not turn:
                down(s, k).start()
            else:
                pl.when(k >= 2)(lambda: down(s, k).start())
            partner(s, k).start()
        else:
            pl.when(k < 2)(lambda: up(s - 1, k).wait_recv())
            pl.when(k >= 2)(lambda: down(s - 1, k).wait_recv())
            partner(s, k).start()

    for copy in halves[:2]:
        copy.start()
    ready = y // 2 == t
    pl.when(ready)(lambda: begin(k_ring, 0, k_own.at[y]))
    send_heads(key_to_owner, t)
    picks = [
        remote(ch_hbm, ch_all.at[NY - k], c_send.at[k], c_recv.at[NY - k], row_peer(k), t)
        for k in range(1, NY)
    ]
    loads[3].wait()
    for copy in halves[2:] + picks:
        copy.start()
    halves[0].wait_recv()
    project_k(other)
    send_heads(key_to_owner, other)

    mine = [
        pltpu.make_async_copy(k_own.at[y], k_all.at[chunk(z, y)], load_sem.at[5]),
        pltpu.make_async_copy(v_own.at[y], v_all.at[chunk(z, y)], load_sem.at[7]),
    ]
    pl.when(jnp.logical_not(ready))(lambda: begin(k_ring, 0, k_own.at[y]))
    send_heads(value_to_owner, t)
    halves[1].wait_recv()
    project_v(other)
    send_heads(value_to_owner, other)
    begin(v_ring, 0, v_own.at[y])
    for copy in mine:
        copy.start()

    def from_row(every, own, send, recv, k):
        remote(
            own.at[0], every.at[chunk(z, row_chip(k))], send.at[0], recv.at[row_chip(k)],
            row_peer(k), t,
        ).wait_recv()

    for k in (1, 3, 2):
        from_row(k_all, k_own, ky_send, ky_recv, k)
        begin(k_ring, k)
    for copy in mine:
        copy.wait()
    for k in (1, 3, 2):
        from_row(v_all, v_own, vy_send, vy_recv, k)
        begin(v_ring, k)
    project_q(t)
    halves[2].wait_recv()
    project_q(other)
    own_q = pltpu.make_async_copy(qs.at[y], q_all.at[0], load_sem.at[6])
    own_q.start()
    queries = [None] * NY
    for k in (2, 1, 3):
        queries[NY - k] = remote(
            qs.at[row_chip(k)], q_all.at[NY - k], q_send.at[k], q_recv.at[NY - k],
            row_peer(k), t,
        )
        queries[NY - k].start()

    for copy in picks:
        copy.wait_recv()
    own_picks.wait()
    to_smem = pltpu.make_async_copy(ch_all, ch_smem, load_sem.at[13])
    to_smem.start()

    order = (0, 1, 3, 2)
    for s in range(1, NZ // 2 + 1):
        for k in order:
            step(k_ring, s, k)
        if s < NZ // 2:
            for k in order:
                step(v_ring, s, k)

    to_smem.wait()
    own_q.wait()
    for k in range(1, NY):
        queries[k].wait_recv()
    for rel in range(NZ):
        for k in range(NY):
            k_ring[2](rel, k).wait_recv()

    key_pos = lax.broadcasted_iota(jnp.int32, (BLK, 4 * BLK), 0)
    query_pos = lax.rem(lax.broadcasted_iota(jnp.int32, (BLK, 4 * BLK), 1), BLK)
    causal = key_pos <= query_pos
    half_blk = BLK // 2

    def own_block(k, jb):
        return (z * NY + row_chip(k)) * 8 + t * 4 + jb

    def gather_keys(k, jb):
        bias = []
        for j in range(PICK + 1):
            if j < PICK:
                pick = ch_smem[k, t * 4 + jb, j]
                bias.append(jnp.where(pick < 0, NEGATIVE, 0.0).astype(F32))
                block = k_all[jnp.maximum(pick, 0)]
            else:
                block = k_all[own_block(k, jb)]
            nothing = jnp.zeros_like(block)
            u, row = jb % 2, j * BLK
            kg[u, row : row + half_blk, :] = jnp.where(left_half, block, nothing)
            kg[u, row + half_blk : row + BLK, :] = jnp.where(left_half, nothing, block)
        return bias

    def load_queries(k, jb):
        heads = []
        for n in range(2):
            x = q_all[k, jb * BLK : jb * BLK + BLK, n * 128 : n * 128 + 128].astype(F32)
            swapped = pltpu.roll(x, 64, 1)
            heads += [jnp.where(left, x, swapped), jnp.where(left, swapped, x)]
        return jnp.concatenate(heads, axis=0).astype(BF)

    def eight(x, op):
        return op(x.reshape(BLK // 8, 8, 4 * BLK), axis=0)

    def score(u, half, q2, bias):
        span = 8 * BLK
        part = lax.dot_general(
            kg[u, half * span : half * span + span, :], q2, (((1,), (1,)), ((), ())),
            preferred_element_type=F32,
        )
        top = None
        for i in range(8):
            j = half * 8 + i
            block = part[i * BLK : i * BLK + BLK, :]
            if j == PICK:
                block = jnp.where(causal, block, NEGATIVE)
            scores[u, j * BLK : j * BLK + BLK, :] = block
            here = eight(block, jnp.max)
            here = here if j == PICK else here + bias[j]
            top = here if top is None else jnp.maximum(top, here)
        return top

    def softmax(state, half):
        k, jb, top, bias, total = state
        for j in range(half * 8, half * 8 + 8):
            shift = top if j == PICK else top - bias[j]
            p = jnp.exp2((scores[jb % 2, j * BLK : j * BLK + BLK, :] - shift) * EXPONENT)
            part = eight(p, jnp.sum)
            total = part if total is None else total + part
            probs[jb, j * BLK : j * BLK + BLK, :] = p.astype(BF)
        if half == 1:
            total = jnp.sum(total, axis=0, keepdims=True)
            inverse[k, pl.ds(jb, 1), :] = 1.0 / total
            logsum = top * HEAD_DIM**-0.5 + jnp.log(total)
            for h in range(4):
                ls_out[k, pl.ds(h, 1), jb * BLK : jb * BLK + BLK] = logsum[:, h * BLK : h * BLK + BLK]
        return k, jb, top, bias, total

    def weigh(k):
        state = None
        for jb in range(4):
            bias = gather_keys(k, jb)
            q2 = load_queries(k, jb)
            tops = []
            for half in range(2):
                tops.append(score(jb % 2, half, q2, bias))
                if state is not None:
                    state = softmax(state, half)
            top = jnp.max(jnp.maximum(*tops), axis=0, keepdims=True)
            state = (k, jb, top, bias, None)
        for half in range(2):
            state = softmax(state, half)

    def gather_values(k, jb):
        previous = None
        for j in range(PICK + 1):
            if j < PICK:
                block = v_all[jnp.maximum(ch_smem[k, t * 4 + jb, j], 0)]
            else:
                block = v_all[own_block(k, jb)]
            block = block.astype(F32)
            if j % 2 == 1:
                low = jnp.where(left_half, previous, pltpu.roll(block, 64, 1))
                high = jnp.where(left_half, pltpu.roll(previous, 64, 1), block)
                columns = slice((j // 2) * 128, (j // 2) * 128 + 128)
                vt[jb, :half_blk, columns] = low.astype(BF)
                vt[jb, half_blk:, columns] = high.astype(BF)
            previous = block

    def combine(k):
        for jb in range(4):
            gather_values(k, jb)
        mixed = [
            jnp.dot(vt[jb], probs[jb], preferred_element_type=F32) for jb in range(4)
        ]
        for jb in range(4):
            turned_back = (mixed[jb] * inverse[k, pl.ds(jb, 1), :]).T
            parts = [turned_back[h * BLK : h * BLK + BLK] for h in range(4)]
            att_out[k, jb * BLK : jb * BLK + BLK, :] = jnp.concatenate(parts, axis=1).astype(BF)

    to_self = y // 2 == t
    slot = (lax.rem(y, 2), t)

    def log_piece(k):
        return remote(
            ls_out.at[k], ls_all.at[slot], l_send.at[k], l_recv.at[slot], row_peer(k), y // 2
        )

    def give_back(k):
        return remote(
            att_out.at[k], att_all.at[NY - k], a_send.at[k], a_recv.at[NY - k], row_peer(k), t
        )

    @pl.loop(0, NY)
    def _(i):
        k = lax.rem(i + 1 - t * (2 * i - 2), NY)
        weigh(k)

        @pl.when(i == 0)
        def _():
            for r in order:
                step(v_ring, NZ // 2, r)
            for rel in range(NZ):
                for r in range(NY):
                    v_ring[2](rel, r).wait_recv()

        combine(k)

        @pl.when(k > 0)
        def _():
            give_back(k).start()
            log_piece(k).start()

    pl.when(jnp.logical_not(to_self))(lambda: log_piece(0).start())

    @pl.when(to_self)
    def _():
        ls_all[slot] = ls_out[0]

    loads[4].wait()
    halves[3].wait_recv()
    def part(k):
        ys = y if k is None else row_chip(k)
        weights = wo[ys // 2, pl.ds(pl.multiple_of(lax.rem(ys, 2) * 256, 256), 256), :]
        piece = att_out[0] if k is None else att_all[k]
        return jnp.dot(piece, weights, preferred_element_type=F32)

    early, late = 3 - 2 * t, 1 + 2 * t
    for k in (early, 2):
        give_back(NY - k).wait_recv()
    acc[...] = part(None) + part(early) + part(2)
    give_back(NY - late).wait_recv()
    projected = acc[...] + part(late)
    square = jnp.mean(projected * projected, axis=-1, keepdims=True)
    out_ref[...] = (projected * lax.rsqrt(square + EPSILON)).astype(BF)

    for ys in range(2):
        for tt in range(2):
            @pl.when(jnp.logical_not((t * 2 + ys == y) & (t == tt)))
            def _():
                remote(
                    ls_out.at[0], ls_all.at[ys, tt], l_send.at[0], l_recv.at[ys, tt], kv, other
                ).wait_recv()

            ls_ref[ys * 4 : ys * 4 + 4, tt * 4 * BLK : tt * 4 * BLK + 4 * BLK] = ls_all[ys, tt]
    for k in range(1, NY):
        log_piece(k).wait_send()
    pl.when(jnp.logical_not(to_self))(lambda: log_piece(0).wait_send())
    for k in range(1, NY):
        key_to_owner(row_chip(k)).wait_send()
        value_to_owner(row_chip(k)).wait_send()
        queries[k].wait_send()
        give_back(k).wait_send()
    for copy in halves + picks:
        copy.wait_send()
    for up, down, partner in (k_ring, v_ring):
        for k in range(NY):
            for s in range(NZ // 2):
                if s < NZ // 2 - 1 or k < 2:
                    up(s, k).wait_send()
                if s < NZ // 2 - 1 or k >= 2:
                    down(s, k).wait_send()
            for rel in range(NZ):
                partner(rel, k).wait_send()


def shards(tokens, w_query, w_key, w_value, w_out, chosen):
    rows, width = tokens.shape[1:]
    tables = rotary_tables(rows, 2 * NY * NZ)
    any_space = pl.BlockSpec(memory_space=pl.ANY)
    vmem = pl.BlockSpec(memory_space=pltpu.VMEM)
    dma = pltpu.SemaphoreType.DMA
    out, logs = pl.pallas_call(
        kernel,
        out_shape=(
            jax.ShapeDtypeStruct((rows, width), BF),
            jax.ShapeDtypeStruct((8, 2 * rows), F32),
        ),
        in_specs=[any_space] * 10,
        out_specs=(vmem, vmem),
        scratch_shapes=[
            pltpu.VMEM((rows, 128), F32),
            pltpu.VMEM((rows, 128), F32),
            pltpu.VMEM((2 * NY * NZ, 128), F32),
            pltpu.VMEM((2 * NY * NZ, 128), F32),
            pltpu.VMEM((rows, width), BF),
            pltpu.VMEM((2,) + w_query.shape, BF),
            pltpu.VMEM((2,) + w_key.shape, BF),
            pltpu.VMEM((2,) + w_value.shape, BF),
            pltpu.VMEM((2,) + w_out.shape, BF),
            pltpu.VMEM((rows, 128), F32),
            pltpu.VMEM((rows, 128), F32),
            pltpu.VMEM((4, 4, BLK // 2, 128), BF),
            pltpu.VMEM((4, 4, BLK // 2, 128), BF),
            pltpu.VMEM((NZ * NY * 8, BLK // 2, 128), BF),
            pltpu.VMEM((NZ * NY * 8, BLK // 2, 128), BF),
            pltpu.VMEM((NY, rows, 256), BF),
            pltpu.VMEM((NY, rows, 256), BF),
            pltpu.VMEM((NY, 8, PICK), jnp.int32),
            pltpu.SMEM((NY, 8, PICK), jnp.int32),
            pltpu.VMEM((2, (PICK + 1) * BLK, 128), BF),
            pltpu.VMEM((4, BLK, (PICK + 1) * BLK), BF),
            pltpu.VMEM((2, (PICK + 1) * BLK, 4 * BLK), F32),
            pltpu.VMEM((4, (PICK + 1) * BLK, 4 * BLK), BF),
            pltpu.VMEM((NY, 4, 4 * BLK), F32),
            pltpu.VMEM((NY, rows, 256), BF),
            pltpu.VMEM((NY, rows, 256), BF),
            pltpu.VMEM((NY, 4, 4 * BLK), F32),
            pltpu.VMEM((2, 2, 4, 4 * BLK), F32),
            pltpu.VMEM((rows, width), F32),
            dma((14,)), dma((4,)), dma((4,)), dma((4,)), dma((4,)), dma((4,)), dma((4,)),
            dma((4, 4)), dma((4, 4)), dma((4, 4)), dma((4, 4)), dma((NZ, 4)), dma((NZ, 4)),
            dma((4, 4)), dma((4, 4)), dma((4, 4)), dma((4, 4)), dma((NZ, 4)), dma((NZ, 4)),
            dma((4,)), dma((4,)), dma((4,)), dma((4,)),
            dma((4,)), dma((4,)), dma((4,)), dma((2, 2)),
        ],
        compiler_params=pltpu.CompilerParams(
            collective_id=0, has_side_effects=True, vmem_limit_bytes=67_000_000
        ),
    )(*tables, tokens[0], w_query, w_key, w_value, w_out, chosen[0])
    return out[None], logs.T[None]


def solution(mesh):
    placed = (
        P("dp", ("kv", "tp"), None),
        P(None, "tp"),
        P(None, "tp"),
        P(None, "tp"),
        P("tp", None),
        P("dp", "kv", None),
    )
    return jax.shard_map(
        shards,
        mesh=mesh,
        in_specs=placed,
        out_specs=(P("dp", ("kv", "tp"), None), P("dp", "kv", "tp")),
        check_vma=False,
    )
```

```python
import math

import jax
import jax.numpy as jnp
import numpy as np
from jax import lax
from jax.experimental import pallas as pl
from jax.experimental.pallas import tpu as pltpu
from jax.sharding import PartitionSpec as P

HEAD_DIM = 64
BLK = 64
PICK = 15
THETA_BASE = 10000.0
NEGATIVE = -1e30
EPSILON = 1e-06
MESH = pl.DeviceIdType.MESH
BF = jnp.bfloat16
F32 = jnp.float32
EXPONENT = math.log2(math.e) / math.sqrt(HEAD_DIM)
NY = 4
NZ = 8


def rotary_tables(rows, bases):
    half = HEAD_DIM // 2
    freq = THETA_BASE ** (-np.arange(half, dtype=np.float64) / half)
    freq = np.tile(freq, 128 // half)[None, :]
    offset = np.arange(rows, dtype=np.float64)[:, None] * freq
    base = np.arange(bases, dtype=np.float64)[:, None] * rows * freq
    return [
        np.asarray(a, np.float32)
        for a in (np.cos(offset), np.sin(offset), np.cos(base), np.sin(base))
    ]


def kernel(
    cr_hbm, sr_hbm, cb_hbm, sb_hbm, tok_hbm, wq_hbm, wk_hbm, wv_hbm, wo_hbm, ch_hbm,
    out_ref, ls_ref,
    cr_ref, sr_ref, cb_ref, sb_ref, tok, wq, wk, wv, wo, cosine, sine, k_own, v_own,
    k_all, v_all, qs, q_all, ch_all, ch_smem, kg, vt, scores, probs, inverse,
    att_out, att_all, ls_out, ls_all, acc,
    load_sem, w_send, w_recv, ky_send, ky_recv, vy_send, vy_recv,
    k_up_send, k_up_recv, k_dn_send, k_dn_recv, k_pt_send, k_pt_recv,
    v_up_send, v_up_recv, v_dn_send, v_dn_recv, v_pt_send, v_pt_recv,
    q_send, q_recv, c_send, c_recv, a_send, a_recv, l_send, l_recv,
):
    kv = lax.axis_index("kv")
    t = lax.axis_index("tp")
    z, y = kv // NY, kv % NY
    other = 1 - t

    def row_chip(k):
        return lax.rem(y + k, NY)

    def row_peer(k):
        return z * NY + row_chip(k)

    def chunk(zz, yy):
        return pl.ds(((zz * NY + yy) * 2 + t) * 4, 4)

    def remote(src, dst, send, recv, kv_to, tp_to):
        return pltpu.make_async_remote_copy(
            src_ref=src, dst_ref=dst, send_sem=send, recv_sem=recv,
            device_id={"kv": kv_to, "tp": tp_to}, device_id_type=MESH,
        )

    barrier = pltpu.get_barrier_semaphore()
    peers = [(row_peer(k), tt) for k in range(1, NY) for tt in (t, other)]
    peers += [(kv, other)]
    z_up = lax.rem(z + 1, NZ) * NY + y
    z_dn = lax.rem(z + NZ - 1, NZ) * NY + y
    peers += [(z_up, t), (z_dn, t)]
    for kv_to, tp_to in peers:
        pl.semaphore_signal(
            barrier, inc=1, device_id={"kv": kv_to, "tp": tp_to}, device_id_type=MESH
        )

    loads = [
        pltpu.make_async_copy(tok_hbm, tok, load_sem.at[0]),
        pltpu.make_async_copy(wk_hbm, wk.at[t], load_sem.at[1]),
        pltpu.make_async_copy(wv_hbm, wv.at[t], load_sem.at[2]),
        pltpu.make_async_copy(wq_hbm, wq.at[t], load_sem.at[3]),
        pltpu.make_async_copy(wo_hbm, wo.at[t], load_sem.at[4]),
    ]
    tables = [
        pltpu.make_async_copy(a, b, load_sem.at[8 + i])
        for i, (a, b) in enumerate(
            ((cr_hbm, cr_ref), (sr_hbm, sr_ref), (cb_hbm, cb_ref), (sb_hbm, sb_ref))
        )
    ]
    own_picks = pltpu.make_async_copy(ch_hbm, ch_all.at[0], load_sem.at[12])
    for load in loads[:3] + tables + loads[3:] + [own_picks]:
        load.start()

    left = lax.broadcasted_iota(jnp.int32, (BLK, 128), 1) < BLK
    left_half = lax.broadcasted_iota(jnp.int32, (BLK // 2, 128), 1) < BLK
    wide = lax.broadcasted_iota(jnp.int32, (4 * BLK, 128), 1)
    first = lax.rem(wide, HEAD_DIM) < HEAD_DIM // 2

    for load in tables:
        load.wait()
    base = kv * 2 + t
    cb, sb = cb_ref[pl.ds(base, 1), :], sb_ref[pl.ds(base, 1), :]
    cr, sr = cr_ref[...], sr_ref[...]
    cosine[...] = cb * cr - sb * sr
    turned = sb * cr + cb * sr
    sine[...] = jnp.where(first, -turned, turned)

    def rotate(x):
        swapped = jnp.where(first, pltpu.roll(x, 96, 1), pltpu.roll(x, 32, 1))
        return x * cosine[...] + swapped * sine[...]

    def project_k(half):
        keys = jnp.dot(tok[...], wk[half], preferred_element_type=F32).astype(BF).astype(F32)
        keys = rotate(keys)
        keys = (keys, pltpu.roll(keys, 64, 1))
        for e in range(2):
            for j in range(4):
                low = keys[e][j * 64 : j * 64 + 32]
                high = keys[1 - e][j * 64 + 32 : j * 64 + 64]
                k_own[2 * half + e, j] = jnp.where(left_half, low, high).astype(BF)

    def project_v(half):
        values = jnp.dot(tok[...], wv[half], preferred_element_type=F32).T
        values = [values[:, i * 128 : i * 128 + 128] for i in range(2)]
        values = [(x, pltpu.roll(x, 64, 1)) for x in values]
        for e in range(2):
            for j in range(4):
                pair = values[j // 2]
                low = pair[j % 2][e * 64 : e * 64 + 32]
                high = pair[1 - j % 2][e * 64 + 32 : e * 64 + 64]
                v_own[2 * half + e, j] = jnp.where(left_half, low, high).astype(BF)

    def project_q(half):
        tokens = tok[...]
        full = jnp.dot(tokens, wq[half], preferred_element_type=F32)
        for n in range(4):
            x = full[:, n * 128 : n * 128 + 128].astype(BF).astype(F32)
            qs[2 * half + n // 2, :, (n % 2) * 128 : (n % 2) * 128 + 128] = rotate(x).astype(BF)

    for load in loads[:3]:
        load.wait()
    project_k(t)
    project_v(t)

    pl.semaphore_wait(barrier, len(peers))

    halves = [
        remote(wk.at[t], wk.at[t], w_send.at[0], w_recv.at[0], kv, other),
        remote(wv.at[t], wv.at[t], w_send.at[1], w_recv.at[1], kv, other),
        remote(wq.at[t], wq.at[t], w_send.at[2], w_recv.at[2], kv, other),
        remote(wo_hbm, wo.at[t], w_send.at[3], w_recv.at[3], kv, other),
    ]

    def to_owner(own, every, send, recv, head):
        return remote(
            own.at[head], every.at[chunk(z, y)], send.at[head], recv.at[y], z * NY + head, t
        )

    def key_to_owner(head):
        return to_owner(k_own, k_all, ky_send, ky_recv, head)

    def value_to_owner(head):
        return to_owner(v_own, v_all, vy_send, vy_recv, head)

    def send_heads(make, half):
        for e in range(2):
            head = 2 * half + e

            @pl.when(head != y)
            def _():
                make(head).start()

    def ring(every, up_send, up_recv, dn_send, dn_recv, pt_send, pt_recv):
        def place(zz, k):
            return every.at[chunk(zz, row_chip(k))]

        def up(s, k, src=None):
            spot = place(lax.rem(z + NZ - s, NZ), k)
            src = spot if src is None else src
            return remote(src, spot, up_send.at[s, k], up_recv.at[s, k], z_up, t)

        def down(s, k, src=None):
            spot = place(lax.rem(z + s, NZ), k)
            src = spot if src is None else src
            return remote(src, spot, dn_send.at[s, k], dn_recv.at[s, k], z_dn, t)

        def partner(rel, k, src=None):
            spot = place(lax.rem(z + rel, NZ), k)
            src = spot if src is None else src
            return remote(src, spot, pt_send.at[rel, k], pt_recv.at[rel, k], kv, other)

        return up, down, partner

    k_ring = ring(k_all, k_up_send, k_up_recv, k_dn_send, k_dn_recv, k_pt_send, k_pt_recv)
    v_ring = ring(v_all, v_up_send, v_up_recv, v_dn_send, v_dn_recv, v_pt_send, v_pt_recv)

    def begin(group, k, src=None):
        up, down, partner = group
        up(0, k, src).start()
        down(0, k, src).start()
        partner(0, k, src).start()

    def step(group, s, k):
        up, down, partner = group
        if s < NZ // 2:
            turn = s == NZ // 2 - 1
            up(s - 1, k).wait_recv()
            if not turn:
                up(s, k).start()
            else:
                pl.when(k < 2)(lambda: up(s, k).start())
            partner(NZ - s, k).start()
            down(s - 1, k).wait_recv()
            if not turn:
                down(s, k).start()
            else:
                pl.when(k >= 2)(lambda: down(s, k).start())
            partner(s, k).start()
        else:
            pl.when(k < 2)(lambda: up(s - 1, k).wait_recv())
            pl.when(k >= 2)(lambda: down(s - 1, k).wait_recv())
            partner(s, k).start()

    for copy in halves[:2]:
        copy.start()
    ready = y // 2 == t
    pl.when(ready)(lambda: begin(k_ring, 0, k_own.at[y]))
    send_heads(key_to_owner, t)
    picks = [
        remote(ch_hbm, ch_all.at[NY - k], c_send.at[k], c_recv.at[NY - k], row_peer(k), t)
        for k in range(1, NY)
    ]
    loads[3].wait()
    for copy in halves[2:] + picks:
        copy.start()
    project_q(t)
    halves[0].wait_recv()
    project_k(other)
    send_heads(key_to_owner, other)

    mine = [
        pltpu.make_async_copy(k_own.at[y], k_all.at[chunk(z, y)], load_sem.at[5]),
        pltpu.make_async_copy(v_own.at[y], v_all.at[chunk(z, y)], load_sem.at[7]),
    ]
    pl.when(jnp.logical_not(ready))(lambda: begin(k_ring, 0, k_own.at[y]))
    send_heads(value_to_owner, t)
    halves[1].wait_recv()
    project_v(other)
    send_heads(value_to_owner, other)
    begin(v_ring, 0, v_own.at[y])
    for copy in mine:
        copy.start()

    def from_row(every, own, send, recv, k):
        remote(
            own.at[0], every.at[chunk(z, row_chip(k))], send.at[0], recv.at[row_chip(k)],
            row_peer(k), t,
        ).wait_recv()

    for k in (1, 3, 2):
        from_row(k_all, k_own, ky_send, ky_recv, k)
        begin(k_ring, k)
    for copy in mine:
        copy.wait()
    for k in (1, 3, 2):
        from_row(v_all, v_own, vy_send, vy_recv, k)
        begin(v_ring, k)
    halves[2].wait_recv()
    project_q(other)
    own_q = pltpu.make_async_copy(qs.at[y], q_all.at[0], load_sem.at[6])
    own_q.start()
    queries = [None] * NY
    for k in (2, 1, 3):
        queries[NY - k] = remote(
            qs.at[row_chip(k)], q_all.at[NY - k], q_send.at[k], q_recv.at[NY - k],
            row_peer(k), t,
        )
        queries[NY - k].start()

    for copy in picks:
        copy.wait_recv()
    own_picks.wait()
    to_smem = pltpu.make_async_copy(ch_all, ch_smem, load_sem.at[13])
    to_smem.start()

    order = (0, 1, 3, 2)
    for s in range(1, NZ // 2 + 1):
        for k in order:
            step(k_ring, s, k)
        if s < NZ // 2:
            for k in order:
                step(v_ring, s, k)

    to_smem.wait()
    own_q.wait()
    for k in range(1, NY):
        queries[k].wait_recv()
    for rel in range(NZ):
        for k in range(NY):
            k_ring[2](rel, k).wait_recv()

    key_pos = lax.broadcasted_iota(jnp.int32, (BLK, 4 * BLK), 0)
    query_pos = lax.rem(lax.broadcasted_iota(jnp.int32, (BLK, 4 * BLK), 1), BLK)
    causal = key_pos <= query_pos
    half_blk = BLK // 2

    def own_block(k, jb):
        return (z * NY + row_chip(k)) * 8 + t * 4 + jb

    def gather_keys(k, jb):
        bias = []
        for j in range(PICK + 1):
            if j < PICK:
                pick = ch_smem[k, t * 4 + jb, j]
                bias.append(jnp.where(pick < 0, NEGATIVE, 0.0).astype(F32))
                block = k_all[jnp.maximum(pick, 0)]
            else:
                block = k_all[own_block(k, jb)]
            nothing = jnp.zeros_like(block)
            u, row = jb % 2, j * BLK
            kg[u, row : row + half_blk, :] = jnp.where(left_half, block, nothing)
            kg[u, row + half_blk : row + BLK, :] = jnp.where(left_half, nothing, block)
        return bias

    def load_queries(k, jb):
        heads = []
        for n in range(2):
            x = q_all[k, jb * BLK : jb * BLK + BLK, n * 128 : n * 128 + 128].astype(F32)
            swapped = pltpu.roll(x, 64, 1)
            heads += [jnp.where(left, x, swapped), jnp.where(left, swapped, x)]
        return jnp.concatenate(heads, axis=0).astype(BF)

    def eight(x, op):
        return op(x.reshape(BLK // 8, 8, 4 * BLK), axis=0)

    def score(u, half, q2, bias):
        span = 8 * BLK
        part = lax.dot_general(
            kg[u, half * span : half * span + span, :], q2, (((1,), (1,)), ((), ())),
            preferred_element_type=F32,
        )
        top = None
        for i in range(8):
            j = half * 8 + i
            block = part[i * BLK : i * BLK + BLK, :]
            if j == PICK:
                block = jnp.where(causal, block, NEGATIVE)
            scores[u, j * BLK : j * BLK + BLK, :] = block
            here = eight(block, jnp.max)
            here = here if j == PICK else here + bias[j]
            top = here if top is None else jnp.maximum(top, here)
        return top

    def softmax(state, half):
        k, jb, top, bias, total = state
        for j in range(half * 8, half * 8 + 8):
            shift = top if j == PICK else top - bias[j]
            p = jnp.exp2((scores[jb % 2, j * BLK : j * BLK + BLK, :] - shift) * EXPONENT)
            part = eight(p, jnp.sum)
            total = part if total is None else total + part
            probs[jb, j * BLK : j * BLK + BLK, :] = p.astype(BF)
        if half == 1:
            total = jnp.sum(total, axis=0, keepdims=True)
            inverse[k, pl.ds(jb, 1), :] = 1.0 / total
            logsum = top * HEAD_DIM**-0.5 + jnp.log(total)
            for h in range(4):
                ls_out[k, pl.ds(h, 1), jb * BLK : jb * BLK + BLK] = logsum[:, h * BLK : h * BLK + BLK]
        return k, jb, top, bias, total

    def weigh(k):
        state = None
        for jb in range(4):
            bias = gather_keys(k, jb)
            q2 = load_queries(k, jb)
            tops = []
            for half in range(2):
                tops.append(score(jb % 2, half, q2, bias))
                if state is not None:
                    state = softmax(state, half)
            top = jnp.max(jnp.maximum(*tops), axis=0, keepdims=True)
            state = (k, jb, top, bias, None)
        for half in range(2):
            state = softmax(state, half)

    def gather_values(k, jb):
        previous = None
        for j in range(PICK + 1):
            if j < PICK:
                block = v_all[jnp.maximum(ch_smem[k, t * 4 + jb, j], 0)]
            else:
                block = v_all[own_block(k, jb)]
            block = block.astype(F32)
            if j % 2 == 1:
                low = jnp.where(left_half, previous, pltpu.roll(block, 64, 1))
                high = jnp.where(left_half, pltpu.roll(previous, 64, 1), block)
                columns = slice((j // 2) * 128, (j // 2) * 128 + 128)
                vt[jb, :half_blk, columns] = low.astype(BF)
                vt[jb, half_blk:, columns] = high.astype(BF)
            previous = block

    def combine(k):
        for jb in range(4):
            gather_values(k, jb)
        mixed = [
            jnp.dot(vt[jb], probs[jb], preferred_element_type=F32) for jb in range(4)
        ]
        for jb in range(4):
            turned_back = (mixed[jb] * inverse[k, pl.ds(jb, 1), :]).T
            parts = [turned_back[h * BLK : h * BLK + BLK] for h in range(4)]
            att_out[k, jb * BLK : jb * BLK + BLK, :] = jnp.concatenate(parts, axis=1).astype(BF)

    to_self = y // 2 == t
    slot = (lax.rem(y, 2), t)

    def log_piece(k):
        return remote(
            ls_out.at[k], ls_all.at[slot], l_send.at[k], l_recv.at[slot], row_peer(k), y // 2
        )

    def give_back(k):
        return remote(
            att_out.at[k], att_all.at[NY - k], a_send.at[k], a_recv.at[NY - k], row_peer(k), t
        )

    @pl.loop(0, NY)
    def _(i):
        k = lax.rem(i + 1, NY)
        weigh(k)

        @pl.when(i == 0)
        def _():
            for r in order:
                step(v_ring, NZ // 2, r)
            for rel in range(NZ):
                for r in range(NY):
                    v_ring[2](rel, r).wait_recv()

        combine(k)

        @pl.when(k > 0)
        def _():
            give_back(k).start()
            log_piece(k).start()

    pl.when(jnp.logical_not(to_self))(lambda: log_piece(0).start())

    @pl.when(to_self)
    def _():
        ls_all[slot] = ls_out[0]

    loads[4].wait()
    halves[3].wait_recv()
    def part(k):
        ys = row_chip(k)
        weights = wo[ys // 2, pl.ds(pl.multiple_of(lax.rem(ys, 2) * 256, 256), 256), :]
        piece = att_out[0] if k == 0 else att_all[k]
        return jnp.dot(piece, weights, preferred_element_type=F32)

    for k in (1, 2):
        give_back(k).wait_recv()
    acc[...] = part(0) + part(3) + part(2)
    give_back(3).wait_recv()
    projected = acc[...] + part(1)
    square = jnp.mean(projected * projected, axis=-1, keepdims=True)
    out_ref[...] = (projected * lax.rsqrt(square + EPSILON)).astype(BF)

    for ys in range(2):
        for tt in range(2):
            @pl.when(jnp.logical_not((t * 2 + ys == y) & (t == tt)))
            def _():
                remote(
                    ls_out.at[0], ls_all.at[ys, tt], l_send.at[0], l_recv.at[ys, tt], kv, other
                ).wait_recv()

            ls_ref[ys * 4 : ys * 4 + 4, tt * 4 * BLK : tt * 4 * BLK + 4 * BLK] = ls_all[ys, tt]
    for k in range(1, NY):
        log_piece(k).wait_send()
    pl.when(jnp.logical_not(to_self))(lambda: log_piece(0).wait_send())
    for k in range(1, NY):
        key_to_owner(row_chip(k)).wait_send()
        value_to_owner(row_chip(k)).wait_send()
        queries[k].wait_send()
        give_back(k).wait_send()
    for copy in halves + picks:
        copy.wait_send()
    for up, down, partner in (k_ring, v_ring):
        for k in range(NY):
            for s in range(NZ // 2):
                if s < NZ // 2 - 1 or k < 2:
                    up(s, k).wait_send()
                if s < NZ // 2 - 1 or k >= 2:
                    down(s, k).wait_send()
            for rel in range(NZ):
                partner(rel, k).wait_send()


def shards(tokens, w_query, w_key, w_value, w_out, chosen):
    rows, width = tokens.shape[1:]
    tables = rotary_tables(rows, 2 * NY * NZ)
    any_space = pl.BlockSpec(memory_space=pl.ANY)
    vmem = pl.BlockSpec(memory_space=pltpu.VMEM)
    dma = pltpu.SemaphoreType.DMA
    out, logs = pl.pallas_call(
        kernel,
        out_shape=(
            jax.ShapeDtypeStruct((rows, width), BF),
            jax.ShapeDtypeStruct((8, 2 * rows), F32),
        ),
        in_specs=[any_space] * 10,
        out_specs=(vmem, vmem),
        scratch_shapes=[
            pltpu.VMEM((rows, 128), F32),
            pltpu.VMEM((rows, 128), F32),
            pltpu.VMEM((2 * NY * NZ, 128), F32),
            pltpu.VMEM((2 * NY * NZ, 128), F32),
            pltpu.VMEM((rows, width), BF),
            pltpu.VMEM((2,) + w_query.shape, BF),
            pltpu.VMEM((2,) + w_key.shape, BF),
            pltpu.VMEM((2,) + w_value.shape, BF),
            pltpu.VMEM((2,) + w_out.shape, BF),
            pltpu.VMEM((rows, 128), F32),
            pltpu.VMEM((rows, 128), F32),
            pltpu.VMEM((4, 4, BLK // 2, 128), BF),
            pltpu.VMEM((4, 4, BLK // 2, 128), BF),
            pltpu.VMEM((NZ * NY * 8, BLK // 2, 128), BF),
            pltpu.VMEM((NZ * NY * 8, BLK // 2, 128), BF),
            pltpu.VMEM((NY, rows, 256), BF),
            pltpu.VMEM((NY, rows, 256), BF),
            pltpu.VMEM((NY, 8, PICK), jnp.int32),
            pltpu.SMEM((NY, 8, PICK), jnp.int32),
            pltpu.VMEM((2, (PICK + 1) * BLK, 128), BF),
            pltpu.VMEM((4, BLK, (PICK + 1) * BLK), BF),
            pltpu.VMEM((2, (PICK + 1) * BLK, 4 * BLK), F32),
            pltpu.VMEM((4, (PICK + 1) * BLK, 4 * BLK), BF),
            pltpu.VMEM((NY, 4, 4 * BLK), F32),
            pltpu.VMEM((NY, rows, 256), BF),
            pltpu.VMEM((NY, rows, 256), BF),
            pltpu.VMEM((NY, 4, 4 * BLK), F32),
            pltpu.VMEM((2, 2, 4, 4 * BLK), F32),
            pltpu.VMEM((rows, width), F32),
            dma((14,)), dma((4,)), dma((4,)), dma((4,)), dma((4,)), dma((4,)), dma((4,)),
            dma((4, 4)), dma((4, 4)), dma((4, 4)), dma((4, 4)), dma((NZ, 4)), dma((NZ, 4)),
            dma((4, 4)), dma((4, 4)), dma((4, 4)), dma((4, 4)), dma((NZ, 4)), dma((NZ, 4)),
            dma((4,)), dma((4,)), dma((4,)), dma((4,)),
            dma((4,)), dma((4,)), dma((4,)), dma((2, 2)),
        ],
        compiler_params=pltpu.CompilerParams(
            collective_id=0, has_side_effects=True, vmem_limit_bytes=67_000_000
        ),
    )(*tables, tokens[0], w_query, w_key, w_value, w_out, chosen[0])
    return out[None], logs.T[None]


def solution(mesh):
    placed = (
        P("dp", ("kv", "tp"), None),
        P(None, "tp"),
        P(None, "tp"),
        P(None, "tp"),
        P("tp", None),
        P("dp", "kv", None),
    )
    return jax.shard_map(
        shards,
        mesh=mesh,
        in_specs=placed,
        out_specs=(P("dp", ("kv", "tp"), None), P("dp", "kv", "tp")),
        check_vma=False,
    )
```

```python
import math

import jax
import jax.numpy as jnp
import numpy as np
from jax import lax
from jax.experimental import pallas as pl
from jax.experimental.pallas import tpu as pltpu
from jax.sharding import PartitionSpec as P

HEAD_DIM = 64
BLK = 64
PICK = 15
THETA_BASE = 10000.0
NEGATIVE = -1e30
EPSILON = 1e-06
MESH = pl.DeviceIdType.MESH
BF = jnp.bfloat16
F32 = jnp.float32
EXPONENT = math.log2(math.e) / math.sqrt(HEAD_DIM)
NY = 4
NZ = 8


def rotary_tables(rows, bases):
    half = HEAD_DIM // 2
    freq = THETA_BASE ** (-np.arange(half, dtype=np.float64) / half)
    freq = np.tile(freq, 128 // half)[None, :]
    offset = np.arange(rows, dtype=np.float64)[:, None] * freq
    base = np.arange(bases, dtype=np.float64)[:, None] * rows * freq
    return [
        np.asarray(a, np.float32)
        for a in (np.cos(offset), np.sin(offset), np.cos(base), np.sin(base))
    ]


def kernel(
    cr_hbm, sr_hbm, cb_hbm, sb_hbm, tok_hbm, wq_hbm, wk_hbm, wv_hbm, wo_hbm, ch_hbm,
    out_ref, ls_ref,
    cr_ref, sr_ref, cb_ref, sb_ref, tok, wq, wk, wv, wo, cosine, sine, k_own, v_own,
    k_all, v_all, qs, q_all, ch_all, ch_smem, kg, vt, scores, probs, inverse,
    att_out, att_all, ls_out, ls_all, acc,
    load_sem, w_send, w_recv, ky_send, ky_recv, vy_send, vy_recv,
    k_up_send, k_up_recv, k_dn_send, k_dn_recv, k_pt_send, k_pt_recv,
    v_up_send, v_up_recv, v_dn_send, v_dn_recv, v_pt_send, v_pt_recv,
    q_send, q_recv, c_send, c_recv, a_send, a_recv, l_send, l_recv,
):
    kv = lax.axis_index("kv")
    t = lax.axis_index("tp")
    z, y = kv // NY, kv % NY
    other = 1 - t

    def row_chip(k):
        return lax.rem(y + k, NY)

    def row_peer(k):
        return z * NY + row_chip(k)

    def chunk(zz, yy):
        return pl.ds(((zz * NY + yy) * 2 + t) * 4, 4)

    def remote(src, dst, send, recv, kv_to, tp_to):
        return pltpu.make_async_remote_copy(
            src_ref=src, dst_ref=dst, send_sem=send, recv_sem=recv,
            device_id={"kv": kv_to, "tp": tp_to}, device_id_type=MESH,
        )

    loads = [
        pltpu.make_async_copy(tok_hbm, tok, load_sem.at[0]),
        pltpu.make_async_copy(wk_hbm, wk.at[t], load_sem.at[1]),
        pltpu.make_async_copy(wv_hbm, wv.at[t], load_sem.at[2]),
        pltpu.make_async_copy(wq_hbm, wq.at[t], load_sem.at[3]),
        pltpu.make_async_copy(wo_hbm, wo.at[t], load_sem.at[4]),
    ]
    tables = [
        pltpu.make_async_copy(a, b, load_sem.at[8 + i])
        for i, (a, b) in enumerate(
            ((cr_hbm, cr_ref), (sr_hbm, sr_ref), (cb_hbm, cb_ref), (sb_hbm, sb_ref))
        )
    ]
    own_picks = pltpu.make_async_copy(ch_hbm, ch_all.at[0], load_sem.at[12])
    for load in loads[:3] + tables + loads[3:] + [own_picks]:
        load.start()

    barrier = pltpu.get_barrier_semaphore()
    peers = [(row_peer(k), tt) for k in range(1, NY) for tt in (t, other)]
    peers += [(kv, other)]
    z_up = lax.rem(z + 1, NZ) * NY + y
    z_dn = lax.rem(z + NZ - 1, NZ) * NY + y
    peers += [(z_up, t), (z_dn, t)]
    for kv_to, tp_to in peers:
        pl.semaphore_signal(
            barrier, inc=1, device_id={"kv": kv_to, "tp": tp_to}, device_id_type=MESH
        )

    left = lax.broadcasted_iota(jnp.int32, (BLK, 128), 1) < BLK
    left_half = lax.broadcasted_iota(jnp.int32, (BLK // 2, 128), 1) < BLK
    wide = lax.broadcasted_iota(jnp.int32, (4 * BLK, 128), 1)
    first = lax.rem(wide, HEAD_DIM) < HEAD_DIM // 2

    for load in tables:
        load.wait()
    base = kv * 2 + t
    cb, sb = cb_ref[pl.ds(base, 1), :], sb_ref[pl.ds(base, 1), :]
    cr, sr = cr_ref[...], sr_ref[...]
    cosine[...] = cb * cr - sb * sr
    turned = sb * cr + cb * sr
    sine[...] = jnp.where(first, -turned, turned)

    def rotate(x):
        swapped = jnp.where(first, pltpu.roll(x, 96, 1), pltpu.roll(x, 32, 1))
        return x * cosine[...] + swapped * sine[...]

    def project_k(half):
        keys = jnp.dot(tok[...], wk[half], preferred_element_type=F32).astype(BF).astype(F32)
        keys = rotate(keys)
        keys = (keys, pltpu.roll(keys, 64, 1))
        for e in range(2):
            for j in range(4):
                low = keys[e][j * 64 : j * 64 + 32]
                high = keys[1 - e][j * 64 + 32 : j * 64 + 64]
                k_own[2 * half + e, j] = jnp.where(left_half, low, high).astype(BF)

    def project_v(half):
        values = jnp.dot(tok[...], wv[half], preferred_element_type=F32).T
        values = [values[:, i * 128 : i * 128 + 128] for i in range(2)]
        values = [(x, pltpu.roll(x, 64, 1)) for x in values]
        for e in range(2):
            for j in range(4):
                pair = values[j // 2]
                low = pair[j % 2][e * 64 : e * 64 + 32]
                high = pair[1 - j % 2][e * 64 + 32 : e * 64 + 64]
                v_own[2 * half + e, j] = jnp.where(left_half, low, high).astype(BF)

    def project_q(half):
        tokens = tok[...]
        full = jnp.dot(tokens, wq[half], preferred_element_type=F32)
        for n in range(4):
            x = full[:, n * 128 : n * 128 + 128].astype(BF).astype(F32)
            qs[2 * half + n // 2, :, (n % 2) * 128 : (n % 2) * 128 + 128] = rotate(x).astype(BF)

    for load in loads[:3]:
        load.wait()
    project_k(t)
    project_v(t)

    pl.semaphore_wait(barrier, len(peers))

    halves = [
        remote(wk.at[t], wk.at[t], w_send.at[0], w_recv.at[0], kv, other),
        remote(wv.at[t], wv.at[t], w_send.at[1], w_recv.at[1], kv, other),
        remote(wq.at[t], wq.at[t], w_send.at[2], w_recv.at[2], kv, other),
        remote(wo_hbm, wo.at[t], w_send.at[3], w_recv.at[3], kv, other),
    ]

    def to_owner(own, every, send, recv, head):
        return remote(
            own.at[head], every.at[chunk(z, y)], send.at[head], recv.at[y], z * NY + head, t
        )

    def key_to_owner(head):
        return to_owner(k_own, k_all, ky_send, ky_recv, head)

    def value_to_owner(head):
        return to_owner(v_own, v_all, vy_send, vy_recv, head)

    def send_heads(make, half):
        for e in range(2):
            head = 2 * half + e

            @pl.when(head != y)
            def _():
                make(head).start()

    def ring(every, up_send, up_recv, dn_send, dn_recv, pt_send, pt_recv):
        def place(zz, k):
            return every.at[chunk(zz, row_chip(k))]

        def up(s, k, src=None):
            spot = place(lax.rem(z + NZ - s, NZ), k)
            src = spot if src is None else src
            return remote(src, spot, up_send.at[s, k], up_recv.at[s, k], z_up, t)

        def down(s, k, src=None):
            spot = place(lax.rem(z + s, NZ), k)
            src = spot if src is None else src
            return remote(src, spot, dn_send.at[s, k], dn_recv.at[s, k], z_dn, t)

        def partner(rel, k, src=None):
            spot = place(lax.rem(z + rel, NZ), k)
            src = spot if src is None else src
            return remote(src, spot, pt_send.at[rel, k], pt_recv.at[rel, k], kv, other)

        return up, down, partner

    k_ring = ring(k_all, k_up_send, k_up_recv, k_dn_send, k_dn_recv, k_pt_send, k_pt_recv)
    v_ring = ring(v_all, v_up_send, v_up_recv, v_dn_send, v_dn_recv, v_pt_send, v_pt_recv)

    def begin(group, k, src=None):
        up, down, partner = group
        up(0, k, src).start()
        down(0, k, src).start()
        partner(0, k, src).start()

    def step(group, s, k):
        up, down, partner = group
        if s < NZ // 2:
            turn = s == NZ // 2 - 1
            up(s - 1, k).wait_recv()
            if not turn:
                up(s, k).start()
            else:
                pl.when(k < 2)(lambda: up(s, k).start())
            partner(NZ - s, k).start()
            down(s - 1, k).wait_recv()
            if not turn:
                down(s, k).start()
            else:
                pl.when(k >= 2)(lambda: down(s, k).start())
            partner(s, k).start()
        else:
            pl.when(k < 2)(lambda: up(s - 1, k).wait_recv())
            pl.when(k >= 2)(lambda: down(s - 1, k).wait_recv())
            partner(s, k).start()

    for copy in halves[:2]:
        copy.start()
    ready = y // 2 == t
    pl.when(ready)(lambda: begin(k_ring, 0, k_own.at[y]))
    send_heads(key_to_owner, t)
    picks = [
        remote(ch_hbm, ch_all.at[NY - k], c_send.at[k], c_recv.at[NY - k], row_peer(k), t)
        for k in range(1, NY)
    ]
    loads[3].wait()
    for copy in halves[2:] + picks:
        copy.start()
    halves[0].wait_recv()
    project_k(other)
    send_heads(key_to_owner, other)

    mine = [
        pltpu.make_async_copy(k_own.at[y], k_all.at[chunk(z, y)], load_sem.at[5]),
        pltpu.make_async_copy(v_own.at[y], v_all.at[chunk(z, y)], load_sem.at[7]),
    ]
    pl.when(jnp.logical_not(ready))(lambda: begin(k_ring, 0, k_own.at[y]))
    send_heads(value_to_owner, t)
    halves[1].wait_recv()
    project_v(other)
    send_heads(value_to_owner, other)
    begin(v_ring, 0, v_own.at[y])
    for copy in mine:
        copy.start()

    def from_row(every, own, send, recv, k):
        remote(
            own.at[0], every.at[chunk(z, row_chip(k))], send.at[0], recv.at[row_chip(k)],
            row_peer(k), t,
        ).wait_recv()

    for k in (1, 3, 2):
        from_row(k_all, k_own, ky_send, ky_recv, k)
        begin(k_ring, k)
    for copy in mine:
        copy.wait()
    for k in (1, 3, 2):
        from_row(v_all, v_own, vy_send, vy_recv, k)
        begin(v_ring, k)
    project_q(t)
    halves[2].wait_recv()
    project_q(other)
    own_q = pltpu.make_async_copy(qs.at[y], q_all.at[0], load_sem.at[6])
    own_q.start()
    queries = [None] * NY
    for k in (2, 1, 3):
        queries[NY - k] = remote(
            qs.at[row_chip(k)], q_all.at[NY - k], q_send.at[k], q_recv.at[NY - k],
            row_peer(k), t,
        )
        queries[NY - k].start()

    for copy in picks:
        copy.wait_recv()
    own_picks.wait()
    to_smem = pltpu.make_async_copy(ch_all, ch_smem, load_sem.at[13])
    to_smem.start()

    order = (0, 1, 3, 2)
    for s in range(1, NZ // 2 + 1):
        for k in order:
            step(k_ring, s, k)
        if s < NZ // 2:
            for k in order:
                step(v_ring, s, k)

    to_smem.wait()
    own_q.wait()
    for k in range(1, NY):
        queries[k].wait_recv()
    for rel in range(NZ):
        for k in range(NY):
            k_ring[2](rel, k).wait_recv()

    key_pos = lax.broadcasted_iota(jnp.int32, (BLK, 4 * BLK), 0)
    query_pos = lax.rem(lax.broadcasted_iota(jnp.int32, (BLK, 4 * BLK), 1), BLK)
    causal = key_pos <= query_pos
    half_blk = BLK // 2

    def own_block(k, jb):
        return (z * NY + row_chip(k)) * 8 + t * 4 + jb

    def gather_keys(k, jb):
        bias = []
        for j in range(PICK + 1):
            if j < PICK:
                pick = ch_smem[k, t * 4 + jb, j]
                bias.append(jnp.where(pick < 0, NEGATIVE, 0.0).astype(F32))
                block = k_all[jnp.maximum(pick, 0)]
            else:
                block = k_all[own_block(k, jb)]
            nothing = jnp.zeros_like(block)
            u, row = jb % 2, j * BLK
            kg[u, row : row + half_blk, :] = jnp.where(left_half, block, nothing)
            kg[u, row + half_blk : row + BLK, :] = jnp.where(left_half, nothing, block)
        return bias

    def load_queries(k, jb):
        heads = []
        for n in range(2):
            x = q_all[k, jb * BLK : jb * BLK + BLK, n * 128 : n * 128 + 128].astype(F32)
            swapped = pltpu.roll(x, 64, 1)
            heads += [jnp.where(left, x, swapped), jnp.where(left, swapped, x)]
        return jnp.concatenate(heads, axis=0).astype(BF)

    def eight(x, op):
        return op(x.reshape(BLK // 8, 8, 4 * BLK), axis=0)

    def score(u, half, q2, bias):
        span = 8 * BLK
        part = lax.dot_general(
            kg[u, half * span : half * span + span, :], q2, (((1,), (1,)), ((), ())),
            preferred_element_type=F32,
        )
        top = None
        for i in range(8):
            j = half * 8 + i
            block = part[i * BLK : i * BLK + BLK, :]
            if j == PICK:
                block = jnp.where(causal, block, NEGATIVE)
            scores[u, j * BLK : j * BLK + BLK, :] = block
            here = eight(block, jnp.max)
            here = here if j == PICK else here + bias[j]
            top = here if top is None else jnp.maximum(top, here)
        return top

    def softmax(state, half):
        k, slab, jb, top, bias, total = state
        for j in range(half * 8, half * 8 + 8):
            shift = top if j == PICK else top - bias[j]
            p = jnp.exp2((scores[jb % 2, j * BLK : j * BLK + BLK, :] - shift) * EXPONENT)
            part = eight(p, jnp.sum)
            total = part if total is None else total + part
            probs[slab * 4 + jb, j * BLK : j * BLK + BLK, :] = p.astype(BF)
        if half == 1:
            total = jnp.sum(total, axis=0, keepdims=True)
            inverse[k, pl.ds(jb, 1), :] = 1.0 / total
            logsum = top * HEAD_DIM**-0.5 + jnp.log(total)
            for h in range(4):
                ls_out[k, pl.ds(h, 1), jb * BLK : jb * BLK + BLK] = logsum[:, h * BLK : h * BLK + BLK]
        return k, slab, jb, top, bias, total

    def weigh(k, slab):
        state = None
        for jb in range(4):
            bias = gather_keys(k, jb)
            q2 = load_queries(k, jb)
            tops = []
            for half in range(2):
                tops.append(score(jb % 2, half, q2, bias))
                if state is not None:
                    state = softmax(state, half)
            top = jnp.max(jnp.maximum(*tops), axis=0, keepdims=True)
            state = (k, slab, jb, top, bias, None)
        for half in range(2):
            state = softmax(state, half)

    def gather_values(k, jb):
        previous = None
        for j in range(PICK + 1):
            if j < PICK:
                block = v_all[jnp.maximum(ch_smem[k, t * 4 + jb, j], 0)]
            else:
                block = v_all[own_block(k, jb)]
            block = block.astype(F32)
            if j % 2 == 1:
                low = jnp.where(left_half, previous, pltpu.roll(block, 64, 1))
                high = jnp.where(left_half, pltpu.roll(previous, 64, 1), block)
                columns = slice((j // 2) * 128, (j // 2) * 128 + 128)
                vt[jb, :half_blk, columns] = low.astype(BF)
                vt[jb, half_blk:, columns] = high.astype(BF)
            previous = block

    def combine(k, slab):
        for jb in range(4):
            gather_values(k, jb)
        mixed = [
            jnp.dot(vt[jb], probs[slab * 4 + jb], preferred_element_type=F32) for jb in range(4)
        ]
        for jb in range(4):
            turned_back = (mixed[jb] * inverse[k, pl.ds(jb, 1), :]).T
            parts = [turned_back[h * BLK : h * BLK + BLK] for h in range(4)]
            att_out[k, jb * BLK : jb * BLK + BLK, :] = jnp.concatenate(parts, axis=1).astype(BF)

    to_self = y // 2 == t
    slot = (lax.rem(y, 2), t)

    def log_piece(k):
        return remote(
            ls_out.at[k], ls_all.at[slot], l_send.at[k], l_recv.at[slot], row_peer(k), y // 2
        )

    def give_back(k):
        return remote(
            att_out.at[k], att_all.at[NY - k], a_send.at[k], a_recv.at[NY - k], row_peer(k), t
        )

    @pl.loop(0, NY)
    def _(i):
        weigh(lax.rem(i + 1, NY), lax.rem(i, 2))

        @pl.when(i == 0)
        def _():
            for r in order:
                step(v_ring, NZ // 2, r)

        @pl.when(i == 1)
        def _():
            for rel in range(NZ):
                for r in range(NY):
                    v_ring[2](rel, r).wait_recv()

        ready_from = jnp.where(i == 1, 0, i)
        ready_to = jnp.where(i == 0, 0, i + 1)

        @pl.loop(ready_from, ready_to)
        def _(g):
            k = lax.rem(g + 1, NY)
            combine(k, lax.rem(g, 2))

            @pl.when(k > 0)
            def _():
                give_back(k).start()
                log_piece(k).start()

    pl.when(jnp.logical_not(to_self))(lambda: log_piece(0).start())

    @pl.when(to_self)
    def _():
        ls_all[slot] = ls_out[0]

    loads[4].wait()
    halves[3].wait_recv()
    def part(k):
        ys = row_chip(k)
        weights = wo[ys // 2, pl.ds(pl.multiple_of(lax.rem(ys, 2) * 256, 256), 256), :]
        piece = att_out[0] if k == 0 else att_all[k]
        return jnp.dot(piece, weights, preferred_element_type=F32)

    for k in (1, 2):
        give_back(k).wait_recv()
    acc[...] = part(0) + part(3) + part(2)
    give_back(3).wait_recv()
    projected = acc[...] + part(1)
    square = jnp.mean(projected * projected, axis=-1, keepdims=True)
    out_ref[...] = (projected * lax.rsqrt(square + EPSILON)).astype(BF)

    for ys in range(2):
        for tt in range(2):
            @pl.when(jnp.logical_not((t * 2 + ys == y) & (t == tt)))
            def _():
                remote(
                    ls_out.at[0], ls_all.at[ys, tt], l_send.at[0], l_recv.at[ys, tt], kv, other
                ).wait_recv()

            ls_ref[ys * 4 : ys * 4 + 4, tt * 4 * BLK : tt * 4 * BLK + 4 * BLK] = ls_all[ys, tt]
    for k in range(1, NY):
        log_piece(k).wait_send()
    pl.when(jnp.logical_not(to_self))(lambda: log_piece(0).wait_send())
    for k in range(1, NY):
        key_to_owner(row_chip(k)).wait_send()
        value_to_owner(row_chip(k)).wait_send()
        queries[k].wait_send()
        give_back(k).wait_send()
    for copy in halves + picks:
        copy.wait_send()
    for up, down, partner in (k_ring, v_ring):
        for k in range(NY):
            for s in range(NZ // 2):
                if s < NZ // 2 - 1 or k < 2:
                    up(s, k).wait_send()
                if s < NZ // 2 - 1 or k >= 2:
                    down(s, k).wait_send()
            for rel in range(NZ):
                partner(rel, k).wait_send()


def shards(tokens, w_query, w_key, w_value, w_out, chosen):
    rows, width = tokens.shape[1:]
    tables = rotary_tables(rows, 2 * NY * NZ)
    any_space = pl.BlockSpec(memory_space=pl.ANY)
    vmem = pl.BlockSpec(memory_space=pltpu.VMEM)
    dma = pltpu.SemaphoreType.DMA
    out, logs = pl.pallas_call(
        kernel,
        out_shape=(
            jax.ShapeDtypeStruct((rows, width), BF),
            jax.ShapeDtypeStruct((8, 2 * rows), F32),
        ),
        in_specs=[any_space] * 10,
        out_specs=(vmem, vmem),
        scratch_shapes=[
            pltpu.VMEM((rows, 128), F32),
            pltpu.VMEM((rows, 128), F32),
            pltpu.VMEM((2 * NY * NZ, 128), F32),
            pltpu.VMEM((2 * NY * NZ, 128), F32),
            pltpu.VMEM((rows, width), BF),
            pltpu.VMEM((2,) + w_query.shape, BF),
            pltpu.VMEM((2,) + w_key.shape, BF),
            pltpu.VMEM((2,) + w_value.shape, BF),
            pltpu.VMEM((2,) + w_out.shape, BF),
            pltpu.VMEM((rows, 128), F32),
            pltpu.VMEM((rows, 128), F32),
            pltpu.VMEM((4, 4, BLK // 2, 128), BF),
            pltpu.VMEM((4, 4, BLK // 2, 128), BF),
            pltpu.VMEM((NZ * NY * 8, BLK // 2, 128), BF),
            pltpu.VMEM((NZ * NY * 8, BLK // 2, 128), BF),
            pltpu.VMEM((NY, rows, 256), BF),
            pltpu.VMEM((NY, rows, 256), BF),
            pltpu.VMEM((NY, 8, PICK), jnp.int32),
            pltpu.SMEM((NY, 8, PICK), jnp.int32),
            pltpu.VMEM((2, (PICK + 1) * BLK, 128), BF),
            pltpu.VMEM((4, BLK, (PICK + 1) * BLK), BF),
            pltpu.VMEM((2, (PICK + 1) * BLK, 4 * BLK), F32),
            pltpu.VMEM((8, (PICK + 1) * BLK, 4 * BLK), BF),
            pltpu.VMEM((NY, 4, 4 * BLK), F32),
            pltpu.VMEM((NY, rows, 256), BF),
            pltpu.VMEM((NY, rows, 256), BF),
            pltpu.VMEM((NY, 4, 4 * BLK), F32),
            pltpu.VMEM((2, 2, 4, 4 * BLK), F32),
            pltpu.VMEM((rows, width), F32),
            dma((14,)), dma((4,)), dma((4,)), dma((4,)), dma((4,)), dma((4,)), dma((4,)),
            dma((4, 4)), dma((4, 4)), dma((4, 4)), dma((4, 4)), dma((NZ, 4)), dma((NZ, 4)),
            dma((4, 4)), dma((4, 4)), dma((4, 4)), dma((4, 4)), dma((NZ, 4)), dma((NZ, 4)),
            dma((4,)), dma((4,)), dma((4,)), dma((4,)),
            dma((4,)), dma((4,)), dma((4,)), dma((2, 2)),
        ],
        compiler_params=pltpu.CompilerParams(
            collective_id=0, has_side_effects=True, vmem_limit_bytes=67_000_000
        ),
    )(*tables, tokens[0], w_query, w_key, w_value, w_out, chosen[0])
    return out[None], logs.T[None]


def solution(mesh):
    placed = (
        P("dp", ("kv", "tp"), None),
        P(None, "tp"),
        P(None, "tp"),
        P(None, "tp"),
        P("tp", None),
        P("dp", "kv", None),
    )
    return jax.shard_map(
        shards,
        mesh=mesh,
        in_specs=placed,
        out_specs=(P("dp", ("kv", "tp"), None), P("dp", "kv", "tp")),
        check_vma=False,
    )
```
